32 devices in a mesh: sp: 8 (over z, x), tp: 4 (over y, core).
Axes of the slice: x: 2, y: 2, z: 4, core: 2. Of those that a mesh axis runs over, the one named last changes fastest.
Arguments:
- moe_input: bfloat16 [1024, 2048], P('sp'), may hold values from -6 to 6
- out_grad: bfloat16 [1024, 2048], P('sp'), may hold values from -6 to 6
- routes: int32 [1024, 2], P('sp'), may hold values from 0 to 7, all different within a row; in each aligned block of 128 rows (0 to 127, 128 to 255, ...) at most 40 rows name the same one
- route_weight: float32 [1024, 2], P('sp'), may hold values from 0.2 to 1.2
- w_gate: bfloat16 [8, 2048, 2048], P('sp', None, 'tp'), may hold values from -0.125 to 0.125
- w_up: bfloat16 [8, 2048, 2048], P('sp', None, 'tp'), may hold values from -0.125 to 0.125
- w_down: bfloat16 [8, 2048, 2048], P('sp', 'tp'), may hold values from -0.125 to 0.125
- w_out: bfloat16 [2048, 4096], P(None, 'tp'), may hold values from -0.09375 to 0.09375
- query_heads: bfloat16 [16, 1024, 128], P('tp', 'sp'), may hold values from -6 to 6
- key_heads: bfloat16 [16, 1024, 128], P('tp', 'sp'), may hold values from -6 to 6
- value_heads: bfloat16 [16, 1024, 256], P('tp', 'sp'), may hold values from -6 to 6
- log_decay: float32 [16, 1024], P('tp', 'sp'), may hold values from -0.6 to 0
- state_in: float32 [16, 8, 128, 256], P('tp', 'sp'), may hold values from -4 to 4
Outputs:
- gate_grad: bfloat16 [8, 2048, 2048], P('sp', None, 'tp')
- up_grad: bfloat16 [8, 2048, 2048], P('sp', None, 'tp')
- down_grad: bfloat16 [8, 2048, 2048], P('sp', 'tp')
- out_proj_grad: float32 [2048, 4096], P('sp', 'tp')
- query_gradient: bfloat16 [16, 1024, 128], P('tp', 'sp')
- key_grad: bfloat16 [16, 1024, 128], P('tp', 'sp')
- value_grad: bfloat16 [16, 1024, 256], P('tp', 'sp')
The draws below stay inside these ranges and needn't reach their ends.
Inputs may be any that keep to these rules, and one draw needn't show every extreme that they name: `routes`: each row names 2 different experts; within each aligned block of 128 tokens no expert is named more than 40 times, and exactly 40 times for some expert in some blocks.
All inputs are finite; a program needn't handle non-finite values.
Results may differ from the reference program's by a relative error of at most 0.025.
Values may be sent and summed in bfloat16 or wider, within the bound.
No kernel may reach another device: no remote copies, remote signals or barrier semaphores. Data moves between devices by JAX's collectives and lax.ppermute only.
A program may use at most 64 MiB of HBM per device.

```python
import math
import jax
import jax.numpy as jnp
import numpy as np
from jax import lax

D = 2048
FF = 2048
RETENTION_HEADS = 16
DK = 128
DV = 256
TOPK = 2
BLOCK = 64
TOK_DEV = 128
SEQUENCE_TOKENS = 1024
EXPERTS = 8
CAP = 40
N_SP = 8
N_TP = 4


def draw_log_decay(key, part):
    random_subkeys = jax.random.split(jax.random.fold_in(key, 11), 6)
    fast_share = 0.5
    quick_heads = jax.random.uniform(random_subkeys[0], (RETENTION_HEADS,), jnp.float32) < fast_share
    fast_rate = jnp.log(10.0) / jax.random.uniform(random_subkeys[1], (RETENTION_HEADS,), jnp.float32, 30.0, 50.0)
    slow_rate = jax.random.uniform(random_subkeys[2], (RETENTION_HEADS,), jnp.float32, 0.2, 0.5) / SEQUENCE_TOKENS
    head_decay_rate = jnp.where(quick_heads, fast_rate, slow_rate)
    span_total = SEQUENCE_TOKENS // TOK_DEV
    span_factor = jnp.exp(jax.random.uniform(random_subkeys[3], (span_total,), jnp.float32, jnp.log(0.5), jnp.log(2.0)))
    position_weighting = jnp.repeat(span_factor, TOK_DEV)
    surge_locations = jax.random.randint(random_subkeys[4], (RETENTION_HEADS, 2), 0, SEQUENCE_TOKENS)
    surge_depth = jnp.log(jax.random.uniform(random_subkeys[5], (RETENTION_HEADS, 2), jnp.float32, 0.6, 0.8))
    token_positions = jnp.arange(SEQUENCE_TOKENS, dtype=jnp.int32)
    match_flags = token_positions[None, :, None] == surge_locations[:, None, :]
    surge_events = jnp.sum(jnp.where(match_flags, surge_depth[:, None, :], 0.0), axis=2)
    logarithm_values = -head_decay_rate[:, None] * position_weighting[None, :] + jnp.where(quick_heads[:, None], 0.0, surge_events)
    return logarithm_values.astype(jnp.float32)


def spiked(values, own_key, source, target, parts, factor):
    owner, partner = [(jnp.arange(values.shape[position]) // (values.shape[position] // parts)).reshape([-1 if axis == position else 1 for axis in range(values.ndim)]) for position in (source, target)]
    chosen = jax.random.permutation(own_key, parts)[partner]
    strong = (owner == chosen) | (owner == (partner + parts // 2) % parts)
    return jnp.where(strong, factor * values, values)


def block_scale(own_key, shape, shards, least, top_value):
    def one(position, blocks):
        heights = jax.random.uniform(jax.random.fold_in(jax.random.fold_in(own_key, 6), position), (blocks,), jnp.float32, least / len(shards), top_value / len(shards))
        return jnp.repeat(jnp.exp(heights), shape[position] // blocks).reshape((-1,) + (1,) * (len(shape) - position - 1))

    loudness = one(*shards[0])
    for cut in shards[1:]:
        loudness = loudness * one(*cut)
    return loudness


def deal_out(rng, own, number, rows, number_of, top, reach, slope):
    ranking = jax.random.permutation(rng, number_of)
    heavy_load, ordinary = load_shares(number_of, rows * top, reach, slope, True), load_shares(number_of, rows * top, reach, slope, False)
    places = jnp.arange(number_of)

    def named(sizes, offset_by):
        used = int((sizes > 0).sum())
        fixed = max(1, used // 4)
        moved = fixed + (places - fixed + offset_by * (used - fixed)) % max(1, number_of - fixed)
        return jnp.zeros((number_of,), jnp.int32).at[ranking[jnp.where(places < fixed, places, moved)]].set(jnp.asarray(sizes, jnp.int32))

    sizes = jnp.where(number % 4 == 0, named(heavy_load, number // 4), named(ordinary, number - number // 4 - 1))
    mixed = jax.random.permutation(jax.random.fold_in(own, 3), number_of)
    giver, taker = mixed[0:number_of // 2 * 2:2], mixed[1:number_of // 2 * 2:2]
    room = jnp.minimum(sizes[giver] - 1, reach - sizes[taker]) // 2
    room = jnp.where((giver == ranking[0]) | (taker == ranking[0]) | (sizes[taker] == 0), 0, jnp.maximum(room, 0))
    moved = jax.random.randint(jax.random.fold_in(own, 4), (number_of // 2,), 0, 1 << 20) % (room + 1)
    sizes = sizes.at[giver].add(-moved).at[taker].add(moved)
    items = jnp.searchsorted(jnp.cumsum(sizes), jnp.arange(rows * top), side="right").astype(jnp.int32)
    grid = items.reshape(top, rows).T
    grid = grid[jax.random.permutation(jax.random.fold_in(own, 1), rows)]
    offset_by = jax.random.randint(jax.random.fold_in(own, 2), (rows, 1), 0, top)
    return jnp.take_along_axis(grid, (jnp.arange(top)[None, :] + offset_by) % top, axis=1)


def load_shares(amount, total, most, lean, full):
    weights = [(1 << 20) // math.isqrt(rank ** lean) + 1 for rank in range(1, amount + 1)]
    largest = most if full else min(most, max(-(-total // amount), total * weights[0] // sum(weights)))
    least = 1 if total - largest >= amount - 1 else 0
    counts, rest = [largest] + [least] * (amount - 1), total - largest - least * (amount - 1)
    while rest > 0:
        free = [i for i in range(1, amount) if counts[i] < largest] or [i for i in range(1, amount) if counts[i] < most]
        whole, remaining = sum([weights[i] for i in free]), rest
        for i in free:
            extra = min(most - counts[i], max(1, remaining * weights[i] // whole), rest)
            counts[i] = counts[i] + extra
            rest = rest - extra
    return np.array(counts)


def bell_draw(own_key, shape, width, reach, shards=(), kind=jnp.bfloat16):
    entries = width * jax.random.normal(own_key, shape, jnp.float32)
    if shards:
        entries = entries * block_scale(own_key, shape, shards, -0.22, 0.18)
    return jnp.clip(entries, -reach, reach).astype(kind)


def bell_draw_with(stream_key, dims, scale, most, shards, heavy, kind=jnp.bfloat16):
    values = scale * jax.random.normal(stream_key, dims, jnp.float32)
    if shards:
        values = values * block_scale(stream_key, dims, shards, -0.22, 0.18)
    return jnp.clip(spiked(values, jax.random.fold_in(stream_key, 3), *heavy), -most, most).astype(kind)


def setup_inputs(seed: int = 0) -> dict:
    streams_of = jax.random.split(jax.random.key(seed), 14)
    moe_input = bell_draw(streams_of[0], (SEQUENCE_TOKENS, D), 1.0, 6.0, ((0, 8),))
    out_grad = bell_draw_with(streams_of[1], (SEQUENCE_TOKENS, D), 1.0, 6.0, ((0, 8),), (0, 1, 8, 2.0))
    routes_keys = jax.random.split(jax.random.fold_in(streams_of[2], 1), SEQUENCE_TOKENS // TOK_DEV)
    routes_turns = jax.random.permutation(jax.random.fold_in(streams_of[2], 3), SEQUENCE_TOKENS // TOK_DEV)
    routes = jax.vmap(lambda own, number: deal_out(jax.random.fold_in(streams_of[2], 2), own, number, TOK_DEV, EXPERTS, TOPK, CAP, 2))(routes_keys, routes_turns).reshape((SEQUENCE_TOKENS, TOPK))
    route_weight = jnp.clip(0.2 + 1 * jax.random.uniform(streams_of[3], (SEQUENCE_TOKENS, TOPK), jnp.float32) ** block_scale(streams_of[3], (SEQUENCE_TOKENS, TOPK), ((0, 8),), -0.2, 0.2), 0.2, 1.2)
    w_gate = bell_draw(streams_of[4], (EXPERTS, D, FF), D ** -0.5, 0.125, ((0, 8), (2, 4)))
    w_up = bell_draw(streams_of[5], (EXPERTS, D, FF), D ** -0.5, 0.125, ((0, 8), (2, 4)))
    w_down = bell_draw(streams_of[6], (EXPERTS, FF, D), FF ** -0.5, 0.125, ((0, 8), (1, 4)))
    w_out = bell_draw(streams_of[7], (D, RETENTION_HEADS * DV), (RETENTION_HEADS * DV) ** -0.5, 0.09375, ((1, 4),))
    query_heads = bell_draw(streams_of[8], (RETENTION_HEADS, SEQUENCE_TOKENS, DK), 1.0, 6.0, ((0, 4), (1, 8)))
    key_heads = bell_draw(streams_of[9], (RETENTION_HEADS, SEQUENCE_TOKENS, DK), 1.0, 6.0, ((0, 4), (1, 8)))
    value_heads = bell_draw(streams_of[10], (RETENTION_HEADS, SEQUENCE_TOKENS, DV), 1.0, 6.0, ((0, 4), (1, 8)))
    log_decay = draw_log_decay(jax.random.fold_in(streams_of[13], 71), 0)
    state_in = bell_draw(streams_of[12], (RETENTION_HEADS, N_SP, DK, DV), 0.5, 4.0, ((0, 4), (1, 8)), jnp.float32)
    return dict(moe_input=moe_input, out_grad=out_grad, routes=routes, route_weight=route_weight, w_gate=w_gate, w_up=w_up, w_down=w_down, w_out=w_out, query_heads=query_heads, key_heads=key_heads, value_heads=value_heads, log_decay=log_decay, state_in=state_in)


exact_precision = lax.Precision.HIGHEST


def stored(array):
    return lax.optimization_barrier(array.astype(jnp.bfloat16))


def silu_slope(gate_pre):
    sigmoid_v = jax.nn.sigmoid(gate_pre)
    return sigmoid_v * (1.0 + gate_pre * (1.0 - sigmoid_v))


def decay_table(log_sums):
    block_size = log_sums.shape[-1]
    token_positions = jnp.arange(block_size)
    lower_mask = (token_positions[:, None] >= token_positions[None, :])[None]
    log_diff = jnp.where(lower_mask, log_sums[:, :, None] - log_sums[:, None, :], 0.0)
    return jnp.where(lower_mask, jnp.exp(log_diff), 0.0)


def forward_block(forwarded_state, inputs):
    query_rows, rescaled_keys, value_rows, head_gradients, log_sums = inputs
    decay_mat = decay_table(log_sums)
    scores = jnp.einsum('htk,hsk->hts', query_rows, rescaled_keys, precision=exact_precision) * decay_mat
    leading_decay = jnp.exp(log_sums)[:, :, None]
    trailing_decay = jnp.exp(log_sums[:, -1:] - log_sums)[:, :, None]
    blended_heads = jnp.einsum('hts,hsv->htv', scores, value_rows, precision=exact_precision)
    blended_heads = blended_heads + jnp.einsum('imj,iju->imu', query_rows * leading_decay, forwarded_state, precision=exact_precision)
    back_scores = jnp.einsum('htv,hsv->hts', head_gradients, value_rows, precision=exact_precision) * decay_mat
    query_gradient = jnp.einsum('hts,hsk->htk', back_scores, rescaled_keys, precision=exact_precision)
    query_gradient = query_gradient + jnp.einsum('fqg,fug->fqu', head_gradients * leading_decay, forwarded_state, precision=exact_precision)
    forwarded_state = jnp.exp(log_sums[:, -1])[:, None, None] * forwarded_state + jnp.einsum(
        'nbq,nbc->nqc', rescaled_keys * trailing_decay, value_rows, precision=exact_precision)
    return forwarded_state, (blended_heads, query_gradient)


def reverse_block(forwarded_state, inputs):
    query_rows, rescaled_keys, value_rows, head_gradients, log_sums = inputs
    decay_mat = decay_table(log_sums)
    scores = jnp.einsum('htk,hsk->hts', query_rows, rescaled_keys, precision=exact_precision) * decay_mat
    back_scores = jnp.einsum('htv,hsv->hts', head_gradients, value_rows, precision=exact_precision) * decay_mat
    leading_decay = jnp.exp(log_sums)[:, :, None]
    trailing_decay = jnp.exp(log_sums[:, -1:] - log_sums)[:, :, None]
    key_portion = jnp.einsum('hts,htk->hsk', back_scores, query_rows, precision=exact_precision)
    key_portion = key_portion + jnp.einsum('lbg,ljg->lbj', value_rows * trailing_decay, forwarded_state, precision=exact_precision)
    value_portion = jnp.einsum('hts,htv->hsv', scores, head_gradients, precision=exact_precision)
    value_portion = value_portion + jnp.einsum('bea,baz->bez', rescaled_keys * trailing_decay, forwarded_state, precision=exact_precision)
    forwarded_state = jnp.exp(log_sums[:, -1])[:, None, None] * forwarded_state + jnp.einsum(
        'byj,byg->bjg', query_rows * leading_decay, head_gradients, precision=exact_precision)
    return forwarded_state, (key_portion, value_portion)


def reference(moe_input, out_grad, routes, route_weight, w_gate, w_up, w_down, w_out,
              query_heads, key_heads, value_heads, log_decay, state_in):
    routed_all = TOK_DEV * TOPK
    route_ids = routes.reshape(N_SP, routed_all)
    onehot = (route_ids[:, :, None] == jnp.arange(EXPERTS, dtype=jnp.int32)[None, None, :]).astype(jnp.int32)
    slot_index = jnp.sum(jnp.cumsum(onehot, axis=1) * onehot, axis=2) - 1
    anchor = jnp.arange(N_SP, dtype=jnp.int32)[:, None]
    row_place = (anchor * CAP + slot_index).astype(jnp.int32)
    token_id = (anchor * TOK_DEV + jnp.arange(routed_all, dtype=jnp.int32)[None, :] // TOPK).astype(jnp.int32)
    expert_rows = N_SP * CAP
    token_table = jnp.full((EXPERTS, expert_rows), -1, jnp.int32).at[route_ids, row_place].set(token_id)
    weight_table = jnp.zeros((EXPERTS, expert_rows), jnp.float32).at[route_ids, row_place].set(
        route_weight.reshape(N_SP, routed_all))
    group_width = FF // N_TP

    def one_expert(expert_items):
        token_row, weight_row, gate_w, up_w, down_w = expert_items
        filled = token_row >= 0
        picked = jnp.where(filled, token_row, 0)
        rows_in = jnp.where(filled[:, None], moe_input[picked], jnp.zeros((), jnp.bfloat16))
        scaled = stored(jnp.where(filled[:, None], weight_row[:, None] * out_grad[picked].astype(jnp.float32), 0.0))
        gate_pre = jnp.dot(rows_in, gate_w, preferred_element_type=jnp.float32)
        up_pre = jnp.dot(rows_in, up_w, preferred_element_type=jnp.float32)
        active = jax.nn.silu(gate_pre)
        hidden = stored(active * up_pre)
        hidden_back = jnp.dot(scaled, down_w.T, preferred_element_type=jnp.float32)
        down_part = jnp.dot(hidden.T, scaled, preferred_element_type=jnp.float32).astype(jnp.bfloat16)
        gate_back = stored(hidden_back * up_pre * silu_slope(gate_pre))
        up_back = stored(hidden_back * active)
        gate_part = jnp.dot(rows_in.T, gate_back, preferred_element_type=jnp.float32).astype(jnp.bfloat16)
        up_part = jnp.dot(rows_in.T, up_back, preferred_element_type=jnp.float32).astype(jnp.bfloat16)
        groups_gate = gate_back.astype(jnp.float32).reshape(expert_rows, N_TP, group_width)
        groups_up = up_back.astype(jnp.float32).reshape(expert_rows, N_TP, group_width)
        weights_gate = gate_w.astype(jnp.float32).reshape(D, N_TP, group_width)
        weights_up = up_w.astype(jnp.float32).reshape(D, N_TP, group_width)
        partial_value = jnp.einsum('rgf,dgf->grd', groups_gate, weights_gate)
        partial_value = partial_value + jnp.einsum('rgf,dgf->grd', groups_up, weights_up)
        route_back = jnp.sum(stored(partial_value).astype(jnp.float32), axis=0).astype(jnp.bfloat16)
        return gate_part, up_part, down_part, route_back

    gate_grad, up_grad, down_grad, route_back = lax.map(
        one_expert, (token_table, weight_table, w_gate, w_up, w_down))
    returned = route_back[route_ids, row_place].reshape(SEQUENCE_TOKENS, TOPK, D)
    mixed_grad = (out_grad.astype(jnp.float32) + jnp.sum(returned.astype(jnp.float32), axis=1)).astype(jnp.bfloat16)

    head_grad = stored(jnp.dot(mixed_grad, w_out, preferred_element_type=jnp.float32))
    head_gradients = head_grad.astype(jnp.float32).reshape(SEQUENCE_TOKENS, RETENTION_HEADS, DV).transpose(1, 0, 2)
    block_count = SEQUENCE_TOKENS // BLOCK
    per_span = TOK_DEV // BLOCK

    def to_blocks(array):
        return array.reshape(RETENTION_HEADS, block_count, BLOCK, array.shape[-1]).transpose(1, 0, 2, 3)

    def from_blocks(array):
        return array.transpose(1, 0, 2, 3).reshape(RETENTION_HEADS, SEQUENCE_TOKENS, array.shape[-1])

    query_rows = query_heads.astype(jnp.float32)
    rescaled_keys = key_heads.astype(jnp.float32) * DK ** -0.5
    value_rows = value_heads.astype(jnp.float32)
    log_sums = jnp.cumsum(log_decay.reshape(RETENTION_HEADS, block_count, BLOCK), axis=2).transpose(1, 0, 2)
    inputs = (to_blocks(query_rows), to_blocks(rescaled_keys), to_blocks(value_rows), to_blocks(head_gradients), log_sums)

    def forward_step(forwarded_state, block_items):
        block_index = block_items[-1]
        fresh_state = lax.dynamic_index_in_dim(state_in, block_index // per_span, axis=1, keepdims=False)
        start_state = jnp.where(block_index % per_span == 0, fresh_state, forwarded_state)
        return forward_block(start_state, block_items[:-1])

    empty_state = jnp.zeros((RETENTION_HEADS, DK, DV), jnp.float32)
    _, (blended_heads, query_gradient) = lax.scan(
        forward_step, empty_state, inputs + (jnp.arange(block_count, dtype=jnp.int32),))
    _, (key_grad, value_grad) = lax.scan(reverse_block, empty_state, inputs, reverse=True)
    mixed_flat = from_blocks(blended_heads).astype(jnp.bfloat16).transpose(1, 0, 2).reshape(SEQUENCE_TOKENS, RETENTION_HEADS * DV)
    out_proj_grad = jnp.dot(mixed_grad.T, mixed_flat, preferred_element_type=jnp.float32)
    query_gradient = from_blocks(query_gradient).astype(jnp.bfloat16)
    key_grad = (from_blocks(key_grad) * DK ** -0.5).astype(jnp.bfloat16)
    value_grad = from_blocks(value_grad).astype(jnp.bfloat16)
    return gate_grad, up_grad, down_grad, out_proj_grad, query_gradient, key_grad, value_grad
```

```python
import functools

import jax
import jax.numpy as jnp
from jax import lax
from jax.experimental import pallas as pl
from jax.experimental.pallas import tpu as pltpu
from jax.sharding import PartitionSpec as P

F32 = jnp.float32
BF16 = jnp.bfloat16
EXACT = lax.Precision.HIGHEST


def dot(a, b, ca=1, cb=0, precision=None):
    return lax.dot_general(
        a, b, (((ca,), (cb,)), ((), ())), preferred_element_type=F32, precision=precision
    )


def iota(shape, axis):
    return lax.broadcasted_iota(jnp.int32, shape, axis)


def dispatch_kernel(core, routes, weight, x, g, rows, grads, place, *, experts, cap):
    tokens = routes.shape[0]
    slots = experts * cap
    expert = iota((tokens, experts), 1)
    first = routes[:, 0:1] == expert
    second = routes[:, 1:2] == expert
    named = jnp.where(first | second, 1.0, 0.0)
    share = jnp.where(first, weight[:, 0:1], 0.0) + jnp.where(second, weight[:, 1:2], 0.0)
    before = jnp.where(iota((tokens, tokens), 0) < iota((tokens, tokens), 1), 1.0, 0.0)
    same = jnp.where(iota((tokens, tokens), 0) == iota((tokens, tokens), 1), 1.0, 0.0)
    rank_t = dot(named.astype(BF16), before.astype(BF16), 0, 0)
    named_t = dot(named.astype(BF16), same.astype(BF16), 0, 0)
    slot = iota((slots, experts), 0)
    base = iota((slots, experts), 1) * cap
    owner = (slot >= base) & (slot < base + cap)
    owner_f = jnp.where(owner, 1.0, 0.0).astype(BF16)
    number = jnp.sum(jnp.where(owner, slot - base, 0).astype(F32), axis=1, keepdims=True)
    rank = dot(owner_f, rank_t.astype(BF16))
    hit = dot(owner_f, named_t.astype(BF16))
    picked = jnp.where((rank == number) & (hit > 0.5), 1.0, 0.0)
    picked_b = picked.astype(BF16)
    share_slot = jnp.sum(
        jnp.where(owner, dot(picked, share, precision=EXACT), 0.0), axis=1, keepdims=True
    )
    place[...] = picked_b
    rows[...] = dot(picked_b, x[...]).astype(BF16)
    grads[...] = (share_slot * dot(picked_b, g[...])).astype(BF16)


def dispatch(core, routes, weight, x, g, experts, cap):
    tokens, width = x.shape
    half = width // 2
    slots = experts * cap
    whole = lambda i, c: (0, 0)
    return pl.pallas_call(
        functools.partial(dispatch_kernel, experts=experts, cap=cap),
        grid_spec=pltpu.PrefetchScalarGridSpec(
            num_scalar_prefetch=1,
            grid=(1,),
            in_specs=[
                pl.BlockSpec(routes.shape, whole),
                pl.BlockSpec(weight.shape, whole),
                pl.BlockSpec((tokens, half), lambda i, c: (0, c[0])),
                pl.BlockSpec((tokens, half), lambda i, c: (0, c[0])),
            ],
            out_specs=[
                pl.BlockSpec((slots, half), whole),
                pl.BlockSpec((slots, half), whole),
                pl.BlockSpec((slots, tokens), whole),
            ],
        ),
        out_shape=[
            jax.ShapeDtypeStruct((slots, half), BF16),
            jax.ShapeDtypeStruct((slots, half), BF16),
            jax.ShapeDtypeStruct((slots, tokens), BF16),
        ],
        name="dispatch",
    )(core, routes, weight, x, g)


def expert_kernel(
    core, ra, rb, ga, gb, wga, wgb, wua, wub, wda, wdb, hidden, gback, uback, pa, pb, acca, accb
):
    step = pl.program_id(0)
    gate = dot(ra[...], wga[...]) + dot(rb[...], wgb[...])
    up = dot(ra[...], wua[...]) + dot(rb[...], wub[...])
    back = dot(ga[...], wda[...], 1, 1) + dot(gb[...], wdb[...], 1, 1)
    sig = 1.0 / (1.0 + jnp.exp(-gate))
    active = gate * sig
    hidden[...] = (active * up).astype(BF16)
    gb_v = (back * up * (sig * (1.0 + gate * (1.0 - sig)))).astype(BF16)
    ub_v = (back * active).astype(BF16)
    gback[...] = gb_v
    uback[...] = ub_v
    part_a = dot(gb_v, wga[...], 1, 1) + dot(ub_v, wua[...], 1, 1)
    part_b = dot(gb_v, wgb[...], 1, 1) + dot(ub_v, wub[...], 1, 1)

    @pl.when(step == 0)
    def _():
        acca[...] = part_a
        accb[...] = part_b

    @pl.when(step > 0)
    def _():
        acca[...] += part_a
        accb[...] += part_b

    @pl.when(step == pl.num_programs(0) - 1)
    def _():
        pa[...] = acca[...].astype(BF16)
        pb[...] = accb[...].astype(BF16)


def expert_back(core, ra, rb, ga, gb, w_gate, w_up, w_down):
    rows, half = ra.shape
    units = w_gate.shape[2]
    chunk = min(units, 256)
    whole = lambda f, c: (0, 0)
    mine = pl.BlockSpec((None, half, chunk), lambda f, c: (0, c[0], f))
    other = pl.BlockSpec((None, half, chunk), lambda f, c: (0, 1 - c[0], f))
    mine_d = pl.BlockSpec((None, chunk, half), lambda f, c: (0, f, c[0]))
    other_d = pl.BlockSpec((None, chunk, half), lambda f, c: (0, f, 1 - c[0]))
    full = pl.BlockSpec((rows, half), whole)
    part = pl.BlockSpec((rows, chunk), lambda f, c: (0, f))
    return pl.pallas_call(
        expert_kernel,
        grid_spec=pltpu.PrefetchScalarGridSpec(
            num_scalar_prefetch=1,
            grid=(units // chunk,),
            in_specs=[full] * 4 + [mine, other, mine, other, mine_d, other_d],
            out_specs=[part, part, part, full, full],
            scratch_shapes=[pltpu.VMEM((rows, half), F32), pltpu.VMEM((rows, half), F32)],
        ),
        out_shape=[jax.ShapeDtypeStruct((rows, units), BF16)] * 3
        + [jax.ShapeDtypeStruct((rows, half), BF16)] * 2,
        name="expert",
    )(core, ra, rb, ga, gb, w_gate, w_gate, w_up, w_up, w_down, w_down)


def weights_kernel(core, ra, rb, ga, gb, hidden, gback, uback, gate_out, up_out, down_out):
    step = pl.program_id(0)
    turn = pl.num_programs(0) // 2

    def write(r, g):
        gate_out[...] = dot(r[...], gback[...], 0, 0).astype(BF16)
        up_out[...] = dot(r[...], uback[...], 0, 0).astype(BF16)
        down_out[...] = dot(hidden[...], g[...], 0, 0).astype(BF16)

    @pl.when(step < turn)
    def _():
        write(ra, ga)

    @pl.when(step >= turn)
    def _():
        write(rb, gb)


def weight_grads(core, ra, rb, ga, gb, hidden, gback, uback):
    rows, half = ra.shape
    units = hidden.shape[1]
    chunk = min(half, 512)
    turn = half // chunk
    whole = lambda i, c: (0, 0)
    left = pl.BlockSpec((rows, chunk), lambda i, c: (0, jnp.minimum(i, turn - 1)))
    right = pl.BlockSpec((rows, chunk), lambda i, c: (0, jnp.maximum(i - turn, 0)))
    at = lambda i, c: jnp.where(i < turn, c[0] * turn + i, (1 - c[0]) * turn + i - turn)
    full = pl.BlockSpec((rows, units), whole)
    tall = pl.BlockSpec((None, chunk, units), lambda i, c: (0, at(i, c), 0))
    wide = pl.BlockSpec((None, units, chunk), lambda i, c: (0, 0, at(i, c)))
    return pl.pallas_call(
        weights_kernel,
        grid_spec=pltpu.PrefetchScalarGridSpec(
            num_scalar_prefetch=1,
            grid=(2 * turn,),
            in_specs=[left, right, left, right, full, full, full],
            out_specs=[tall, tall, wide],
        ),
        out_shape=[
            jax.ShapeDtypeStruct((1, 2 * half, units), BF16),
            jax.ShapeDtypeStruct((1, 2 * half, units), BF16),
            jax.ShapeDtypeStruct((1, units, 2 * half), BF16),
        ],
        name="weight_grads",
    )(core, ra, rb, ga, gb, hidden, gback, uback)


def combine_kernel(place, back, out):
    out[...] = dot(place[...], back[...], 0, 0).astype(BF16)


def combine(place, back):
    return pl.pallas_call(
        combine_kernel,
        out_shape=jax.ShapeDtypeStruct((place.shape[1], back.shape[1]), BF16),
        name="combine",
    )(place, back)


def decays(log_decay, head):
    span = log_decay.shape[-1]
    row = iota((span, span), 0)
    col = iota((span, span), 1)
    keep = row >= col
    lower = jnp.where(keep, 1.0, 0.0)
    own = log_decay[head : head + 1, :]
    down = jnp.sum(lower * own, axis=1, keepdims=True)
    across = jnp.sum(jnp.where(row <= col, 1.0, 0.0) * jnp.sum(
        jnp.where(row == col, own, 0.0), axis=1, keepdims=True), axis=0, keepdims=True)
    total = jnp.sum(own, axis=1, keepdims=True)
    table = jnp.where(keep, jnp.exp(jnp.where(keep, down - across, 0.0)), 0.0)
    return table, jnp.exp(down), jnp.exp(total - down), total


def mixed_kernel(q, k, v, log_decay, state, mixed, totals):
    heads, span, size = q.shape
    width = v.shape[2]
    scale = size**-0.5
    for h in range(heads):
        table, lead, _, total = decays(log_decay[...], h)
        scores = (dot(q[h], k[h], 1, 1) * (scale * table)).astype(BF16)
        out = dot(scores, v[h]) + lead * dot(q[h], state[h, 0].astype(BF16))
        mixed[:, h * width : (h + 1) * width] = out.astype(BF16)
        totals[h : h + 1, :] = jnp.broadcast_to(total, (1, totals.shape[1]))


def mixed_heads(q, k, v, log_decay, state):
    heads, span, _ = q.shape
    return pl.pallas_call(
        mixed_kernel,
        out_shape=[
            jax.ShapeDtypeStruct((span, heads * v.shape[2]), BF16),
            jax.ShapeDtypeStruct((heads, 128), F32),
        ],
        name="mixed_heads",
    )(q, k, v, log_decay, state)


def carry_kernel(core, ma, mb, wa, wb, q, log_decay, hg, carried, slices, *, groups):
    head = pl.program_id(0)
    h_grad = (dot(ma[...], wa[...]) + dot(mb[...], wb[...])).astype(BF16)
    hg[...] = h_grad
    span = log_decay.shape[-1]
    lower = jnp.where(iota((span, span), 0) >= iota((span, span), 1), 1.0, 0.0)
    lead = jnp.exp(jnp.sum(lower * log_decay[pl.ds(head, 1), :], axis=1, keepdims=True))
    carried[...] = dot((q[...].astype(F32) * lead).astype(BF16), h_grad, 0, 0).astype(BF16)

    @pl.when(head == 0)
    def _():
        size = slices.shape[2]
        turn = groups // 2
        for i in range(turn):
            slices[core[0] * turn + i] = ma[:, i * size : (i + 1) * size]
            slices[(1 - core[0]) * turn + i] = mb[:, i * size : (i + 1) * size]


def carry(core, ma, mb, w_out, q, log_decay, groups, value_size):
    span, half = ma.shape
    heads, _, size = q.shape
    whole = lambda h, c: (0, 0)
    by_head = lambda h, c: (h, 0, 0)
    return pl.pallas_call(
        functools.partial(carry_kernel, groups=groups),
        grid_spec=pltpu.PrefetchScalarGridSpec(
            num_scalar_prefetch=1,
            grid=(heads,),
            in_specs=[
                pl.BlockSpec((span, half), whole),
                pl.BlockSpec((span, half), whole),
                pl.BlockSpec((half, value_size), lambda h, c: (c[0], h)),
                pl.BlockSpec((half, value_size), lambda h, c: (1 - c[0], h)),
                pl.BlockSpec((None, span, size), by_head),
                pl.BlockSpec(log_decay.shape, whole),
            ],
            out_specs=[
                pl.BlockSpec((None, span, value_size), by_head),
                pl.BlockSpec((None, size, value_size), by_head),
                pl.BlockSpec((groups, span, 2 * half // groups), lambda h, c: (0, 0, 0)),
            ],
        ),
        out_shape=[
            jax.ShapeDtypeStruct((heads, span, value_size), BF16),
            jax.ShapeDtypeStruct((heads, size, value_size), BF16),
            jax.ShapeDtypeStruct((groups, span, 2 * half // groups), BF16),
        ],
        name="carry",
    )(core, ma, mb, w_out, w_out, q, log_decay)


def local_kernel(q, k, v, log_decay, state, hg, q_grad, k_part, v_part):
    heads, span, size = q.shape
    scale = size**-0.5
    for h in range(heads):
        table, lead, _, _ = decays(log_decay[...], h)
        scores = (dot(q[h], k[h], 1, 1) * (scale * table)).astype(BF16)
        back = (dot(hg[h], v[h], 1, 1) * table).astype(BF16)
        from_state = dot(hg[h], state[h, 0].astype(BF16), 1, 1)
        q_grad[h] = (scale * dot(back, k[h]) + lead * from_state).astype(BF16)
        k_part[h] = dot(back, q[h], 0, 0)
        v_part[h] = dot(scores, hg[h], 0, 0)


def local_grads(q, k, v, log_decay, state, hg):
    return pl.pallas_call(
        local_kernel,
        out_shape=[
            jax.ShapeDtypeStruct(q.shape, BF16),
            jax.ShapeDtypeStruct(k.shape, F32),
            jax.ShapeDtypeStruct(v.shape, F32),
        ],
        name="local_grads",
    )(q, k, v, log_decay, state, hg)


def final_kernel(k, v, log_decay, later, last, factor, k_part, v_part, k_grad, v_grad):
    heads, span, size = k.shape
    scale = size**-0.5
    for h in range(heads):
        _, _, trail, _ = decays(log_decay[...], h)
        state = (later[h] + factor[h : h + 1, 0:1] * last[h].astype(F32)).astype(BF16)
        k_grad[h] = (scale * (k_part[h] + trail * dot(v[h], state, 1, 1))).astype(BF16)
        v_grad[h] = (v_part[h] + (scale * trail) * dot(k[h], state)).astype(BF16)


def final_grads(k, v, log_decay, later, last, factor, k_part, v_part):
    return pl.pallas_call(
        final_kernel,
        out_shape=[jax.ShapeDtypeStruct(k.shape, BF16), jax.ShapeDtypeStruct(v.shape, BF16)],
        name="final_grads",
    )(k, v, log_decay, later, last, factor, k_part, v_part)


def project_kernel(order, x, y, out):
    part = dot(x[...], y[...], 0, 0)

    @pl.when(pl.program_id(0) == 0)
    def _():
        out[...] = part

    @pl.when(pl.program_id(0) > 0)
    def _():
        out[...] += part


def project(order, x, y):
    groups, span, size = x.shape
    width = y.shape[2]
    return pl.pallas_call(
        project_kernel,
        grid_spec=pltpu.PrefetchScalarGridSpec(
            num_scalar_prefetch=1,
            grid=(groups,),
            in_specs=[
                pl.BlockSpec((None, span, size), lambda i, o: (o[i], 0, 0)),
                pl.BlockSpec((None, span, width), lambda i, o: (i, 0, 0)),
            ],
            out_specs=pl.BlockSpec((size, width), lambda i, o: (0, 0)),
        ),
        out_shape=jax.ShapeDtypeStruct((size, width), F32),
        name="project",
    )(order, x, y)


def swap(a, axis, bit):
    count = lax.axis_size(axis)
    return lax.ppermute(a, axis, [(i, i ^ bit) for i in range(count)])


def bits_of(count):
    return [1 << i for i in range(count.bit_length() - 1)]


def join_factors(totals, place, count):
    spans = jnp.arange(count)
    rows = []
    for bit in bits_of(count):
        start = (place // bit) * bit
        rows.append((spans > place) & (spans < start + bit))
        rows.append((spans >= start) & (spans < start + bit))
        other = start ^ bit
        rows.append((spans >= other) & (spans < other + bit))
    sums = jnp.dot(jnp.stack(rows).astype(F32), totals, precision=EXACT)
    scales = jnp.exp(sums)
    out = []
    for n, bit in enumerate(bits_of(count)):
        low = (place & bit) == 0
        one = jnp.ones_like(scales[0])
        out.append((
            jnp.where(low, scales[3 * n], 0.0),
            jnp.where(low, one, scales[3 * n + 2]),
            jnp.where(low, scales[3 * n + 1], one),
        ))
    return out


def body(
    moe_input,
    out_grad,
    routes,
    route_weight,
    w_gate,
    w_up,
    w_down,
    w_out,
    query_heads,
    key_heads,
    value_heads,
    log_decay,
    state_in,
):
    tokens, width = moe_input.shape
    half = width // 2
    sp = lax.axis_size("sp")
    tp = lax.axis_size("tp")
    place = lax.axis_index("sp")
    core = lax.axis_index("tp") & 1
    core_at = core.reshape(1).astype(jnp.int32)
    experts = w_gate.shape[0] * sp
    cap = 5 * tokens * routes.shape[1] // (4 * experts)
    value_size = value_heads.shape[-1]

    rows, grads, picked = dispatch(
        core_at, routes, route_weight, moe_input, out_grad, experts, cap
    )
    mixed, totals = mixed_heads(query_heads, key_heads, value_heads, log_decay, state_in)
    span_totals = lax.all_gather(totals[:, 0], "sp")
    factors = join_factors(span_totals, place, sp)

    def exchange(a):
        a = a.reshape(experts, cap, half)
        return lax.all_to_all(a, "sp", split_axis=0, concat_axis=0, tiled=True).reshape(-1, half)

    rows_a = exchange(rows)
    grads_a = exchange(grads)
    rows_b = swap(rows_a, "tp", 1)
    grads_b = swap(grads_a, "tp", 1)

    hidden, gate_back, up_back, part_a, part_b = expert_back(
        core_at, rows_a, rows_b, grads_a, grads_b, w_gate, w_up, w_down
    )
    part = (part_a.astype(F32) + swap(part_b, "tp", 1).astype(F32)).astype(BF16)
    gate_grad, up_grad, down_grad = weight_grads(
        core_at, rows_a, rows_b, grads_a, grads_b, hidden, gate_back, up_back
    )

    mixed, rows_b2 = lax.optimization_barrier((mixed, rows_b))
    gathered = mixed[None]
    for bit in reversed(bits_of(sp)):
        gathered = jnp.concatenate([gathered, swap(gathered, "sp", bit)], axis=0)

    returned = exchange(part)
    token_part = combine(picked, returned)
    for bit in bits_of(tp)[1:]:
        token_part = token_part.astype(F32) + swap(token_part, "tp", bit).astype(F32)
        if bit * 2 < tp:
            token_part = token_part.astype(BF16)
    own_grad = lax.dynamic_slice_in_dim(out_grad, core * half, half, axis=1)
    mixed_a = (own_grad.astype(F32) + token_part.astype(F32)).astype(BF16)
    mixed_b = swap(mixed_a, "tp", 1)

    head_grad, carried, slices = carry(
        core_at, mixed_a, mixed_b, w_out, query_heads, log_decay, sp, value_size
    )
    q_grad, k_part, v_part = local_grads(
        query_heads, key_heads, value_heads, log_decay, state_in, head_grad
    )
    later = jnp.zeros(carried.shape, F32)
    whole = carried
    for n, bit in enumerate(bits_of(sp)):
        came = swap(whole, "sp", bit)
        f_later, f_own, f_came = factors[n]
        if bit * 2 < sp:
            later = later + f_later[:, None, None] * came.astype(F32)
            whole = (
                f_own[:, None, None] * whole.astype(F32) + f_came[:, None, None] * came.astype(F32)
            ).astype(BF16)
    k_grad, v_grad = final_grads(
        key_heads, value_heads, log_decay, later, came,
        jnp.broadcast_to(factors[-1][0][:, None], (factors[-1][0].shape[0], 128)),
        k_part, v_part,
    )
    slices = lax.all_to_all(slices, "sp", split_axis=0, concat_axis=0, tiled=True)
    offsets = [0]
    for bit in reversed(bits_of(sp)):
        offsets = offsets + [o ^ bit for o in offsets]
    order = (place ^ jnp.array(offsets, jnp.int32)).astype(jnp.int32)
    out_proj_grad = project(order, slices, gathered)
    return gate_grad, up_grad, down_grad, out_proj_grad, q_grad, k_grad, v_grad


def solution(mesh):
    return jax.shard_map(
        body,
        mesh=mesh,
        in_specs=(
            P("sp", None),
            P("sp", None),
            P("sp", None),
            P("sp", None),
            P("sp", None, "tp"),
            P("sp", None, "tp"),
            P("sp", "tp", None),
            P(None, "tp"),
            P("tp", "sp", None),
            P("tp", "sp", None),
            P("tp", "sp", None),
            P("tp", "sp"),
            P("tp", "sp", None, None),
        ),
        out_specs=(
            P("sp", None, "tp"),
            P("sp", None, "tp"),
            P("sp", "tp", None),
            P("sp", "tp"),
            P("tp", "sp", None),
            P("tp", "sp", None),
            P("tp", "sp", None),
        ),
        check_vma=False,
    )
```

```python
import functools

import jax
import jax.numpy as jnp
from jax import lax
from jax.experimental import pallas as pl
from jax.experimental.pallas import tpu as pltpu
from jax.sharding import PartitionSpec as P

F32 = jnp.float32
BF16 = jnp.bfloat16
EXACT = lax.Precision.HIGHEST


def dot(a, b, ca=1, cb=0, precision=None):
    return lax.dot_general(
        a, b, (((ca,), (cb,)), ((), ())), preferred_element_type=F32, precision=precision
    )


def iota(shape, axis):
    return lax.broadcasted_iota(jnp.int32, shape, axis)


def limit(mib):
    return pltpu.CompilerParams(vmem_limit_bytes=mib << 20)


def dispatch_kernel(core, routes, weight, x, g, out, place, *, experts, cap):
    tokens, half = x.shape
    slots = experts * cap
    expert = iota((experts, tokens), 0)
    first = routes[0:1, :] == expert
    second = routes[1:2, :] == expert
    named = jnp.where(first | second, 1.0, 0.0)
    share = jnp.where(first, weight[0:1, :], 0.0) + jnp.where(second, weight[1:2, :], 0.0)
    before = jnp.where(iota((tokens, tokens), 0) < iota((tokens, tokens), 1), 1.0, 0.0)
    rank_t = dot(named.astype(BF16), before.astype(BF16))
    rank_t = jnp.where(named > 0.5, rank_t, 2.0 * cap)
    slot = iota((slots, experts), 0)
    base = iota((slots, experts), 1) * cap
    owner = (slot >= base) & (slot < base + cap)
    owner_f = jnp.where(owner, 1.0, 0.0)
    number = jnp.sum(jnp.where(owner, slot - base, 0).astype(F32), axis=1, keepdims=True)
    rank = dot(owner_f.astype(BF16), rank_t.astype(BF16))
    hit = rank == number
    picked = jnp.where(hit, 1.0, 0.0).astype(BF16)
    share_slot = jnp.sum(
        jnp.where(hit, dot(owner_f, share, precision=EXACT), 0.0), axis=1, keepdims=True
    )
    place[...] = picked
    out[:, :half] = dot(picked, x[...]).astype(BF16)
    out[:, half:] = (share_slot * dot(picked, g[...])).astype(BF16)


def dispatch(core, routes, weight, x, g, experts, cap):
    tokens, width = x.shape
    half = width // 2
    slots = experts * cap
    whole = lambda i, c: (0, 0)
    return pl.pallas_call(
        functools.partial(dispatch_kernel, experts=experts, cap=cap),
        grid_spec=pltpu.PrefetchScalarGridSpec(
            num_scalar_prefetch=1,
            grid=(1,),
            in_specs=[
                pl.BlockSpec(routes.shape, whole),
                pl.BlockSpec(weight.shape, whole),
                pl.BlockSpec((tokens, half), lambda i, c: (0, c[0])),
                pl.BlockSpec((tokens, half), lambda i, c: (0, c[0])),
            ],
            out_specs=[
                pl.BlockSpec((slots, width), whole),
                pl.BlockSpec((slots, tokens), whole),
            ],
        ),
        out_shape=[
            jax.ShapeDtypeStruct((slots, width), BF16),
            jax.ShapeDtypeStruct((slots, tokens), BF16),
        ],
        compiler_params=limit(16),
        name="dispatch",
    )(core, routes, weight, x, g)


def expert_kernel(
    core, ra, rb, ga, gb, wga, wgb, wua, wub, wda, wdb, hidden, gback, uback, pb, accb
):
    step = pl.program_id(0)
    gate = dot(ra[...], wga[...]) + dot(rb[...], wgb[...])
    up = dot(ra[...], wua[...]) + dot(rb[...], wub[...])
    back = dot(ga[...], wda[...], 1, 1) + dot(gb[...], wdb[...], 1, 1)
    sig = 1.0 / (1.0 + jnp.exp(-gate))
    active = gate * sig
    hidden[...] = (active * up).astype(BF16)
    gb_v = (back * up * (sig * (1.0 + gate * (1.0 - sig)))).astype(BF16)
    ub_v = (back * active).astype(BF16)
    gback[...] = gb_v
    uback[...] = ub_v
    part_b = dot(gb_v, wgb[...], 1, 1) + dot(ub_v, wub[...], 1, 1)
    last = pl.num_programs(0) - 1

    @pl.when((step == 0) & (last > 0))
    def _():
        accb[...] = part_b

    @pl.when((step > 0) & (step < last))
    def _():
        accb[...] += part_b

    @pl.when((step == last) & (last > 0))
    def _():
        pb[...] = (accb[...] + part_b).astype(BF16)

    @pl.when((step == last) & (last == 0))
    def _():
        pb[...] = part_b.astype(BF16)


def expert_back(core, own, other, w_gate, w_up, w_down):
    rows, width = own.shape
    half = width // 2
    units = w_gate.shape[2]
    chunk = min(units, 256)
    left = pl.BlockSpec((rows, half), lambda f, c: (0, 0))
    right = pl.BlockSpec((rows, half), lambda f, c: (0, 1))
    near = pl.BlockSpec((None, half, chunk), lambda f, c: (0, c[0], f))
    far = pl.BlockSpec((None, half, chunk), lambda f, c: (0, 1 - c[0], f))
    near_d = pl.BlockSpec((None, chunk, half), lambda f, c: (0, f, c[0]))
    far_d = pl.BlockSpec((None, chunk, half), lambda f, c: (0, f, 1 - c[0]))
    part = pl.BlockSpec((rows, chunk), lambda f, c: (0, f))
    return pl.pallas_call(
        expert_kernel,
        grid_spec=pltpu.PrefetchScalarGridSpec(
            num_scalar_prefetch=1,
            grid=(units // chunk,),
            in_specs=[left, left, right, right, near, far, near, far, near_d, far_d],
            out_specs=[part, part, part, left],
            scratch_shapes=[pltpu.VMEM((rows, half), F32)],
        ),
        out_shape=[jax.ShapeDtypeStruct((rows, units), BF16)] * 3
        + [jax.ShapeDtypeStruct((rows, half), BF16)],
        compiler_params=limit(28),
        name="expert",
    )(core, own, other, own, other, w_gate, w_gate, w_up, w_up, w_down, w_down)


def partial_kernel(core, gback, uback, wg, wu, out):
    out[...] = (dot(gback[...], wg[...], 1, 1) + dot(uback[...], wu[...], 1, 1)).astype(BF16)


def expert_part(core, gback, uback, w_gate, w_up):
    rows, units = gback.shape
    half = w_gate.shape[1] // 2
    chunk = half // 2
    full = pl.BlockSpec((rows, units), lambda i, c: (0, 0))
    near = pl.BlockSpec((None, chunk, units), lambda i, c: (0, 2 * c[0] + i, 0))
    return pl.pallas_call(
        partial_kernel,
        grid_spec=pltpu.PrefetchScalarGridSpec(
            num_scalar_prefetch=1,
            grid=(2,),
            in_specs=[full, full, near, near],
            out_specs=pl.BlockSpec((rows, chunk), lambda i, c: (0, i)),
        ),
        out_shape=jax.ShapeDtypeStruct((rows, half), BF16),
        compiler_params=limit(12),
        name="expert_part",
    )(core, gback, uback, w_gate, w_up)


def weights_kernel(core, ra, rb, ga, gb, hidden, gback, uback, gate_out, up_out, down_out):
    step = pl.program_id(0)
    turn = pl.num_programs(0) // 2

    def write(r, g):
        gate_out[...] = dot(r[...], gback[...], 0, 0).astype(BF16)
        up_out[...] = dot(r[...], uback[...], 0, 0).astype(BF16)
        down_out[...] = dot(hidden[...], g[...], 0, 0).astype(BF16)

    @pl.when(step < turn)
    def _():
        write(ra, ga)

    @pl.when(step >= turn)
    def _():
        write(rb, gb)


def weight_grads(core, own, other, hidden, gback, uback):
    rows, width = own.shape
    half = width // 2
    units = hidden.shape[1]
    chunk = min(half, 512)
    turn = half // chunk
    near = lambda i: jnp.minimum(i, turn - 1)
    far = lambda i: jnp.maximum(i - turn, 0)
    at = lambda i, c: jnp.where(i < turn, c[0] * turn + i, (1 - c[0]) * turn + i - turn)
    full = pl.BlockSpec((rows, units), lambda i, c: (0, 0))
    tall = pl.BlockSpec((None, chunk, units), lambda i, c: (0, at(i, c), 0))
    wide = pl.BlockSpec((None, units, chunk), lambda i, c: (0, 0, at(i, c)))
    return pl.pallas_call(
        weights_kernel,
        grid_spec=pltpu.PrefetchScalarGridSpec(
            num_scalar_prefetch=1,
            grid=(2 * turn,),
            in_specs=[
                pl.BlockSpec((rows, chunk), lambda i, c: (0, near(i))),
                pl.BlockSpec((rows, chunk), lambda i, c: (0, far(i))),
                pl.BlockSpec((rows, chunk), lambda i, c: (0, turn + near(i))),
                pl.BlockSpec((rows, chunk), lambda i, c: (0, turn + far(i))),
                full, full, full,
            ],
            out_specs=[tall, tall, wide],
        ),
        out_shape=[
            jax.ShapeDtypeStruct((1, width, units), BF16),
            jax.ShapeDtypeStruct((1, width, units), BF16),
            jax.ShapeDtypeStruct((1, units, width), BF16),
        ],
        compiler_params=limit(20),
        name="weight_grads",
    )(core, own, other, own, other, hidden, gback, uback)


def combine_kernel(place, back, out):
    out[...] = dot(place[...], back[...], 0, 0).astype(BF16)


def combine(place, back):
    return pl.pallas_call(
        combine_kernel,
        out_shape=jax.ShapeDtypeStruct((place.shape[1], back.shape[1]), BF16),
        compiler_params=limit(8),
        name="combine",
    )(place, back)


def decays(log_decay, head):
    span = log_decay.shape[-1]
    row = iota((span, span), 0)
    col = iota((span, span), 1)
    keep = row >= col
    lower = jnp.where(keep, 1.0, 0.0)
    own = log_decay[head : head + 1, :]
    down = jnp.sum(lower * own, axis=1, keepdims=True)
    across = jnp.sum(jnp.where(row <= col, 1.0, 0.0) * jnp.sum(
        jnp.where(row == col, own, 0.0), axis=1, keepdims=True), axis=0, keepdims=True)
    total = jnp.sum(own, axis=1, keepdims=True)
    table = jnp.where(keep, jnp.exp(jnp.where(keep, down - across, 0.0)), 0.0)
    return table, jnp.exp(down), jnp.exp(total - down), total


def mixed_kernel(q, k, v, log_decay, state, mixed):
    heads, span, size = q.shape
    width = v.shape[2]
    scale = size**-0.5
    for h in range(heads):
        table, lead, _, _ = decays(log_decay[...], h)
        scores = (dot(q[h], k[h], 1, 1) * (scale * table)).astype(BF16)
        out = dot(scores, v[h]) + lead * dot(q[h], state[h, 0].astype(BF16))
        mixed[:, h * width : (h + 1) * width] = out.astype(BF16)


def mixed_heads(q, k, v, log_decay, state):
    heads, span, _ = q.shape
    return pl.pallas_call(
        mixed_kernel,
        out_shape=jax.ShapeDtypeStruct((span, heads * v.shape[2]), BF16),
        compiler_params=limit(8),
        name="mixed_heads",
    )(q, k, v, log_decay, state)


PIECES = 16


def pieces(decay, shape):
    row = iota(shape, 0)
    high = decay.astype(BF16).astype(F32)
    rest = decay - high
    middle = rest.astype(BF16).astype(F32)
    low = rest - middle
    return jnp.where(row == 0, high, jnp.where(row == 1, middle, jnp.where(row == 2, low, 0.0)))


def put_message(ref, h, body, decay):
    size = body.shape[0]
    ref[h, :size, :] = body.astype(BF16)
    ref[h, size:, :] = pieces(decay, (PIECES, body.shape[1])).astype(BF16)


def get_message(ref, h):
    size = ref.shape[1] - PIECES
    decay = jnp.sum(ref[h, size:, :].astype(F32), axis=0, keepdims=True)[:, 0:1]
    return ref[h, :size, :].astype(F32), decay


def carry_kernel(at, ma, mb, wa, wb, q, log_decay, hg, keep, send, slices, *, groups):
    head = pl.program_id(0)
    h_grad = (dot(ma[...], wa[...]) + dot(mb[...], wb[...])).astype(BF16)
    hg[...] = h_grad
    span = log_decay.shape[-1]
    own = log_decay[pl.ds(head, 1), :]
    lower = jnp.where(iota((span, span), 0) >= iota((span, span), 1), 1.0, 0.0)
    lead = jnp.exp(jnp.sum(lower * own, axis=1, keepdims=True))
    total = jnp.exp(jnp.sum(own, axis=1, keepdims=True))
    part = dot((q[...].astype(F32) * lead).astype(BF16), h_grad, 0, 0)
    half = part.shape[1] // 2
    upper = (at[1] & 1) == 1
    put_message(keep, 0, jnp.where(upper, part[:, half:], part[:, :half]), total)
    put_message(send, 0, jnp.where(upper, part[:, :half], part[:, half:]), total)

    @pl.when(head == 0)
    def _():
        size = slices.shape[2]
        turn = groups // 2
        for i in range(turn):
            slices[at[0] * turn + i] = ma[:, i * size : (i + 1) * size]
            slices[(1 - at[0]) * turn + i] = mb[:, i * size : (i + 1) * size]


def carry(at, ma, mb, w_out, q, log_decay, groups, value_size):
    span, half = ma.shape
    heads, _, size = q.shape
    whole = lambda h, c: (0, 0)
    by_head = lambda h, c: (h, 0, 0)
    message = (size + PIECES, value_size // 2)
    return pl.pallas_call(
        functools.partial(carry_kernel, groups=groups),
        grid_spec=pltpu.PrefetchScalarGridSpec(
            num_scalar_prefetch=1,
            grid=(heads,),
            in_specs=[
                pl.BlockSpec((span, half), whole),
                pl.BlockSpec((span, half), whole),
                pl.BlockSpec((half, value_size), lambda h, c: (c[0], h)),
                pl.BlockSpec((half, value_size), lambda h, c: (1 - c[0], h)),
                pl.BlockSpec((None, span, size), by_head),
                pl.BlockSpec(log_decay.shape, whole),
            ],
            out_specs=[
                pl.BlockSpec((None, span, value_size), by_head),
                pl.BlockSpec((1,) + message, by_head),
                pl.BlockSpec((1,) + message, by_head),
                pl.BlockSpec((groups, span, 2 * half // groups), lambda h, c: (0, 0, 0)),
            ],
        ),
        out_shape=[
            jax.ShapeDtypeStruct((heads, span, value_size), BF16),
            jax.ShapeDtypeStruct((heads,) + message, BF16),
            jax.ShapeDtypeStruct((heads,) + message, BF16),
            jax.ShapeDtypeStruct((groups, span, 2 * half // groups), BF16),
        ],
        compiler_params=limit(12),
        name="carry",
    )(at, ma, mb, w_out, w_out, q, log_decay)


def pair_kernel(at, keep, came, out):
    upper = (at[1] & 1) == 1
    for h in range(keep.shape[0]):
        mine, mine_decay = get_message(keep, h)
        theirs, their_decay = get_message(came, h)
        first = jnp.where(upper, theirs, mine)
        second = jnp.where(upper, mine, theirs)
        decay = jnp.where(upper, their_decay, mine_decay)
        put_message(out, h, first + decay * second, mine_decay * their_decay)


def join_kernel(at, group, came, later, reach, out, later_out, reach_out, *, bit):
    upper = (at[1] & bit) != 0
    for h in range(group.shape[0]):
        mine, mine_decay = get_message(group, h)
        theirs, their_decay = get_message(came, h)
        first = jnp.where(upper, theirs, mine)
        second = jnp.where(upper, mine, theirs)
        decay = jnp.where(upper, their_decay, mine_decay)
        put_message(out, h, first + decay * second, mine_decay * their_decay)
        old = reach[h : h + 1, :]
        later_out[h] = later[h] + jnp.where(upper, 0.0, old[:, 0:1]) * theirs
        reach_out[h : h + 1, :] = old * jnp.where(upper, 1.0, their_decay)


def close_kernel(at, came, later, reach, keep, first_came, own, send, *, bit):
    upper = (at[1] & bit) != 0
    right = (at[1] & 1) == 1
    for h in range(keep.shape[0]):
        theirs, _ = get_message(came, h)
        after = later[h] + jnp.where(upper, 0.0, reach[h : h + 1, 0:1]) * theirs
        mine, mine_decay = get_message(keep, h)
        pair, pair_decay = get_message(first_came, h)
        second = jnp.where(right, mine, pair)
        decay = jnp.where(right, mine_decay, pair_decay)
        through = second + decay * after
        own[h] = jnp.where(right, after, through).astype(BF16)
        send[h] = jnp.where(right, through, after).astype(BF16)


def small(kernel, name, outs, at, *operands):
    spec = pl.BlockSpec(memory_space=pltpu.VMEM)
    return pl.pallas_call(
        kernel,
        in_specs=[pl.BlockSpec(memory_space=pltpu.SMEM)] + [spec] * len(operands),
        out_shape=outs,
        compiler_params=limit(8),
        name=name,
    )(at, *operands)


def local_kernel(q, k, v, log_decay, state, hg, q_grad, k_part, v_part):
    heads, span, size = q.shape
    scale = size**-0.5
    for h in range(heads):
        table, lead, _, _ = decays(log_decay[...], h)
        scores = (dot(q[h], k[h], 1, 1) * (scale * table)).astype(BF16)
        back = (dot(hg[h], v[h], 1, 1) * table).astype(BF16)
        from_state = dot(hg[h], state[h, 0].astype(BF16), 1, 1)
        q_grad[h] = (scale * dot(back, k[h]) + lead * from_state).astype(BF16)
        k_part[h] = dot(back, q[h], 0, 0)
        v_part[h] = dot(scores, hg[h], 0, 0)


def local_grads(q, k, v, log_decay, state, hg):
    return pl.pallas_call(
        local_kernel,
        out_shape=[
            jax.ShapeDtypeStruct(q.shape, BF16),
            jax.ShapeDtypeStruct(k.shape, F32),
            jax.ShapeDtypeStruct(v.shape, F32),
        ],
        compiler_params=limit(12),
        name="local_grads",
    )(q, k, v, log_decay, state, hg)


def final_kernel(at, k, v, log_decay, own, came, k_part, v_part, k_grad, v_grad):
    heads, span, size = k.shape
    half = v.shape[2] // 2
    scale = size**-0.5
    right = (at[1] & 1) == 1
    for h in range(heads):
        _, _, trail, _ = decays(log_decay[...], h)
        low = jnp.where(right, came[h].astype(F32), own[h].astype(F32)).astype(BF16)
        high = jnp.where(right, own[h].astype(F32), came[h].astype(F32)).astype(BF16)
        back = dot(v[h, :, :half], low, 1, 1) + dot(v[h, :, half:], high, 1, 1)
        k_grad[h] = (scale * (k_part[h] + trail * back)).astype(BF16)
        strength = scale * trail
        v_grad[h, :, :half] = (v_part[h, :, :half] + strength * dot(k[h], low)).astype(BF16)
        v_grad[h, :, half:] = (v_part[h, :, half:] + strength * dot(k[h], high)).astype(BF16)


def project_kernel(order, x, ya, yb, out):
    turn = ya.shape[0]
    span, width = ya.shape[1], ya.shape[2]
    left = jnp.concatenate([x[order[i]] for i in range(turn)], axis=0)
    right = jnp.concatenate([x[order[turn + i]] for i in range(turn)], axis=0)
    out[...] = dot(left, ya[...].reshape(turn * span, width), 0, 0) + dot(
        right, yb[...].reshape(turn * span, width), 0, 0
    )


def project(order, x, ya, yb):
    groups, span, size = x.shape
    turn, _, width = ya.shape
    chunk = min(width, 512)
    return pl.pallas_call(
        project_kernel,
        grid_spec=pltpu.PrefetchScalarGridSpec(
            num_scalar_prefetch=1,
            grid=(width // chunk,),
            in_specs=[
                pl.BlockSpec((groups, span, size), lambda i, o: (0, 0, 0)),
                pl.BlockSpec((turn, span, chunk), lambda i, o: (0, 0, i)),
                pl.BlockSpec((turn, span, chunk), lambda i, o: (0, 0, i)),
            ],
            out_specs=pl.BlockSpec((size, chunk), lambda i, o: (0, i)),
        ),
        out_shape=jax.ShapeDtypeStruct((size, width), F32),
        compiler_params=limit(16),
        name="project",
    )(order, x, ya, yb)


def swap(a, axis, bit):
    count = lax.axis_size(axis)
    return lax.ppermute(a, axis, [(i, i ^ bit) for i in range(count)])


def bits_of(count):
    return [1 << i for i in range(count.bit_length() - 1)]


def body(
    moe_input,
    out_grad,
    routes,
    route_weight,
    w_gate,
    w_up,
    w_down,
    w_out,
    query_heads,
    key_heads,
    value_heads,
    log_decay,
    state_in,
):
    tokens, width = moe_input.shape
    half = width // 2
    sp = lax.axis_size("sp")
    tp = lax.axis_size("tp")
    place = lax.axis_index("sp").astype(jnp.int32)
    core = (lax.axis_index("tp") & 1).astype(jnp.int32)
    at = jnp.stack([core, place])
    experts = w_gate.shape[0] * sp
    cap = 5 * tokens * routes.shape[1] // (4 * experts)
    heads, _, size = query_heads.shape
    value_size = value_heads.shape[-1]

    def exchange(a):
        wide = a.shape[1]
        a = a.reshape(experts, cap, wide)
        return lax.all_to_all(a, "sp", split_axis=0, concat_axis=0, tiled=True).reshape(-1, wide)

    sent, picked = dispatch(at, routes.T, route_weight.T, moe_input, out_grad, experts, cap)
    own = exchange(sent)
    other = swap(own, "tp", 1)
    mixed = mixed_heads(query_heads, key_heads, value_heads, log_decay, state_in)
    mixed, _ = lax.optimization_barrier((mixed, own))

    hidden, gate_back, up_back, part_b = expert_back(at, own, other, w_gate, w_up, w_down)
    part_came = swap(part_b, "tp", 1)
    part_a = expert_part(at, gate_back, up_back, w_gate, w_up)
    part = (part_a.astype(F32) + part_came.astype(F32)).astype(BF16)
    gate_grad, up_grad, down_grad = weight_grads(at, own, other, hidden, gate_back, up_back)

    returned = exchange(part)

    gathered = mixed[None]
    offsets = [0]
    for bit in reversed(bits_of(sp)):
        came = swap(gathered, "sp", bit)
        if bit > 1:
            gathered = jnp.concatenate([gathered, came], axis=0)
        offsets = offsets + [o ^ bit for o in offsets]
    order = (place ^ jnp.array(offsets, jnp.int32)).astype(jnp.int32)

    token_part = combine(picked, returned)
    for bit in bits_of(tp)[1:]:
        token_part = token_part.astype(F32) + swap(token_part, "tp", bit).astype(F32)
        if bit * 2 < tp:
            token_part = token_part.astype(BF16)
    own_grad = lax.dynamic_slice_in_dim(out_grad, core * half, half, axis=1)
    mixed_a = (own_grad.astype(F32) + token_part.astype(F32)).astype(BF16)
    mixed_b = swap(mixed_a, "tp", 1)

    head_grad, keep, send, slices = carry(
        at, mixed_a, mixed_b, w_out, query_heads, log_decay, sp, value_size
    )
    first_came = swap(send, "sp", 1)
    q_grad, k_part, v_part = local_grads(
        query_heads, key_heads, value_heads, log_decay, state_in, head_grad
    )
    message = jax.ShapeDtypeStruct(keep.shape, BF16)
    state_shape = (heads, size, value_size // 2)
    group = small(pair_kernel, "pair", message, at, keep, first_came)
    later = jnp.zeros(state_shape, F32)
    reach = jnp.ones((heads, 128), F32)
    for bit in bits_of(sp)[1:]:
        came_state = swap(group, "sp", bit)
        if bit * 2 < sp:
            group, later, reach = small(
                functools.partial(join_kernel, bit=bit),
                "join",
                [message, jax.ShapeDtypeStruct(state_shape, F32),
                 jax.ShapeDtypeStruct((heads, 128), F32)],
                at, group, came_state, later, reach,
            )
    state_out = jax.ShapeDtypeStruct(state_shape, BF16)
    own_state, send_state = small(
        functools.partial(close_kernel, bit=bit),
        "close", [state_out, state_out], at, came_state, later, reach, keep, first_came,
    )
    other_state = swap(send_state, "sp", 1)
    k_grad, v_grad = small(
        final_kernel,
        "final",
        [jax.ShapeDtypeStruct(key_heads.shape, BF16), jax.ShapeDtypeStruct(value_heads.shape, BF16)],
        at, key_heads, value_heads, log_decay, own_state, other_state, k_part, v_part,
    )
    slices = lax.all_to_all(slices, "sp", split_axis=0, concat_axis=0, tiled=True)
    out_proj_grad = project(order, slices, gathered, came)
    return gate_grad, up_grad, down_grad, out_proj_grad, q_grad, k_grad, v_grad


def solution(mesh):
    return jax.shard_map(
        body,
        mesh=mesh,
        in_specs=(
            P("sp", None),
            P("sp", None),
            P("sp", None),
            P("sp", None),
            P("sp", None, "tp"),
            P("sp", None, "tp"),
            P("sp", "tp", None),
            P(None, "tp"),
            P("tp", "sp", None),
            P("tp", "sp", None),
            P("tp", "sp", None),
            P("tp", "sp"),
            P("tp", "sp", None, None),
        ),
        out_specs=(
            P("sp", None, "tp"),
            P("sp", None, "tp"),
            P("sp", "tp", None),
            P("sp", "tp"),
            P("tp", "sp", None),
            P("tp", "sp", None),
            P("tp", "sp", None),
        ),
        check_vma=False,
    )
```

```python
import functools

import jax
import jax.numpy as jnp
from jax import lax
from jax.experimental import pallas as pl
from jax.experimental.pallas import tpu as pltpu
from jax.sharding import PartitionSpec as P


F32 = jnp.float32
BF16 = jnp.bfloat16
EXACT = lax.Precision.HIGHEST


def dot(a, b, ca=1, cb=0, precision=None):
    return lax.dot_general(
        a, b, (((ca,), (cb,)), ((), ())), preferred_element_type=F32, precision=precision
    )


def iota(shape, axis):
    return lax.broadcasted_iota(jnp.int32, shape, axis)


def in_hbm(a):
    return pltpu.with_memory_space_constraint(a, pltpu.HBM)


def limit(mib):
    return pltpu.CompilerParams(vmem_limit_bytes=mib << 20)


def dispatch_kernel(core, routes, weight, x, g, out, place, *, experts, cap):
    tokens, half = x.shape
    slots = experts * cap
    expert = iota((experts, tokens), 0)
    first = routes[0:1, :] == expert
    second = routes[1:2, :] == expert
    named = jnp.where(first | second, 1.0, 0.0)
    share = jnp.where(first, weight[0:1, :], 0.0) + jnp.where(second, weight[1:2, :], 0.0)
    before = jnp.where(iota((tokens, tokens), 0) < iota((tokens, tokens), 1), 1.0, 0.0)
    rank_t = dot(named.astype(BF16), before.astype(BF16))
    rank_t = jnp.where(named > 0.5, rank_t, 2.0 * cap)
    slot = iota((slots, experts), 0)
    base = iota((slots, experts), 1) * cap
    owner = (slot >= base) & (slot < base + cap)
    owner_f = jnp.where(owner, 1.0, 0.0)
    number = jnp.sum(jnp.where(owner, slot - base, 0).astype(F32), axis=1, keepdims=True)
    rank = dot(owner_f.astype(BF16), rank_t.astype(BF16))
    hit = rank == number
    picked = jnp.where(hit, 1.0, 0.0).astype(BF16)
    share_slot = jnp.sum(
        jnp.where(hit, dot(owner_f, share, precision=EXACT), 0.0), axis=1, keepdims=True
    )
    place[...] = picked
    out[:, :half] = dot(picked, x[...]).astype(BF16)
    out[:, half:] = (share_slot * dot(picked, g[...])).astype(BF16)


def dispatch(core, routes, weight, x, g, experts, cap):
    tokens, width = x.shape
    half = width // 2
    slots = experts * cap
    whole = lambda i, c: (0, 0)
    return pl.pallas_call(
        functools.partial(dispatch_kernel, experts=experts, cap=cap),
        grid_spec=pltpu.PrefetchScalarGridSpec(
            num_scalar_prefetch=1,
            grid=(1,),
            in_specs=[
                pl.BlockSpec(routes.shape, whole),
                pl.BlockSpec(weight.shape, whole),
                pl.BlockSpec((tokens, half), lambda i, c: (0, c[0])),
                pl.BlockSpec((tokens, half), lambda i, c: (0, c[0])),
            ],
            out_specs=[
                pl.BlockSpec((slots, width), whole),
                pl.BlockSpec((slots, tokens), whole),
            ],
        ),
        out_shape=[
            jax.ShapeDtypeStruct((slots, width), BF16),
            pltpu.HBM((slots, tokens), BF16),
        ],
        compiler_params=limit(16),
        name="dispatch",
    )(core, in_hbm(routes), in_hbm(weight), in_hbm(x), in_hbm(g))


def expert_kernel(
    core, ra, rb, ga, gb, wga, wgb, wua, wub, wda, wdb, hidden, gback, uback, pb, accb
):
    step = pl.program_id(0)
    gate = dot(ra[...], wga[...]) + dot(rb[...], wgb[...])
    up = dot(ra[...], wua[...]) + dot(rb[...], wub[...])
    back = dot(ga[...], wda[...], 1, 1) + dot(gb[...], wdb[...], 1, 1)
    sig = 1.0 / (1.0 + jnp.exp(-gate))
    active = gate * sig
    hidden[...] = (active * up).astype(BF16)
    gb_v = (back * up * (sig * (1.0 + gate * (1.0 - sig)))).astype(BF16)
    ub_v = (back * active).astype(BF16)
    gback[...] = gb_v
    uback[...] = ub_v
    part_b = dot(gb_v, wgb[...], 1, 1) + dot(ub_v, wub[...], 1, 1)
    last = pl.num_programs(0) - 1

    @pl.when((step == 0) & (last > 0))
    def _():
        accb[...] = part_b

    @pl.when((step > 0) & (step < last))
    def _():
        accb[...] += part_b

    @pl.when((step == last) & (last > 0))
    def _():
        pb[...] = (accb[...] + part_b).astype(BF16)

    @pl.when((step == last) & (last == 0))
    def _():
        pb[...] = part_b.astype(BF16)


def expert_back(core, own, other, w_gate, w_up, w_down):
    rows, width = own.shape
    half = width // 2
    units = w_gate.shape[2]
    chunk = min(units, 256)
    left = pl.BlockSpec((rows, half), lambda f, c: (0, 0))
    right = pl.BlockSpec((rows, half), lambda f, c: (0, 1))
    near = pl.BlockSpec((None, half, chunk), lambda f, c: (0, c[0], f))
    far = pl.BlockSpec((None, half, chunk), lambda f, c: (0, 1 - c[0], f))
    near_d = pl.BlockSpec((None, chunk, half), lambda f, c: (0, f, c[0]))
    far_d = pl.BlockSpec((None, chunk, half), lambda f, c: (0, f, 1 - c[0]))
    part = pl.BlockSpec((rows, chunk), lambda f, c: (0, f))
    return pl.pallas_call(
        expert_kernel,
        grid_spec=pltpu.PrefetchScalarGridSpec(
            num_scalar_prefetch=1,
            grid=(units // chunk,),
            in_specs=[left, left, right, right, near, far, near, far, near_d, far_d],
            out_specs=[part, part, part, left],
            scratch_shapes=[pltpu.VMEM((rows, half), F32)],
        ),
        out_shape=[jax.ShapeDtypeStruct((rows, units), BF16)] * 3
        + [jax.ShapeDtypeStruct((rows, half), BF16)],
        compiler_params=limit(28),
        name="expert",
    )(core, own, other, own, other, w_gate, w_gate, *[in_hbm(w) for w in (w_up, w_up, w_down, w_down)])


def partial_kernel(core, gback, uback, wg, wu, out):
    out[...] = (dot(gback[...], wg[...], 1, 1) + dot(uback[...], wu[...], 1, 1)).astype(BF16)


def expert_part(core, gback, uback, w_gate, w_up):
    rows, units = gback.shape
    half = w_gate.shape[1] // 2
    chunk = half // 2
    full = pl.BlockSpec((rows, units), lambda i, c: (0, 0))
    near = pl.BlockSpec((None, chunk, units), lambda i, c: (0, 2 * c[0] + i, 0))
    return pl.pallas_call(
        partial_kernel,
        grid_spec=pltpu.PrefetchScalarGridSpec(
            num_scalar_prefetch=1,
            grid=(2,),
            in_specs=[full, full, near, near],
            out_specs=pl.BlockSpec((rows, chunk), lambda i, c: (0, i)),
        ),
        out_shape=jax.ShapeDtypeStruct((rows, half), BF16),
        compiler_params=limit(12),
        name="expert_part",
    )(core, gback, uback, w_gate, w_up)


def weights_kernel(core, ra, rb, ga, gb, hidden, gback, uback, gate_out, up_out, down_out):
    step = pl.program_id(0)
    turn = pl.num_programs(0) // 2

    def write(r, g):
        gate_out[...] = dot(r[...], gback[...], 0, 0).astype(BF16)
        up_out[...] = dot(r[...], uback[...], 0, 0).astype(BF16)
        down_out[...] = dot(hidden[...], g[...], 0, 0).astype(BF16)

    @pl.when(step < turn)
    def _():
        write(ra, ga)

    @pl.when(step >= turn)
    def _():
        write(rb, gb)


def weight_grads(core, own, other, hidden, gback, uback):
    rows, width = own.shape
    half = width // 2
    units = hidden.shape[1]
    chunk = min(half, 512)
    turn = half // chunk
    near = lambda i: jnp.minimum(i, turn - 1)
    far = lambda i: jnp.maximum(i - turn, 0)
    at = lambda i, c: jnp.where(i < turn, c[0] * turn + i, (1 - c[0]) * turn + i - turn)
    full = pl.BlockSpec((rows, units), lambda i, c: (0, 0))
    tall = pl.BlockSpec((None, chunk, units), lambda i, c: (0, at(i, c), 0))
    wide = pl.BlockSpec((None, units, chunk), lambda i, c: (0, 0, at(i, c)))
    return pl.pallas_call(
        weights_kernel,
        grid_spec=pltpu.PrefetchScalarGridSpec(
            num_scalar_prefetch=1,
            grid=(2 * turn,),
            in_specs=[
                pl.BlockSpec((rows, chunk), lambda i, c: (0, near(i))),
                pl.BlockSpec((rows, chunk), lambda i, c: (0, far(i))),
                pl.BlockSpec((rows, chunk), lambda i, c: (0, turn + near(i))),
                pl.BlockSpec((rows, chunk), lambda i, c: (0, turn + far(i))),
                full, full, full,
            ],
            out_specs=[tall, tall, wide],
        ),
        out_shape=[
            jax.ShapeDtypeStruct((1, width, units), BF16),
            jax.ShapeDtypeStruct((1, width, units), BF16),
            jax.ShapeDtypeStruct((1, units, width), BF16),
        ],
        compiler_params=limit(20),
        name="weight_grads",
    )(core, own, other, own, other, hidden, gback, uback)


def combine_kernel(place, back, out):
    out[...] = dot(place[...], back[...], 0, 0).astype(BF16)


def combine(place, back):
    return pl.pallas_call(
        combine_kernel,
        out_shape=jax.ShapeDtypeStruct((place.shape[1], back.shape[1]), BF16),
        compiler_params=limit(8),
        name="combine",
    )(place, back)


def decays(log_decay, head):
    span = log_decay.shape[-1]
    row = iota((span, span), 0)
    col = iota((span, span), 1)
    keep = row >= col
    lower = jnp.where(keep, 1.0, 0.0)
    own = log_decay[head : head + 1, :]
    down = jnp.sum(lower * own, axis=1, keepdims=True)
    across = jnp.sum(jnp.where(row <= col, 1.0, 0.0) * jnp.sum(
        jnp.where(row == col, own, 0.0), axis=1, keepdims=True), axis=0, keepdims=True)
    total = jnp.sum(own, axis=1, keepdims=True)
    table = jnp.where(keep, jnp.exp(jnp.where(keep, down - across, 0.0)), 0.0)
    return table, jnp.exp(down), jnp.exp(total - down), total


def mixed_kernel(q, k, v, log_decay, state, mixed):
    heads, _, size = q.shape
    width = v.shape[2]
    scale = size**-0.5
    for h in range(heads):
        table, lead, _, _ = decays(log_decay[...], h)
        scores = (dot(q[h], k[h], 1, 1) * (scale * table)).astype(BF16)
        out = dot(scores, v[h]) + lead * dot(q[h], state[h, 0].astype(BF16))
        mixed[:, h * width : (h + 1) * width] = out.astype(BF16)


def mixed_heads(q, k, v, log_decay, state):
    heads, span, _ = q.shape
    return pl.pallas_call(
        mixed_kernel,
        out_shape=jax.ShapeDtypeStruct((span, heads * v.shape[2]), BF16),
        compiler_params=limit(8),
        name="mixed_heads",
    )(q, k, v, log_decay, state)


PIECES = 16


def pieces(decay, shape):
    row = iota(shape, 0)
    high = decay.astype(BF16).astype(F32)
    rest = decay - high
    middle = rest.astype(BF16).astype(F32)
    low = rest - middle
    return jnp.where(row == 0, high, jnp.where(row == 1, middle, jnp.where(row == 2, low, 0.0)))


def put_message(ref, h, body, decay):
    size = body.shape[0]
    ref[h, :size, :] = body.astype(BF16)
    ref[h, size:, :] = pieces(decay, (PIECES, body.shape[1])).astype(BF16)


def get_message(ref, h):
    size = ref.shape[1] - PIECES
    decay = jnp.sum(ref[h, size:, :].astype(F32), axis=0, keepdims=True)[:, 0:1]
    return ref[h, :size, :].astype(F32), decay


def carry_kernel(at, ma, mb, wa, wb, q, log_decay, hg, keep, send, slices, *, groups):
    head = pl.program_id(0)
    h_grad = (dot(ma[...], wa[...]) + dot(mb[...], wb[...])).astype(BF16)
    hg[...] = h_grad
    span = log_decay.shape[-1]
    own = log_decay[pl.ds(head, 1), :]
    lower = jnp.where(iota((span, span), 0) >= iota((span, span), 1), 1.0, 0.0)
    lead = jnp.exp(jnp.sum(lower * own, axis=1, keepdims=True))
    total = jnp.exp(jnp.sum(own, axis=1, keepdims=True))
    part = dot((q[...].astype(F32) * lead).astype(BF16), h_grad, 0, 0)
    half = part.shape[1] // 2
    upper = (at[1] & 1) == 1
    put_message(keep, 0, jnp.where(upper, part[:, half:], part[:, :half]), total)
    put_message(send, 0, jnp.where(upper, part[:, :half], part[:, half:]), total)

    @pl.when(head == 0)
    def _():
        size = slices.shape[2]
        turn = groups // 2
        for i in range(turn):
            slices[at[0] * turn + i] = ma[:, i * size : (i + 1) * size]
            slices[(1 - at[0]) * turn + i] = mb[:, i * size : (i + 1) * size]


def carry(at, ma, mb, w_out, q, log_decay, groups, value_size):
    span, half = ma.shape
    heads, _, size = q.shape
    whole = lambda h, c: (0, 0)
    by_head = lambda h, c: (h, 0, 0)
    message = (size + PIECES, value_size // 2)
    return pl.pallas_call(
        functools.partial(carry_kernel, groups=groups),
        grid_spec=pltpu.PrefetchScalarGridSpec(
            num_scalar_prefetch=1,
            grid=(heads,),
            in_specs=[
                pl.BlockSpec((span, half), whole),
                pl.BlockSpec((span, half), whole),
                pl.BlockSpec((half, value_size), lambda h, c: (c[0], h)),
                pl.BlockSpec((half, value_size), lambda h, c: (1 - c[0], h)),
                pl.BlockSpec((None, span, size), by_head),
                pl.BlockSpec(log_decay.shape, whole),
            ],
            out_specs=[
                pl.BlockSpec((None, span, value_size), by_head),
                pl.BlockSpec((1,) + message, by_head),
                pl.BlockSpec((1,) + message, by_head),
                pl.BlockSpec((groups, span, 2 * half // groups), lambda h, c: (0, 0, 0)),
            ],
        ),
        out_shape=[
            pltpu.HBM((heads, span, value_size), BF16),
            pltpu.HBM((heads,) + message, BF16),
            jax.ShapeDtypeStruct((heads,) + message, BF16),
            pltpu.HBM((groups, span, 2 * half // groups), BF16),
        ],
        compiler_params=limit(12),
        name="carry",
    )(at, ma, mb, in_hbm(w_out), in_hbm(w_out), in_hbm(q), log_decay)


def pair_kernel(at, keep, came, out):
    upper = (at[1] & 1) == 1
    for h in range(keep.shape[0]):
        mine, mine_decay = get_message(keep, h)
        theirs, their_decay = get_message(came, h)
        first = jnp.where(upper, theirs, mine)
        second = jnp.where(upper, mine, theirs)
        decay = jnp.where(upper, their_decay, mine_decay)
        put_message(out, h, first + decay * second, mine_decay * their_decay)


def join_kernel(at, group, came, later, reach, out, later_out, reach_out, *, bit):
    upper = (at[1] & bit) != 0
    for h in range(group.shape[0]):
        mine, mine_decay = get_message(group, h)
        theirs, their_decay = get_message(came, h)
        first = jnp.where(upper, theirs, mine)
        second = jnp.where(upper, mine, theirs)
        decay = jnp.where(upper, their_decay, mine_decay)
        put_message(out, h, first + decay * second, mine_decay * their_decay)
        old = reach[h : h + 1, :]
        later_out[h] = later[h] + jnp.where(upper, 0.0, old[:, 0:1]) * theirs
        reach_out[h : h + 1, :] = old * jnp.where(upper, 1.0, their_decay)


def close_kernel(at, came, later, reach, keep, first_came, own, send, *, bit):
    upper = (at[1] & bit) != 0
    right = (at[1] & 1) == 1
    for h in range(keep.shape[0]):
        theirs, _ = get_message(came, h)
        after = later[h] + jnp.where(upper, 0.0, reach[h : h + 1, 0:1]) * theirs
        mine, mine_decay = get_message(keep, h)
        pair, pair_decay = get_message(first_came, h)
        second = jnp.where(right, mine, pair)
        decay = jnp.where(right, mine_decay, pair_decay)
        through = second + decay * after
        own[h] = jnp.where(right, after, through).astype(BF16)
        send[h] = jnp.where(right, through, after).astype(BF16)


def small(kernel, outs, at, *operands):
    spec = pl.BlockSpec(memory_space=pltpu.VMEM)
    return pl.pallas_call(
        kernel,
        in_specs=[pl.BlockSpec(memory_space=pltpu.SMEM)] + [spec] * len(operands),
        out_shape=outs,
        compiler_params=limit(8),
    )(at, *operands)


def local_kernel(q, k, v, log_decay, state, hg, q_grad, k_part, v_part):
    heads, _, size = q.shape
    scale = size**-0.5
    for h in range(heads):
        table, lead, _, _ = decays(log_decay[...], h)
        scores = (dot(q[h], k[h], 1, 1) * (scale * table)).astype(BF16)
        back = (dot(hg[h], v[h], 1, 1) * table).astype(BF16)
        from_state = dot(hg[h], state[h, 0].astype(BF16), 1, 1)
        q_grad[h] = (scale * dot(back, k[h]) + lead * from_state).astype(BF16)
        k_part[h] = dot(back, q[h], 0, 0)
        v_part[h] = dot(scores, hg[h], 0, 0)


def local_grads(q, k, v, log_decay, state, hg):
    return pl.pallas_call(
        local_kernel,
        out_shape=[
            jax.ShapeDtypeStruct(q.shape, BF16),
            jax.ShapeDtypeStruct(k.shape, F32),
            jax.ShapeDtypeStruct(v.shape, F32),
        ],
        compiler_params=limit(12),
        name="local_grads",
    )(q, k, v, log_decay, state, hg)


def final_kernel(at, k, v, log_decay, own, came, k_part, v_part, k_grad, v_grad):
    heads, _, size = k.shape
    half = v.shape[2] // 2
    scale = size**-0.5
    right = (at[1] & 1) == 1
    for h in range(heads):
        _, _, trail, _ = decays(log_decay[...], h)
        low = jnp.where(right, came[h].astype(F32), own[h].astype(F32)).astype(BF16)
        high = jnp.where(right, own[h].astype(F32), came[h].astype(F32)).astype(BF16)
        back = dot(v[h, :, :half], low, 1, 1) + dot(v[h, :, half:], high, 1, 1)
        k_grad[h] = (scale * (k_part[h] + trail * back)).astype(BF16)
        strength = scale * trail
        v_grad[h, :, :half] = (v_part[h, :, :half] + strength * dot(k[h], low)).astype(BF16)
        v_grad[h, :, half:] = (v_part[h, :, half:] + strength * dot(k[h], high)).astype(BF16)


def project_kernel(order, x, *refs):
    out = refs[-1]
    total, at = None, 0
    for y in refs[:-1]:
        blocks, span, width = y.shape
        rows = jnp.concatenate([x[order[at + i]] for i in range(blocks)], axis=0)
        part = dot(rows, y[...].reshape(blocks * span, width), 0, 0)
        total = part if total is None else total + part
        at += blocks
    out[...] = total


def project(order, x, parts):
    groups, span, size = x.shape
    width = parts[0].shape[2]
    chunk = min(width, 512)
    return pl.pallas_call(
        project_kernel,
        grid_spec=pltpu.PrefetchScalarGridSpec(
            num_scalar_prefetch=1,
            grid=(width // chunk,),
            in_specs=[pl.BlockSpec((groups, span, size), lambda i, o: (0, 0, 0))]
            + [pl.BlockSpec(y.shape[:2] + (chunk,), lambda i, o: (0, 0, i)) for y in parts],
            out_specs=pl.BlockSpec((size, chunk), lambda i, o: (0, i)),
        ),
        out_shape=jax.ShapeDtypeStruct((size, width), F32),
        compiler_params=limit(16),
        name="project",
    )(order, x, *parts)


def swap(a, axis, bit):
    count = lax.axis_size(axis)
    return lax.ppermute(a, axis, [(i, i ^ bit) for i in range(count)])


def bits_of(count):
    return [1 << i for i in range(count.bit_length() - 1)]


def step(
    moe_input,
    out_grad,
    routes,
    route_weight,
    w_gate,
    w_up,
    w_down,
    w_out,
    query_heads,
    key_heads,
    value_heads,
    log_decay,
    state_in,
):
    tokens, width = moe_input.shape
    half = width // 2
    sp = lax.axis_size("sp")
    tp = lax.axis_size("tp")
    place = lax.axis_index("sp").astype(jnp.int32)
    core = (lax.axis_index("tp") & 1).astype(jnp.int32)
    at = jnp.stack([core, place])
    experts = w_gate.shape[0] * sp
    cap = 5 * tokens * routes.shape[1] // (4 * experts)
    heads, _, size = query_heads.shape
    value_size = value_heads.shape[-1]

    def exchange(a):
        wide = a.shape[1]
        a = a.reshape(experts, cap, wide)
        return lax.all_to_all(a, "sp", split_axis=0, concat_axis=0, tiled=True).reshape(-1, wide)

    sent, picked = dispatch(at, routes.T, route_weight.T, moe_input, out_grad, experts, cap)
    own = exchange(sent)
    other = swap(own, "tp", 1)
    mixed = mixed_heads(query_heads, key_heads, value_heads, log_decay, state_in)
    hidden, gate_back, up_back, part_b = expert_back(at, own, other, w_gate, w_up, w_down)
    part_came = swap(part_b, "tp", 1)
    part_a = expert_part(at, gate_back, up_back, w_gate, w_up)
    part = (part_a.astype(F32) + part_came.astype(F32)).astype(BF16)
    returned = exchange(part)
    gate_grad, up_grad, down_grad = weight_grads(at, own, other, hidden, gate_back, up_back)

    blocks = mixed[None]
    parts, offsets = [], [0]
    for bit in reversed(bits_of(sp)):
        if not parts:
            parts = [jnp.concatenate([blocks, swap(blocks, "sp", bit)], axis=0)]
        else:
            came = []
            for piece in parts:
                came.append(swap(piece, "sp", bit))
            parts = parts + came
        offsets = offsets + [o ^ bit for o in offsets]
    order = (place ^ jnp.array(offsets, jnp.int32)).astype(jnp.int32)

    token_part = combine(picked, returned)
    for bit in bits_of(tp)[1:]:
        came = swap(token_part, "tp", bit)
        token_part = token_part.astype(F32) + came.astype(F32)
        if bit * 2 < tp:
            token_part = token_part.astype(BF16)
        else:
            own_grad = lax.dynamic_slice_in_dim(out_grad, core * half, half, axis=1)
            mixed_a = (own_grad.astype(F32) + token_part).astype(BF16)
    mixed_b = swap(mixed_a, "tp", 1)

    head_grad, keep, send, slices = carry(
        at, mixed_a, mixed_b, w_out, query_heads, log_decay, sp, value_size
    )
    first_came = swap(send, "sp", 1)
    q_grad, k_part, v_part = local_grads(
        query_heads, key_heads, value_heads, log_decay, state_in, head_grad
    )
    message = jax.ShapeDtypeStruct(keep.shape, BF16)
    state_shape = (heads, size, value_size // 2)
    group = small(pair_kernel, message, at, keep, first_came)
    later = jnp.zeros(state_shape, F32)
    reach = jnp.ones((heads, 128), F32)
    for bit in bits_of(sp)[1:]:
        came_state = swap(group, "sp", bit)
        if bit * 2 < sp:
            group, later, reach = small(
                functools.partial(join_kernel, bit=bit),
                [message, jax.ShapeDtypeStruct(state_shape, F32),
                 jax.ShapeDtypeStruct((heads, 128), F32)],
                at, group, came_state, later, reach,
            )
    state_out = jax.ShapeDtypeStruct(state_shape, BF16)
    own_state, send_state = small(
        functools.partial(close_kernel, bit=bit),
        [state_out, state_out], at, came_state, later, reach, keep, first_came,
    )
    other_state = swap(send_state, "sp", 1)
    slices = lax.all_to_all(slices, "sp", split_axis=0, concat_axis=0, tiled=True)
    out_proj_grad = project(order, slices, parts)
    k_grad, v_grad = small(
        final_kernel,
        [jax.ShapeDtypeStruct(key_heads.shape, BF16),
         jax.ShapeDtypeStruct(value_heads.shape, BF16)],
        at, key_heads, value_heads, log_decay, own_state, other_state, k_part, v_part,
    )
    return gate_grad, up_grad, down_grad, out_proj_grad, q_grad, k_grad, v_grad


def solution(mesh):
    return jax.shard_map(
        step,
        mesh=mesh,
        in_specs=(
            P("sp", None),
            P("sp", None),
            P("sp", None),
            P("sp", None),
            P("sp", None, "tp"),
            P("sp", None, "tp"),
            P("sp", "tp", None),
            P(None, "tp"),
            P("tp", "sp", None),
            P("tp", "sp", None),
            P("tp", "sp", None),
            P("tp", "sp"),
            P("tp", "sp", None, None),
        ),
        out_specs=(
            P("sp", None, "tp"),
            P("sp", None, "tp"),
            P("sp", "tp", None),
            P("sp", "tp"),
            P("tp", "sp", None),
            P("tp", "sp", None),
            P("tp", "sp", None),
        ),
        check_vma=False,
    )
```

```python
import functools

import jax
import jax.numpy as jnp
from jax import lax
from jax.experimental import pallas as pl
from jax.experimental.pallas import tpu as pltpu
from jax.sharding import PartitionSpec as P


F32 = jnp.float32
BF16 = jnp.bfloat16
EXACT = lax.Precision.HIGHEST


def dot(a, b, ca=1, cb=0, precision=None):
    return lax.dot_general(
        a, b, (((ca,), (cb,)), ((), ())), preferred_element_type=F32, precision=precision
    )


def iota(shape, axis):
    return lax.broadcasted_iota(jnp.int32, shape, axis)


def in_hbm(a):
    return pltpu.with_memory_space_constraint(a, pltpu.HBM)


def limit(mib):
    return pltpu.CompilerParams(vmem_limit_bytes=mib << 20)


def dispatch_kernel(at, routes, weight, x, g, place, *blocks, experts, cap):
    tokens, half = x.shape
    slots = experts * cap
    expert = iota((experts, tokens), 0)
    first = routes[0:1, :] == expert
    second = routes[1:2, :] == expert
    named = jnp.where(first | second, 1.0, 0.0)
    share = jnp.where(first, weight[0:1, :], 0.0) + jnp.where(second, weight[1:2, :], 0.0)
    before = jnp.where(iota((tokens, tokens), 0) < iota((tokens, tokens), 1), 1.0, 0.0)
    rank_t = dot(named.astype(BF16), before.astype(BF16))
    rank_t = jnp.where(named > 0.5, rank_t, 2.0 * cap)
    slot = iota((slots, experts), 0)
    base = (iota((slots, experts), 1) ^ at[1]) * cap
    owner = (slot >= base) & (slot < base + cap)
    owner_f = jnp.where(owner, 1.0, 0.0)
    number = jnp.sum(jnp.where(owner, slot - base, 0).astype(F32), axis=1, keepdims=True)
    hit = dot(owner_f.astype(BF16), rank_t.astype(BF16)) == number
    picked = jnp.where(hit, 1.0, 0.0).astype(BF16)
    share_slot = jnp.sum(
        jnp.where(hit, dot(owner_f, share, precision=EXACT), 0.0), axis=1, keepdims=True
    )
    place[...] = picked
    rows = dot(picked, x[...]).astype(BF16)
    grads = (share_slot * dot(picked, g[...])).astype(BF16)
    for n, block in enumerate(blocks):
        block[:, :half] = rows[n * cap : (n + 1) * cap]
        block[:, half:] = grads[n * cap : (n + 1) * cap]


def dispatch(at, routes, weight, x, g, experts, cap):
    tokens, width = x.shape
    half = width // 2
    slots = experts * cap
    whole = lambda i, c: (0, 0)
    mine = pl.BlockSpec((tokens, half), lambda i, c: (0, c[0]))
    return pl.pallas_call(
        functools.partial(dispatch_kernel, experts=experts, cap=cap),
        grid_spec=pltpu.PrefetchScalarGridSpec(
            num_scalar_prefetch=1,
            grid=(1,),
            in_specs=[
                pl.BlockSpec(routes.shape, whole), pl.BlockSpec(weight.shape, whole), mine, mine,
            ],
            out_specs=[pl.BlockSpec((slots, tokens), whole)]
            + [pl.BlockSpec((cap, width), whole)] * experts,
        ),
        out_shape=[pltpu.HBM((slots, tokens), BF16)]
        + [pltpu.HBM((cap, width), BF16)] * experts,
        compiler_params=limit(12),
        name="dispatch",
    )(at, in_hbm(routes), in_hbm(weight), in_hbm(x), in_hbm(g))


def gather_kernel(*refs):
    blocks, out, sems = refs[:-2], refs[-2], refs[-1]
    copies = [
        pltpu.make_async_copy(block, out.at[n], sems.at[n]) for n, block in enumerate(blocks)
    ]
    for each in copies:
        each.start()
    for each in copies:
        each.wait()


def gather(blocks):
    cap, width = blocks[0].shape
    out = pl.pallas_call(
        gather_kernel,
        in_specs=[pl.BlockSpec(memory_space=pltpu.HBM)] * len(blocks),
        out_specs=pl.BlockSpec(memory_space=pltpu.VMEM),
        out_shape=jax.ShapeDtypeStruct((len(blocks), cap, width), BF16),
        scratch_shapes=[pltpu.SemaphoreType.DMA((len(blocks),))],
        compiler_params=limit(4),
        name="gather",
    )(*[in_hbm(block) for block in blocks])
    return out.reshape(len(blocks) * cap, width)


def expert_kernel(
    core, ra, rb, ga, gb, wga, wgb, wua, wub, wda, wdb, hidden, gback, uback, pb, accb
):
    step = pl.program_id(0)
    gate = dot(ra[...], wga[...]) + dot(rb[...], wgb[...])
    up = dot(ra[...], wua[...]) + dot(rb[...], wub[...])
    back = dot(ga[...], wda[...], 1, 1) + dot(gb[...], wdb[...], 1, 1)
    sig = 1.0 / (1.0 + jnp.exp(-gate))
    active = gate * sig
    hidden[...] = (active * up).astype(BF16)
    gb_v = (back * up * (sig * (1.0 + gate * (1.0 - sig)))).astype(BF16)
    ub_v = (back * active).astype(BF16)
    gback[...] = gb_v
    uback[...] = ub_v
    part_b = dot(gb_v, wgb[...], 1, 1) + dot(ub_v, wub[...], 1, 1)
    last = pl.num_programs(0) - 1

    @pl.when((step == 0) & (last > 0))
    def _():
        accb[...] = part_b

    @pl.when((step > 0) & (step < last))
    def _():
        accb[...] += part_b

    @pl.when((step == last) & (last > 0))
    def _():
        pb[...] = (accb[...] + part_b).astype(BF16)

    @pl.when((step == last) & (last == 0))
    def _():
        pb[...] = part_b.astype(BF16)


def expert_back(core, own, other, w_gate, w_up, w_down):
    rows, width = own.shape
    half = width // 2
    units = w_gate.shape[2]
    chunk = min(units, 256)
    left = pl.BlockSpec((rows, half), lambda f, c: (0, 0))
    right = pl.BlockSpec((rows, half), lambda f, c: (0, 1))
    near = pl.BlockSpec((None, half, chunk), lambda f, c: (0, c[0], f))
    far = pl.BlockSpec((None, half, chunk), lambda f, c: (0, 1 - c[0], f))
    near_d = pl.BlockSpec((None, chunk, half), lambda f, c: (0, f, c[0]))
    far_d = pl.BlockSpec((None, chunk, half), lambda f, c: (0, f, 1 - c[0]))
    part = pl.BlockSpec((rows, chunk), lambda f, c: (0, f))
    return pl.pallas_call(
        expert_kernel,
        grid_spec=pltpu.PrefetchScalarGridSpec(
            num_scalar_prefetch=1,
            grid=(units // chunk,),
            in_specs=[left, left, right, right, near, far, near, far, near_d, far_d],
            out_specs=[part, part, part, left],
            scratch_shapes=[pltpu.VMEM((rows, half), F32)],
        ),
        out_shape=[jax.ShapeDtypeStruct((rows, units), BF16)] * 3
        + [jax.ShapeDtypeStruct((rows, half), BF16)],
        compiler_params=limit(28),
        name="expert",
    )(core, own, other, own, other, w_gate, w_gate, *[in_hbm(w) for w in (w_up, w_up, w_down, w_down)])


def partial_kernel(core, gback, uback, wg, wu, out):
    out[...] = (dot(gback[...], wg[...], 1, 1) + dot(uback[...], wu[...], 1, 1)).astype(BF16)


def expert_part(core, gback, uback, w_gate, w_up):
    rows, units = gback.shape
    half = w_gate.shape[1] // 2
    chunk = half // 2
    full = pl.BlockSpec((rows, units), lambda i, c: (0, 0))
    near = pl.BlockSpec((None, chunk, units), lambda i, c: (0, 2 * c[0] + i, 0))
    return pl.pallas_call(
        partial_kernel,
        grid_spec=pltpu.PrefetchScalarGridSpec(
            num_scalar_prefetch=1,
            grid=(2,),
            in_specs=[full, full, near, near],
            out_specs=pl.BlockSpec((rows, chunk), lambda i, c: (0, i)),
        ),
        out_shape=jax.ShapeDtypeStruct((rows, half), BF16),
        compiler_params=limit(12),
        name="expert_part",
    )(core, gback, uback, w_gate, w_up)


def add_blocks_kernel(at, a, b, *blocks):
    cap = blocks[0].shape[0]
    for n, block in enumerate(blocks):
        cut = slice(n * cap, (n + 1) * cap)
        block[...] = (a[cut, :].astype(F32) + b[cut, :].astype(F32)).astype(BF16)


def add_kernel(at, a, b, out):
    out[...] = (a[...].astype(F32) + b[...].astype(F32)).astype(out.dtype)


def weights_kernel(core, ra, rb, ga, gb, hidden, gback, uback, gate_out, up_out, down_out):
    step = pl.program_id(0)
    turn = pl.num_programs(0) // 2

    def write(r, g):
        gate_out[...] = dot(r[...], gback[...], 0, 0).astype(BF16)
        up_out[...] = dot(r[...], uback[...], 0, 0).astype(BF16)
        down_out[...] = dot(hidden[...], g[...], 0, 0).astype(BF16)

    @pl.when(step < turn)
    def _():
        write(ra, ga)

    @pl.when(step >= turn)
    def _():
        write(rb, gb)


def weight_grads(core, own, other, hidden, gback, uback):
    rows, width = own.shape
    half = width // 2
    units = hidden.shape[1]
    chunk = min(half, 512)
    turn = half // chunk
    near = lambda i: jnp.minimum(i, turn - 1)
    far = lambda i: jnp.maximum(i - turn, 0)
    at = lambda i, c: jnp.where(i < turn, c[0] * turn + i, (1 - c[0]) * turn + i - turn)
    full = pl.BlockSpec((rows, units), lambda i, c: (0, 0))
    tall = pl.BlockSpec((None, chunk, units), lambda i, c: (0, at(i, c), 0))
    wide = pl.BlockSpec((None, units, chunk), lambda i, c: (0, 0, at(i, c)))
    return pl.pallas_call(
        weights_kernel,
        grid_spec=pltpu.PrefetchScalarGridSpec(
            num_scalar_prefetch=1,
            grid=(2 * turn,),
            in_specs=[
                pl.BlockSpec((rows, chunk), lambda i, c: (0, near(i))),
                pl.BlockSpec((rows, chunk), lambda i, c: (0, far(i))),
                pl.BlockSpec((rows, chunk), lambda i, c: (0, turn + near(i))),
                pl.BlockSpec((rows, chunk), lambda i, c: (0, turn + far(i))),
                full, full, full,
            ],
            out_specs=[tall, tall, wide],
        ),
        out_shape=[
            jax.ShapeDtypeStruct((1, width, units), BF16),
            jax.ShapeDtypeStruct((1, width, units), BF16),
            jax.ShapeDtypeStruct((1, units, width), BF16),
        ],
        compiler_params=limit(20),
        name="weight_grads",
    )(core, own, other, own, other, hidden, gback, uback)


def combine_kernel(at, place, *refs):
    blocks, out = refs[:-1], refs[-1]
    cap = blocks[0].shape[0]
    total = None
    for n, block in enumerate(blocks):
        part = dot(place[n * cap : (n + 1) * cap, :], block[...], 0, 0)
        total = part if total is None else total + part
    out[...] = total.astype(BF16)


def base_kernel(at, g, part, wo, out, near, sem):
    half = part.shape[1]
    begin = pl.multiple_of(at[0] * half, half)
    copy = pltpu.make_async_copy(wo.at[pl.ds(begin, half), :], near, sem)
    copy.start()
    out[...] = g[...].astype(F32) + part[...].astype(F32)
    copy.wait()


def base_sum(at, g, part, w_out):
    tokens, half = part.shape
    whole = lambda i, c: (0, 0)
    near = (half, w_out.shape[1])
    return pl.pallas_call(
        base_kernel,
        grid_spec=pltpu.PrefetchScalarGridSpec(
            num_scalar_prefetch=1,
            grid=(1,),
            in_specs=[
                pl.BlockSpec((tokens, half), lambda i, c: (0, c[0])),
                pl.BlockSpec((tokens, half), whole),
                pl.BlockSpec(memory_space=pltpu.HBM),
            ],
            out_specs=[pl.BlockSpec((tokens, half), whole), pl.BlockSpec(memory_space=pltpu.VMEM)],
            scratch_shapes=[pltpu.SemaphoreType.DMA],
        ),
        out_shape=[jax.ShapeDtypeStruct((tokens, half), F32), pltpu.VMEM(near, BF16)],
        compiler_params=limit(4),
        name="base",
    )(at, in_hbm(g), part, in_hbm(w_out))


def decays(log_decay, head):
    span = log_decay.shape[-1]
    row = iota((span, span), 0)
    col = iota((span, span), 1)
    keep = row >= col
    lower = jnp.where(keep, 1.0, 0.0)
    own = log_decay[head : head + 1, :]
    down = jnp.sum(lower * own, axis=1, keepdims=True)
    across = jnp.sum(jnp.where(row <= col, 1.0, 0.0) * jnp.sum(
        jnp.where(row == col, own, 0.0), axis=1, keepdims=True), axis=0, keepdims=True)
    total = jnp.sum(own, axis=1, keepdims=True)
    table = jnp.where(keep, jnp.exp(jnp.where(keep, down - across, 0.0)), 0.0)
    return table, jnp.exp(down), jnp.exp(total - down), total


def mixed_kernel(at, q, k, v, log_decay, state, mixed):
    heads, _, size = q.shape
    width = v.shape[2]
    scale = size**-0.5
    for h in range(heads):
        table, lead, _, _ = decays(log_decay[...], h)
        scores = (dot(q[h], k[h], 1, 1) * (scale * table)).astype(BF16)
        out = dot(scores, v[h]) + lead * dot(q[h], state[h, 0].astype(BF16))
        mixed[:, h * width : (h + 1) * width] = out.astype(BF16)


PIECES = 16


def pieces(decay, shape):
    row = iota(shape, 0)
    high = decay.astype(BF16).astype(F32)
    rest = decay - high
    middle = rest.astype(BF16).astype(F32)
    low = rest - middle
    return jnp.where(row == 0, high, jnp.where(row == 1, middle, jnp.where(row == 2, low, 0.0)))


def put_message(ref, h, body, decay):
    size = body.shape[0]
    ref[h, :size, :] = body.astype(BF16)
    ref[h, size:, :] = pieces(decay, (PIECES, body.shape[1])).astype(BF16)


def get_message(ref, h):
    size = ref.shape[1] - PIECES
    decay = jnp.sum(ref[h, size:, :].astype(F32), axis=0, keepdims=True)[:, 0:1]
    return ref[h, :size, :].astype(F32), decay


def carry_kernel(
    at, ma, mb, near, q_in, decay_in, wo, hg, keep, send, slices, far, q, log_decay, sems
):
    heads, span, _ = q.shape
    groups, rows, size = slices.shape
    width = hg.shape[2]
    half = width // 2
    tall = ma.shape[1]
    begin = pl.multiple_of((1 - at[0]) * tall, tall)
    copies = [
        pltpu.make_async_copy(decay_in, log_decay, sems.at[heads + 1]),
        pltpu.make_async_copy(q_in, q, sems.at[heads]),
    ]
    for h in range(heads):
        cut = slice(h * width, (h + 1) * width)
        copies.append(
            pltpu.make_async_copy(wo.at[pl.ds(begin, tall), cut], far.at[:, cut], sems.at[h])
        )
    for each in copies:
        each.start()
    mine = pl.ds(pl.multiple_of(at[0] * rows, rows), rows)
    turn = groups // 2
    for i in range(turn):
        slices[at[0] * turn + i] = ma[mine, i * size : (i + 1) * size]
        slices[(1 - at[0]) * turn + i] = mb[mine, i * size : (i + 1) * size]
    upper = (at[1] & 1) == 1
    lower = jnp.where(iota((span, span), 0) >= iota((span, span), 1), 1.0, 0.0)
    copies[0].wait()
    copies[1].wait()
    for h in range(heads):
        cut = slice(h * width, (h + 1) * width)
        first = dot(ma[...], near[:, cut])
        copies[2 + h].wait()
        h_grad = (first + dot(mb[...], far[:, cut])).astype(BF16)
        hg[h] = h_grad
        own = log_decay[h : h + 1, :]
        lead = jnp.exp(jnp.sum(lower * own, axis=1, keepdims=True))
        total = jnp.exp(jnp.sum(own, axis=1, keepdims=True))
        part = dot((q[h].astype(F32) * lead).astype(BF16), h_grad, 0, 0)
        put_message(keep, h, jnp.where(upper, part[:, half:], part[:, :half]), total)
        put_message(send, h, jnp.where(upper, part[:, :half], part[:, half:]), total)


def carry(at, ma, mb, near, w_out, q, log_decay, groups, value_size):
    span, half = ma.shape
    heads, _, size = q.shape
    message = (heads, size + PIECES, value_size // 2)
    inside = pl.BlockSpec(memory_space=pltpu.VMEM)
    outside = pl.BlockSpec(memory_space=pltpu.HBM)
    return pl.pallas_call(
        carry_kernel,
        in_specs=[pl.BlockSpec(memory_space=pltpu.SMEM)] + [inside] * 3 + [outside] * 3,
        out_specs=[pl.BlockSpec()] * 4,
        out_shape=[
            pltpu.HBM((heads, span, value_size), BF16),
            jax.ShapeDtypeStruct(message, BF16),
            jax.ShapeDtypeStruct(message, BF16),
            pltpu.HBM((groups, span // 2, 2 * half // groups), BF16),
        ],
        scratch_shapes=[
            pltpu.VMEM((half, heads * value_size), BF16),
            pltpu.VMEM(q.shape, BF16),
            pltpu.VMEM(log_decay.shape, F32),
            pltpu.SemaphoreType.DMA((heads + 2,)),
        ],
        compiler_params=limit(12),
        name="carry",
    )(at, ma, mb, near, in_hbm(q), in_hbm(log_decay), in_hbm(w_out))


def pair_kernel(at, keep, came, out):
    upper = (at[1] & 1) == 1
    for h in range(keep.shape[0]):
        mine, mine_decay = get_message(keep, h)
        theirs, their_decay = get_message(came, h)
        first = jnp.where(upper, theirs, mine)
        second = jnp.where(upper, mine, theirs)
        decay = jnp.where(upper, their_decay, mine_decay)
        put_message(out, h, first + decay * second, mine_decay * their_decay)


def join_kernel(at, group, came, later, reach, out, later_out, reach_out, *, bit):
    upper = (at[1] & bit) != 0
    for h in range(group.shape[0]):
        mine, mine_decay = get_message(group, h)
        theirs, their_decay = get_message(came, h)
        first = jnp.where(upper, theirs, mine)
        second = jnp.where(upper, mine, theirs)
        decay = jnp.where(upper, their_decay, mine_decay)
        put_message(out, h, first + decay * second, mine_decay * their_decay)
        old = reach[h : h + 1, :]
        later_out[h] = later[h] + jnp.where(upper, 0.0, old[:, 0:1]) * theirs
        reach_out[h : h + 1, :] = old * jnp.where(upper, 1.0, their_decay)


def close_kernel(at, came, later, reach, keep, first_came, own, send, *, bit):
    upper = (at[1] & bit) != 0
    right = (at[1] & 1) == 1
    for h in range(keep.shape[0]):
        theirs, _ = get_message(came, h)
        after = later[h] + jnp.where(upper, 0.0, reach[h : h + 1, 0:1]) * theirs
        mine, mine_decay = get_message(keep, h)
        pair, pair_decay = get_message(first_came, h)
        second = jnp.where(right, mine, pair)
        decay = jnp.where(right, mine_decay, pair_decay)
        through = second + decay * after
        own[h] = jnp.where(right, after, through).astype(BF16)
        send[h] = jnp.where(right, through, after).astype(BF16)


def small(kernel, outs, at, *operands, mib=8):
    spec = pl.BlockSpec()
    many = isinstance(outs, (list, tuple))
    return pl.pallas_call(
        kernel,
        in_specs=[pl.BlockSpec(memory_space=pltpu.SMEM)] + [spec] * len(operands),
        out_specs=[spec] * len(outs) if many else spec,
        out_shape=outs,
        compiler_params=limit(mib),
    )(at, *operands)


def local_kernel(at, q, k, v, log_decay, state, hg, q_grad, k_part, v_part):
    heads, _, size = q.shape
    scale = size**-0.5
    for h in range(heads):
        table, lead, _, _ = decays(log_decay[...], h)
        scores = (dot(q[h], k[h], 1, 1) * (scale * table)).astype(BF16)
        back = (dot(hg[h], v[h], 1, 1) * table).astype(BF16)
        from_state = dot(hg[h], state[h, 0].astype(BF16), 1, 1)
        q_grad[h] = (scale * dot(back, k[h]) + lead * from_state).astype(BF16)
        k_part[h] = dot(back, q[h], 0, 0)
        v_part[h] = dot(scores, hg[h], 0, 0)


def final_kernel(at, k, v, log_decay, own, came, k_part, v_part, k_grad, v_grad):
    heads, _, size = k.shape
    half = v.shape[2] // 2
    scale = size**-0.5
    right = (at[1] & 1) == 1
    for h in range(heads):
        _, _, trail, _ = decays(log_decay[...], h)
        low = jnp.where(right, came[h].astype(F32), own[h].astype(F32)).astype(BF16)
        high = jnp.where(right, own[h].astype(F32), came[h].astype(F32)).astype(BF16)
        back = dot(v[h, :, :half], low, 1, 1) + dot(v[h, :, half:], high, 1, 1)
        k_grad[h] = (scale * (k_part[h] + trail * back)).astype(BF16)
        strength = scale * trail
        v_grad[h, :, :half] = (v_part[h, :, :half] + strength * dot(k[h], low)).astype(BF16)
        v_grad[h, :, half:] = (v_part[h, :, half:] + strength * dot(k[h], high)).astype(BF16)


def project_kernel(order, core, xa, xb, *refs):
    out, x = refs[-2:]
    rows = xa.shape[1]

    @pl.when(pl.program_id(0) == 0)
    def _():
        x[:, pl.ds(pl.multiple_of(core[0] * rows, rows), rows), :] = xa[...]
        x[:, pl.ds(pl.multiple_of((1 - core[0]) * rows, rows), rows), :] = xb[...]

    total, at = None, 0
    for y in refs[:-2]:
        blocks, span, width = y.shape
        left = jnp.concatenate([x[order[at + i]] for i in range(blocks)], axis=0)
        part = dot(left, y[...].reshape(blocks * span, width), 0, 0)
        total = part if total is None else total + part
        at += blocks
    out[...] = total


def project(order, at, xa, xb, parts):
    groups, rows, size = xa.shape
    width = parts[0].shape[2]
    chunk = min(width, 512)
    piece = pl.BlockSpec((groups, rows, size), lambda i, *_: (0, 0, 0))
    return pl.pallas_call(
        project_kernel,
        grid_spec=pltpu.PrefetchScalarGridSpec(
            num_scalar_prefetch=2,
            grid=(width // chunk,),
            in_specs=[piece, piece]
            + [pl.BlockSpec(y.shape[:2] + (chunk,), lambda i, *_: (0, 0, i)) for y in parts],
            out_specs=pl.BlockSpec((size, chunk), lambda i, *_: (0, i)),
            scratch_shapes=[pltpu.VMEM((groups, 2 * rows, size), BF16)],
        ),
        out_shape=jax.ShapeDtypeStruct((size, width), F32),
        compiler_params=limit(16),
        name="project",
    )(order, at, xa, xb, *parts)


def swap(a, axis, bit):
    count = lax.axis_size(axis)
    return lax.ppermute(a, axis, [(i, i ^ bit) for i in range(count)])


def far_first(count):
    return list(range(count // 2, count)) + list(range(count // 2 - 1, 0, -1))


def bits_of(count):
    return [1 << i for i in range(count.bit_length() - 1)]


def step(
    moe_input,
    out_grad,
    routes,
    route_weight,
    w_gate,
    w_up,
    w_down,
    w_out,
    query_heads,
    key_heads,
    value_heads,
    log_decay,
    state_in,
):
    tokens, width = moe_input.shape
    half = width // 2
    sp = lax.axis_size("sp")
    tp = lax.axis_size("tp")
    place = lax.axis_index("sp").astype(jnp.int32)
    column = lax.axis_index("tp").astype(jnp.int32)
    core = column & 1
    at = jnp.stack([core, place, (column >> 1) & 1])
    experts = w_gate.shape[0] * sp
    cap = 5 * tokens * routes.shape[1] // (4 * experts)
    heads, _, size = query_heads.shape
    value_size = value_heads.shape[-1]

    picked, *sent = dispatch(at, routes.T, route_weight.T, moe_input, out_grad, experts, cap)
    came = {0: sent[0]}
    for n in far_first(sp):
        came[n] = swap(sent[n], "sp", n)
    mixed = small(
        mixed_kernel, jax.ShapeDtypeStruct((tokens, heads * value_size), BF16),
        at, *[in_hbm(a) for a in (query_heads, key_heads, value_heads, log_decay, state_in)],
    )
    own = gather([came[n] for n in range(sp)])
    other = swap(own, "tp", 1)
    hidden, gate_back, up_back, part_b = expert_back(at, own, other, w_gate, w_up, w_down)
    part_came = swap(part_b, "tp", 1)
    part_a = expert_part(at, gate_back, up_back, w_gate, w_up)
    parts_out = small(add_blocks_kernel, [pltpu.HBM((cap, half), BF16)] * sp, at, part_a, part_came)
    back = {0: parts_out[0]}
    for n in far_first(sp):
        back[n] = swap(parts_out[n], "sp", n)
    gate_grad, up_grad, down_grad = weight_grads(at, own, other, hidden, gate_back, up_back)

    blocks = mixed[None]
    parts, offsets = [], [0]
    for bit in reversed(bits_of(sp)):
        if not parts:
            parts = [jnp.concatenate([blocks, swap(blocks, "sp", bit)], axis=0)]
        else:
            came = []
            for piece in parts:
                came.append(swap(piece, "sp", bit))
            parts = parts + came
        offsets = offsets + [o ^ bit for o in offsets]
    order = (place ^ jnp.array(offsets, jnp.int32)).astype(jnp.int32)

    token_shape = jax.ShapeDtypeStruct((tokens, half), BF16)
    token_part = small(combine_kernel, token_shape, at, in_hbm(picked), *[in_hbm(back[n]) for n in range(sp)])
    for bit in bits_of(tp)[1:]:
        came = swap(token_part, "tp", bit)
        if bit * 2 < tp:
            token_part = (token_part.astype(F32) + came.astype(F32)).astype(BF16)
    base, near_out = base_sum(at, out_grad, token_part, w_out)
    mixed_a = small(add_kernel, token_shape, at, base, came)
    mixed_b = swap(mixed_a, "tp", 1)

    message = jax.ShapeDtypeStruct((heads, size + PIECES, value_size // 2), BF16)
    head_grad, keep, send, slices = carry(
        at, mixed_a, mixed_b, near_out, w_out, query_heads, log_decay, sp, value_size
    )
    first_came = swap(send, "sp", 1)
    q_grad, k_part, v_part = small(
        local_kernel,
        [
            jax.ShapeDtypeStruct(query_heads.shape, BF16),
            jax.ShapeDtypeStruct(key_heads.shape, F32),
            jax.ShapeDtypeStruct(value_heads.shape, F32),
        ],
        at,
        *[in_hbm(a) for a in (query_heads, key_heads, value_heads, log_decay, state_in, head_grad)],
        mib=12,
    )
    state_shape = (heads, size, value_size // 2)
    group = small(pair_kernel, message, at, keep, first_came)
    later = jnp.zeros(state_shape, F32)
    reach = jnp.ones((heads, 128), F32)
    for bit in bits_of(sp)[1:]:
        came_state = swap(group, "sp", bit)
        if bit * 2 < sp:
            group, later, reach = small(
                functools.partial(join_kernel, bit=bit),
                [message, jax.ShapeDtypeStruct(state_shape, F32),
                 jax.ShapeDtypeStruct((heads, 128), F32)],
                at, group, came_state, later, reach,
            )
    state_out = jax.ShapeDtypeStruct(state_shape, BF16)
    own_state, send_state = small(
        functools.partial(close_kernel, bit=bit),
        [state_out, state_out], at, came_state, later, reach, keep, first_came,
    )
    other_state = swap(send_state, "sp", 1)
    slices_a = lax.all_to_all(slices, "sp", split_axis=0, concat_axis=0, tiled=True)
    slices_b = swap(slices_a, "tp", 1)
    out_proj_grad = project(order, at, slices_a, slices_b, parts)
    k_grad, v_grad = small(
        final_kernel,
        [jax.ShapeDtypeStruct(key_heads.shape, BF16),
         jax.ShapeDtypeStruct(value_heads.shape, BF16)],
        at, key_heads, value_heads, log_decay, own_state, other_state, k_part, v_part,
    )
    return gate_grad, up_grad, down_grad, out_proj_grad, q_grad, k_grad, v_grad


def solution(mesh):
    return jax.shard_map(
        step,
        mesh=mesh,
        in_specs=(
            P("sp", None),
            P("sp", None),
            P("sp", None),
            P("sp", None),
            P("sp", None, "tp"),
            P("sp", None, "tp"),
            P("sp", "tp", None),
            P(None, "tp"),
            P("tp", "sp", None),
            P("tp", "sp", None),
            P("tp", "sp", None),
            P("tp", "sp"),
            P("tp", "sp", None, None),
        ),
        out_specs=(
            P("sp", None, "tp"),
            P("sp", None, "tp"),
            P("sp", "tp", None),
            P("sp", "tp"),
            P("tp", "sp", None),
            P("tp", "sp", None),
            P("tp", "sp", None),
        ),
        check_vma=False,
    )
```

```python
import functools

import jax
import jax.numpy as jnp
from jax import lax
from jax.experimental import pallas as pl
from jax.experimental.pallas import tpu as pltpu
from jax.sharding import PartitionSpec as P


F32 = jnp.float32
BF16 = jnp.bfloat16
EXACT = lax.Precision.HIGHEST


def dot(a, b, ca=1, cb=0, precision=None):
    return lax.dot_general(
        a, b, (((ca,), (cb,)), ((), ())), preferred_element_type=F32, precision=precision
    )


def iota(shape, axis):
    return lax.broadcasted_iota(jnp.int32, shape, axis)


def in_hbm(a):
    return pltpu.with_memory_space_constraint(a, pltpu.HBM)


def limit(mib):
    return pltpu.CompilerParams(vmem_limit_bytes=mib << 20)


def dispatch_kernel(at, routes, weight, x, g, place, *blocks, experts, cap):
    tokens, half = x.shape
    slots = experts * cap
    expert = iota((experts, tokens), 0)
    first = routes[0:1, :] == expert
    second = routes[1:2, :] == expert
    named = jnp.where(first | second, 1.0, 0.0)
    share = jnp.where(first, weight[0:1, :], 0.0) + jnp.where(second, weight[1:2, :], 0.0)
    before = jnp.where(iota((tokens, tokens), 0) < iota((tokens, tokens), 1), 1.0, 0.0)
    rank_t = dot(named.astype(BF16), before.astype(BF16))
    rank_t = jnp.where(named > 0.5, rank_t, 2.0 * cap)
    slot = iota((slots, experts), 0)
    base = (iota((slots, experts), 1) ^ at[1]) * cap
    owner = (slot >= base) & (slot < base + cap)
    owner_f = jnp.where(owner, 1.0, 0.0)
    number = jnp.sum(jnp.where(owner, slot - base, 0).astype(F32), axis=1, keepdims=True)
    hit = dot(owner_f.astype(BF16), rank_t.astype(BF16)) == number
    picked = jnp.where(hit, 1.0, 0.0).astype(BF16)
    share_slot = jnp.sum(
        jnp.where(hit, dot(owner_f, share, precision=EXACT), 0.0), axis=1, keepdims=True
    )
    place[...] = picked
    rows = dot(picked, x[...])
    grads = share_slot * dot(picked, g[...])
    quarter = half // 2
    upper = at[2] == 1
    for n, block in enumerate(blocks):
        cut = slice(n * cap, (n + 1) * cap)
        if block.shape[1] == half:
            for m, a in enumerate((rows, grads)):
                mine = jnp.where(upper, a[cut, quarter:], a[cut, :quarter])
                block[:, m * quarter : (m + 1) * quarter] = mine.astype(BF16)
        else:
            block[:, :half] = rows[cut].astype(BF16)
            block[:, half:] = grads[cut].astype(BF16)


def dispatch(at, routes, weight, x, g, experts, cap):
    tokens, width = x.shape
    half = width // 2
    slots = experts * cap
    whole = lambda i, c: (0, 0)
    mine = pl.BlockSpec((tokens, half), lambda i, c: (0, c[0]))
    wide = [half if n in shared_far(experts) else width for n in range(experts)]
    return pl.pallas_call(
        functools.partial(dispatch_kernel, experts=experts, cap=cap),
        grid_spec=pltpu.PrefetchScalarGridSpec(
            num_scalar_prefetch=1,
            grid=(1,),
            in_specs=[
                pl.BlockSpec(routes.shape, whole), pl.BlockSpec(weight.shape, whole), mine, mine,
            ],
            out_specs=[pl.BlockSpec((slots, tokens), whole)]
            + [pl.BlockSpec((cap, w), whole) for w in wide],
        ),
        out_shape=[jax.ShapeDtypeStruct((slots, tokens), BF16)]
        + [jax.ShapeDtypeStruct((cap, w), BF16) for w in wide],
        compiler_params=limit(12),
        name="dispatch",
    )(at, in_hbm(routes), in_hbm(weight), in_hbm(x), in_hbm(g))


def gather_kernel(at, *refs, homes):
    blocks, out, sems = refs[:-2], refs[-2], refs[-1]
    half = out.shape[2] // 2
    quarter = half // 2
    copies = []

    def copy(source, target):
        copies.append(pltpu.make_async_copy(source, target, sems.at[len(copies)]))
        copies[-1].start()

    for block, (n, side) in zip(blocks, homes):
        if side is None:
            copy(block, out.at[n])
        else:
            place = at[2] if side == 0 else 1 - at[2]
            for m in range(2):
                begin = pl.multiple_of(m * half + place * quarter, quarter)
                copy(
                    block.at[:, m * quarter : (m + 1) * quarter],
                    out.at[n, :, pl.ds(begin, quarter)],
                )
    for each in copies:
        each.wait()


def gather(at, blocks, homes, experts, cap, width):
    out = pl.pallas_call(
        functools.partial(gather_kernel, homes=homes),
        in_specs=[pl.BlockSpec(memory_space=pltpu.SMEM)]
        + [pl.BlockSpec(memory_space=pl.ANY)] * len(blocks),
        out_specs=pl.BlockSpec(memory_space=pltpu.VMEM),
        out_shape=jax.ShapeDtypeStruct((experts, cap, width), BF16),
        scratch_shapes=[pltpu.SemaphoreType.DMA((2 * len(blocks),))],
        compiler_params=limit(4),
        name="gather",
    )(at, *blocks)
    return out.reshape(experts * cap, width)


def stage_kernel(at, *refs, kinds):
    count = len(kinds)
    sources, outs, sems = refs[:count], refs[count:-1], refs[-1]
    copies = []

    def copy(source, target):
        copies.append(pltpu.make_async_copy(source, target, sems.at[len(copies)]))
        copies[-1].start()

    for source, target, kind in zip(sources, outs, kinds):
        if kind == "plain":
            copy(source, target)
            continue
        half = target.shape[1] if kind == "tall" else target.shape[2]
        for side in range(2):
            begin = pl.multiple_of((at[0] if side == 0 else 1 - at[0]) * half, half)
            cut = pl.ds(begin, half)
            copy(source.at[cut, :] if kind == "tall" else source.at[:, cut], target.at[side])
    for each in copies:
        each.wait()


def stage(at, kinds, arrays):
    shapes = []
    for a, kind in zip(arrays, kinds):
        if kind == "tall":
            shapes.append(pltpu.VMEM((2, a.shape[0] // 2, a.shape[1]), a.dtype))
        elif kind == "wide":
            shapes.append(pltpu.VMEM((2, a.shape[0], a.shape[1] // 2), a.dtype))
        else:
            shapes.append(pltpu.VMEM(a.shape, a.dtype))
    count = len(arrays)
    return pl.pallas_call(
        functools.partial(stage_kernel, kinds=kinds),
        in_specs=[pl.BlockSpec(memory_space=pltpu.SMEM)]
        + [pl.BlockSpec(memory_space=pltpu.HBM)] * count,
        out_specs=[pl.BlockSpec(memory_space=pltpu.VMEM)] * count,
        out_shape=shapes,
        scratch_shapes=[pltpu.SemaphoreType.DMA((2 * count,))],
        compiler_params=limit(2),
        name="stage",
    )(at, *[in_hbm(a) for a in arrays])


def expert_kernel(at, own, other, wg, wu, wd, hidden, gback, uback, pb):
    half = own.shape[1] // 2
    units = hidden.shape[1]
    chunk = min(units, 256)
    for f in range(0, units, chunk):
        cut = slice(f, f + chunk)
        gate = dot(own[:, :half], wg[0, :, cut]) + dot(other[:, :half], wg[1, :, cut])
        up = dot(own[:, :half], wu[0, :, cut]) + dot(other[:, :half], wu[1, :, cut])
        back = dot(own[:, half:], wd[0, cut, :], 1, 1) + dot(other[:, half:], wd[1, cut, :], 1, 1)
        sig = 1.0 / (1.0 + jnp.exp(-gate))
        active = gate * sig
        hidden[:, cut] = (active * up).astype(BF16)
        gback[:, cut] = (back * up * (sig * (1.0 + gate * (1.0 - sig)))).astype(BF16)
        uback[:, cut] = (back * active).astype(BF16)
    pb[...] = (dot(gback[...], wg[1], 1, 1) + dot(uback[...], wu[1], 1, 1)).astype(BF16)


def partial_kernel(at, gback, uback, wg, wu, out):
    out[...] = (dot(gback[...], wg[0], 1, 1) + dot(uback[...], wu[0], 1, 1)).astype(BF16)


def add_blocks_kernel(at, a, b, *blocks):
    cap = blocks[0].shape[0]
    for n, block in enumerate(blocks):
        cut = slice(n * cap, (n + 1) * cap)
        block[...] = (a[cut, :].astype(F32) + b[cut, :].astype(F32)).astype(BF16)


def add_kernel(at, a, b, out):
    out[...] = (a[...].astype(F32) + b[...].astype(F32)).astype(out.dtype)


def weights_kernel(core, ra, rb, ga, gb, hidden, gback, uback, gate_out, up_out, down_out):
    step = pl.program_id(0)
    turn = pl.num_programs(0) // 2

    def write(r, g):
        gate_out[...] = dot(r[...], gback[...], 0, 0).astype(BF16)
        up_out[...] = dot(r[...], uback[...], 0, 0).astype(BF16)
        down_out[...] = dot(hidden[...], g[...], 0, 0).astype(BF16)

    @pl.when(step < turn)
    def _():
        write(ra, ga)

    @pl.when(step >= turn)
    def _():
        write(rb, gb)


def weight_grads(core, own, other, hidden, gback, uback):
    rows, width = own.shape
    half = width // 2
    units = hidden.shape[1]
    chunk = min(half, 512)
    turn = half // chunk
    near = lambda i: jnp.minimum(i, turn - 1)
    far = lambda i: jnp.maximum(i - turn, 0)
    at = lambda i, c: jnp.where(i < turn, c[0] * turn + i, (1 - c[0]) * turn + i - turn)
    full = pl.BlockSpec((rows, units), lambda i, c: (0, 0))
    tall = pl.BlockSpec((None, chunk, units), lambda i, c: (0, at(i, c), 0))
    wide = pl.BlockSpec((None, units, chunk), lambda i, c: (0, 0, at(i, c)))
    return pl.pallas_call(
        weights_kernel,
        grid_spec=pltpu.PrefetchScalarGridSpec(
            num_scalar_prefetch=1,
            grid=(2 * turn,),
            in_specs=[
                pl.BlockSpec((rows, chunk), lambda i, c: (0, near(i))),
                pl.BlockSpec((rows, chunk), lambda i, c: (0, far(i))),
                pl.BlockSpec((rows, chunk), lambda i, c: (0, turn + near(i))),
                pl.BlockSpec((rows, chunk), lambda i, c: (0, turn + far(i))),
                full, full, full,
            ],
            out_specs=[tall, tall, wide],
        ),
        out_shape=[
            jax.ShapeDtypeStruct((1, width, units), BF16),
            jax.ShapeDtypeStruct((1, width, units), BF16),
            jax.ShapeDtypeStruct((1, units, width), BF16),
        ],
        compiler_params=limit(20),
        name="weight_grads",
    )(core, own, other, own, other, hidden, gback, uback)


def combine_kernel(at, place, *refs):
    blocks, out = refs[:-1], refs[-1]
    cap = blocks[0].shape[0]
    total = None
    for n, block in enumerate(blocks):
        part = dot(place[n * cap : (n + 1) * cap, :], block[...], 0, 0)
        total = part if total is None else total + part
    out[...] = total.astype(BF16)


def base_kernel(at, g, part, out):
    out[...] = g[...].astype(F32) + part[...].astype(F32)


def base_sum(at, g, part):
    tokens, half = part.shape
    whole = lambda i, c: (0, 0)
    return pl.pallas_call(
        base_kernel,
        grid_spec=pltpu.PrefetchScalarGridSpec(
            num_scalar_prefetch=1,
            grid=(1,),
            in_specs=[
                pl.BlockSpec((tokens, half), lambda i, c: (0, c[0])),
                pl.BlockSpec((tokens, half), whole),
            ],
            out_specs=pl.BlockSpec((tokens, half), whole),
        ),
        out_shape=jax.ShapeDtypeStruct((tokens, half), F32),
        compiler_params=limit(4),
        name="base",
    )(at, in_hbm(g), part)


def decays(log_decay, head):
    span = log_decay.shape[-1]
    row = iota((span, span), 0)
    col = iota((span, span), 1)
    keep = row >= col
    lower = jnp.where(keep, 1.0, 0.0)
    own = log_decay[head : head + 1, :]
    down = jnp.sum(lower * own, axis=1, keepdims=True)
    across = jnp.sum(jnp.where(row <= col, 1.0, 0.0) * jnp.sum(
        jnp.where(row == col, own, 0.0), axis=1, keepdims=True), axis=0, keepdims=True)
    total = jnp.sum(own, axis=1, keepdims=True)
    table = jnp.where(keep, jnp.exp(jnp.where(keep, down - across, 0.0)), 0.0)
    return table, jnp.exp(down), jnp.exp(total - down), total


def mixed_kernel(at, q, k, v, log_decay, state, mixed):
    heads, _, size = q.shape
    width = v.shape[2]
    scale = size**-0.5
    for h in range(heads):
        table, lead, _, _ = decays(log_decay[...], h)
        scores = (dot(q[h], k[h], 1, 1) * (scale * table)).astype(BF16)
        out = dot(scores, v[h]) + lead * dot(q[h], state[h, 0].astype(BF16))
        mixed[:, h * width : (h + 1) * width] = out.astype(BF16)


PIECES = 16


def pieces(decay, shape):
    row = iota(shape, 0)
    high = decay.astype(BF16).astype(F32)
    rest = decay - high
    middle = rest.astype(BF16).astype(F32)
    low = rest - middle
    return jnp.where(row == 0, high, jnp.where(row == 1, middle, jnp.where(row == 2, low, 0.0)))


def put_message(ref, h, body, decay):
    size = body.shape[0]
    ref[h, :size, :] = body.astype(BF16)
    ref[h, size:, :] = pieces(decay, (PIECES, body.shape[1])).astype(BF16)


def get_message(ref, h):
    size = ref.shape[1] - PIECES
    decay = jnp.sum(ref[h, size:, :].astype(F32), axis=0, keepdims=True)[:, 0:1]
    return ref[h, :size, :].astype(F32), decay


def carry_kernel(at, ma, mb, wo, q, log_decay, hg, keep, send, stay, leave):
    heads, span, _ = q.shape
    turn, rows, size = stay.shape
    width = hg.shape[2]
    half = width // 2
    upper = (at[1] & 1) == 1
    lower = jnp.where(iota((span, span), 0) >= iota((span, span), 1), 1.0, 0.0)
    for h in range(heads):
        cut = slice(h * width, (h + 1) * width)
        h_grad = (dot(ma[...], wo[0, :, cut]) + dot(mb[...], wo[1, :, cut])).astype(BF16)
        hg[h] = h_grad
        own = log_decay[h : h + 1, :]
        lead = jnp.exp(jnp.sum(lower * own, axis=1, keepdims=True))
        total = jnp.exp(jnp.sum(own, axis=1, keepdims=True))
        part = dot((q[h].astype(F32) * lead).astype(BF16), h_grad, 0, 0)
        put_message(keep, h, jnp.where(upper, part[:, half:], part[:, :half]), total)
        put_message(send, h, jnp.where(upper, part[:, :half], part[:, half:]), total)
    mine = pl.ds(pl.multiple_of(at[0] * rows, rows), rows)
    side = at[0] ^ (at[1] // turn)

    def sort(near, far):
        for i in range(turn):
            n = i ^ (at[1] % turn)
            stay[n] = near[mine, i * size : (i + 1) * size]
            leave[n] = far[mine, i * size : (i + 1) * size]

    @pl.when(side == 0)
    def _():
        sort(ma, mb)

    @pl.when(side == 1)
    def _():
        sort(mb, ma)


def split_kernel(at, kept, came, stay, leave):
    sources, count = kept.shape[:2]
    for n, part in enumerate((kept, came)):
        for m in range(sources):
            stay[n * sources + m] = part[m, : count // 2]
            leave[n * sources + m] = part[m, count // 2 :]


def pair_kernel(at, keep, came, out):
    upper = (at[1] & 1) == 1
    for h in range(keep.shape[0]):
        mine, mine_decay = get_message(keep, h)
        theirs, their_decay = get_message(came, h)
        first = jnp.where(upper, theirs, mine)
        second = jnp.where(upper, mine, theirs)
        decay = jnp.where(upper, their_decay, mine_decay)
        put_message(out, h, first + decay * second, mine_decay * their_decay)


def join_kernel(at, group, came, later, reach, out, later_out, reach_out, *, bit):
    upper = (at[1] & bit) != 0
    for h in range(group.shape[0]):
        mine, mine_decay = get_message(group, h)
        theirs, their_decay = get_message(came, h)
        first = jnp.where(upper, theirs, mine)
        second = jnp.where(upper, mine, theirs)
        decay = jnp.where(upper, their_decay, mine_decay)
        put_message(out, h, first + decay * second, mine_decay * their_decay)
        old = reach[h : h + 1, :]
        later_out[h] = later[h] + jnp.where(upper, 0.0, old[:, 0:1]) * theirs
        reach_out[h : h + 1, :] = old * jnp.where(upper, 1.0, their_decay)


def close_kernel(at, came, later, reach, keep, first_came, own, send, *, bit):
    upper = (at[1] & bit) != 0
    right = (at[1] & 1) == 1
    for h in range(keep.shape[0]):
        theirs, _ = get_message(came, h)
        after = later[h] + jnp.where(upper, 0.0, reach[h : h + 1, 0:1]) * theirs
        mine, mine_decay = get_message(keep, h)
        pair, pair_decay = get_message(first_came, h)
        second = jnp.where(right, mine, pair)
        decay = jnp.where(right, mine_decay, pair_decay)
        through = second + decay * after
        own[h] = jnp.where(right, after, through).astype(BF16)
        send[h] = jnp.where(right, through, after).astype(BF16)


def small(kernel, outs, at, *operands, mib=8):
    spec = pl.BlockSpec()
    many = isinstance(outs, (list, tuple))
    return pl.pallas_call(
        kernel,
        in_specs=[pl.BlockSpec(memory_space=pltpu.SMEM)] + [spec] * len(operands),
        out_specs=[spec] * len(outs) if many else spec,
        out_shape=outs,
        compiler_params=limit(mib),
    )(at, *operands)


def local_kernel(at, q, k, v, log_decay, state, hg, q_grad, k_part, v_part, trails):
    heads, _, size = q.shape
    scale = size**-0.5
    for h in range(heads):
        table, lead, trail, _ = decays(log_decay[...], h)
        trails[h] = scale * trail
        scores = (dot(q[h], k[h], 1, 1) * (scale * table)).astype(BF16)
        back = (dot(hg[h], v[h], 1, 1) * table).astype(BF16)
        from_state = dot(hg[h], state[h, 0].astype(BF16), 1, 1)
        q_grad[h] = (scale * dot(back, k[h]) + lead * from_state).astype(BF16)
        k_part[h] = scale * dot(back, q[h], 0, 0)
        v_part[h] = dot(scores, hg[h], 0, 0)


def final_kernel(at, k, v, trails, own, came, k_part, v_part, k_grad, v_grad):
    heads = k.shape[0]
    half = v.shape[2] // 2
    right = (at[1] & 1) == 1
    for h in range(heads):
        low = jnp.where(right, came[h].astype(F32), own[h].astype(F32)).astype(BF16)
        high = jnp.where(right, own[h].astype(F32), came[h].astype(F32)).astype(BF16)
        back = dot(v[h, :, :half], low, 1, 1) + dot(v[h, :, half:], high, 1, 1)
        trail = trails[h]
        k_grad[h] = (k_part[h] + trail * back).astype(BF16)
        v_grad[h, :, :half] = (v_part[h, :, :half] + trail * dot(k[h], low)).astype(BF16)
        v_grad[h, :, half:] = (v_part[h, :, half:] + trail * dot(k[h], high)).astype(BF16)


def project_kernel(core, a0, a1, b0, b1, *refs):
    out, x = refs[-2:]
    turn, rows, size = a0.shape

    @pl.when(pl.program_id(0) == 0)
    def _():
        mine = pl.ds(pl.multiple_of(core[0] * rows, rows), rows)
        other = pl.ds(pl.multiple_of((1 - core[0]) * rows, rows), rows)
        for place, pair in ((mine, (a0, a1)), (other, (b0, b1))):
            x[:turn, place, :] = pair[0][...]
            x[turn:, place, :] = pair[1][...]

    total, at = None, 0
    for y in refs[:-2]:
        blocks, span, width = y.shape
        left = x[at : at + blocks].reshape(blocks * span, size)
        part = dot(left, y[...].reshape(blocks * span, width), 0, 0)
        total = part if total is None else total + part
        at += blocks
    out[...] = total


def project(at, slices, parts):
    turn, rows, size = slices[0].shape
    width = parts[0].shape[2]
    chunk = min(width, 512)
    piece = pl.BlockSpec((turn, rows, size), lambda i, *_: (0, 0, 0))
    return pl.pallas_call(
        project_kernel,
        grid_spec=pltpu.PrefetchScalarGridSpec(
            num_scalar_prefetch=1,
            grid=(width // chunk,),
            in_specs=[piece] * 4
            + [pl.BlockSpec(y.shape[:2] + (chunk,), lambda i, *_: (0, 0, i)) for y in parts],
            out_specs=pl.BlockSpec((size, chunk), lambda i, *_: (0, i)),
            scratch_shapes=[pltpu.VMEM((2 * turn, 2 * rows, size), BF16)],
        ),
        out_shape=jax.ShapeDtypeStruct((size, width), F32),
        compiler_params=limit(16),
        name="project",
    )(at, *slices, *parts)


def swap(a, axis, bit):
    count = lax.axis_size(axis)
    return lax.ppermute(a, axis, [(i, i ^ bit) for i in range(count)])


def far_first(count):
    return list(range(count // 2, count)) + list(range(count // 2 - 1, 0, -1))


def shared_far(count):
    return far_first(count)[: count // 2 - 1]


def bits_of(count):
    return [1 << i for i in range(count.bit_length() - 1)]


def step(
    moe_input,
    out_grad,
    routes,
    route_weight,
    w_gate,
    w_up,
    w_down,
    w_out,
    query_heads,
    key_heads,
    value_heads,
    log_decay,
    state_in,
):
    tokens, width = moe_input.shape
    half = width // 2
    sp = lax.axis_size("sp")
    tp = lax.axis_size("tp")
    place = lax.axis_index("sp").astype(jnp.int32)
    column = lax.axis_index("tp").astype(jnp.int32)
    core = column & 1
    at = jnp.stack([core, place, (column >> 1) & 1])
    experts = w_gate.shape[0] * sp
    cap = 5 * tokens * routes.shape[1] // (4 * experts)
    slots = experts * cap
    units = w_gate.shape[2]
    heads, _, size = query_heads.shape
    value_size = value_heads.shape[-1]

    picked, *sent = dispatch(at, routes.T, route_weight.T, moe_input, out_grad, experts, cap)
    came = {0: sent[0]}
    for n in far_first(sp):
        came[n] = swap(sent[n], "sp", n)
    wg, q, k, v, state, decay = stage(
        at, ("tall",) + ("plain",) * 5,
        (w_gate[0], query_heads, key_heads, value_heads, state_in, log_decay),
    )
    wu, wd = stage(at, ("tall", "wide"), (w_up[0], w_down[0]))
    (wo,) = stage(at, ("tall",), (w_out,))
    mixed = small(
        mixed_kernel, jax.ShapeDtypeStruct((tokens, heads * value_size), BF16),
        at, q, k, v, decay, state,
    )
    blocks, homes = [], []
    for n in range(sp):
        blocks.append(came[n])
        homes.append((n, 0 if n in shared_far(sp) else None))
        if n in shared_far(sp):
            blocks.append(swap(came[n], "tp", 2))
            homes.append((n, 1))
    own = gather(at, blocks, tuple(homes), experts, cap, width)
    other = swap(own, "tp", 1)
    hidden, gate_back, up_back, part_b = small(
        expert_kernel,
        [jax.ShapeDtypeStruct((slots, units), BF16)] * 3
        + [jax.ShapeDtypeStruct((slots, half), BF16)],
        at, own, other, wg, wu, wd, mib=16,
    )
    part_came = swap(part_b, "tp", 1)
    part_a = small(
        partial_kernel, jax.ShapeDtypeStruct((slots, half), BF16),
        at, gate_back, up_back, wg, wu,
    )
    parts_out = small(
        add_blocks_kernel, [jax.ShapeDtypeStruct((cap, half), BF16)] * sp,
        at, part_a, part_came,
    )
    back = {0: parts_out[0]}
    for n in far_first(sp):
        back[n] = swap(parts_out[n], "sp", n)
    gate_grad, up_grad, down_grad = weight_grads(at, own, other, hidden, gate_back, up_back)

    blocks = mixed[None]
    parts = []
    for bit in reversed(bits_of(sp)):
        if not parts:
            parts = [jnp.concatenate([blocks, swap(blocks, "sp", bit)], axis=0)]
        else:
            came = []
            for piece in parts:
                came.append(swap(piece, "sp", bit))
            parts = parts + came

    token_shape = jax.ShapeDtypeStruct((tokens, half), BF16)
    token_part = small(combine_kernel, token_shape, at, picked, *[back[n] for n in range(sp)])
    for bit in bits_of(tp)[1:]:
        came = swap(token_part, "tp", bit)
        if bit * 2 < tp:
            token_part = (token_part.astype(F32) + came.astype(F32)).astype(BF16)
    base = base_sum(at, out_grad, token_part)
    mixed_a = small(add_kernel, token_shape, at, base, came)
    mixed_b = swap(mixed_a, "tp", 1)

    message = jax.ShapeDtypeStruct((heads, size + PIECES, value_size // 2), BF16)
    turn = sp // 2
    block = (tokens // 2, width // sp)
    head_grad, keep, send, stay, leave = small(
        carry_kernel,
        [jax.ShapeDtypeStruct((heads, tokens, value_size), BF16), message, message]
        + [jax.ShapeDtypeStruct((turn,) + block, BF16)] * 2,
        at, mixed_a, mixed_b, wo, q, decay,
    )
    sources, slices = 1, []
    for bit in reversed(bits_of(sp)):
        came_slices = swap(leave, "sp", bit)
        if bit > 1:
            grid = (sources, bit) + block
            out = jax.ShapeDtypeStruct((2 * sources, bit // 2) + block, BF16)
            stay, leave = small(
                split_kernel, [out, out], at,
                stay.reshape(grid), came_slices.reshape(grid),
            )
            sources *= 2
        stay, leave = stay.reshape((turn,) + block), leave.reshape((turn,) + block)
    slices = [stay, came_slices.reshape((turn,) + block)]
    for n in range(2):
        slices.append(swap(slices[n], "tp", 1))
    first_came = swap(send, "sp", 1)
    q_grad, k_part, v_part, trails = small(
        local_kernel,
        [
            jax.ShapeDtypeStruct(query_heads.shape, BF16),
            jax.ShapeDtypeStruct(key_heads.shape, F32),
            jax.ShapeDtypeStruct(value_heads.shape, F32),
            jax.ShapeDtypeStruct((heads, tokens, 1), F32),
        ],
        at,
        q, k, v, decay, state, head_grad, mib=12,
    )
    state_shape = (heads, size, value_size // 2)
    group = small(pair_kernel, message, at, keep, first_came)
    later = jnp.zeros(state_shape, F32)
    reach = jnp.ones((heads, 128), F32)
    for bit in bits_of(sp)[1:]:
        came_state = swap(group, "sp", bit)
        if bit * 2 < sp:
            group, later, reach = small(
                functools.partial(join_kernel, bit=bit),
                [message, jax.ShapeDtypeStruct(state_shape, F32),
                 jax.ShapeDtypeStruct((heads, 128), F32)],
                at, group, came_state, later, reach,
            )
    state_out = jax.ShapeDtypeStruct(state_shape, BF16)
    own_state, send_state = small(
        functools.partial(close_kernel, bit=bit),
        [state_out, state_out], at, came_state, later, reach, keep, first_came,
    )
    other_state = swap(send_state, "sp", 1)
    out_proj_grad = project(at, slices, parts)
    k_grad, v_grad = small(
        final_kernel,
        [jax.ShapeDtypeStruct(key_heads.shape, BF16),
         jax.ShapeDtypeStruct(value_heads.shape, BF16)],
        at, k, v, trails, own_state, other_state, k_part, v_part,
    )
    return gate_grad, up_grad, down_grad, out_proj_grad, q_grad, k_grad, v_grad


def solution(mesh):
    return jax.shard_map(
        step,
        mesh=mesh,
        in_specs=(
            P("sp", None),
            P("sp", None),
            P("sp", None),
            P("sp", None),
            P("sp", None, "tp"),
            P("sp", None, "tp"),
            P("sp", "tp", None),
            P(None, "tp"),
            P("tp", "sp", None),
            P("tp", "sp", None),
            P("tp", "sp", None),
            P("tp", "sp"),
            P("tp", "sp", None, None),
        ),
        out_specs=(
            P("sp", None, "tp"),
            P("sp", None, "tp"),
            P("sp", "tp", None),
            P("sp", "tp"),
            P("tp", "sp", None),
            P("tp", "sp", None),
            P("tp", "sp", None),
        ),
        check_vma=False,
    )
```

```python
import functools

import jax
import jax.numpy as jnp
from jax import lax
from jax.experimental import pallas as pl
from jax.experimental.pallas import tpu as pltpu
from jax.sharding import PartitionSpec as P


F32 = jnp.float32
BF16 = jnp.bfloat16
EXACT = lax.Precision.HIGHEST
SP, TP = "sp", "tp"
TALL, WIDE, PLAIN = range(3)


def dot(a, b, ca=1, cb=0, precision=None):
    return lax.dot_general(
        a, b, (((ca,), (cb,)), ((), ())), preferred_element_type=F32, precision=precision
    )


def iota(shape, axis):
    return lax.broadcasted_iota(jnp.int32, shape, axis)


def in_hbm(a):
    return pltpu.with_memory_space_constraint(a, pltpu.HBM)


def limit(mib):
    return pltpu.CompilerParams(vmem_limit_bytes=mib << 20)


def dispatch_kernel(at, routes, weight, x, g, place, *blocks, experts, cap):
    tokens, half = x.shape
    slots = experts * cap
    expert = iota((experts, tokens), 0)
    first = routes[0:1, :] == expert
    second = routes[1:2, :] == expert
    named = jnp.where(first | second, 1.0, 0.0)
    share = jnp.where(first, weight[0:1, :], 0.0) + jnp.where(second, weight[1:2, :], 0.0)
    before = jnp.where(iota((tokens, tokens), 0) < iota((tokens, tokens), 1), 1.0, 0.0)
    rank_t = dot(named.astype(BF16), before.astype(BF16))
    rank_t = jnp.where(named > 0.5, rank_t, 2.0 * cap)
    slot = iota((slots, experts), 0)
    base = (iota((slots, experts), 1) ^ at[1]) * cap
    owner = (slot >= base) & (slot < base + cap)
    owner_f = jnp.where(owner, 1.0, 0.0)
    number = jnp.sum(jnp.where(owner, slot - base, 0).astype(F32), axis=1, keepdims=True)
    hit = dot(owner_f.astype(BF16), rank_t.astype(BF16)) == number
    picked = jnp.where(hit, 1.0, 0.0).astype(BF16)
    share_slot = jnp.sum(
        jnp.where(hit, dot(owner_f, share, precision=EXACT), 0.0), axis=1, keepdims=True
    )
    place[...] = picked
    rows = dot(picked, x[...])
    grads = share_slot * dot(picked, g[...])
    quarter = half // 2
    upper = at[2] == 1
    for n, block in enumerate(blocks):
        cut = slice(n * cap, (n + 1) * cap)
        if block.shape[1] == half:
            for m, a in enumerate((rows, grads)):
                mine = jnp.where(upper, a[cut, quarter:], a[cut, :quarter])
                block[:, m * quarter : (m + 1) * quarter] = mine.astype(BF16)
        else:
            block[:, :half] = rows[cut].astype(BF16)
            block[:, half:] = grads[cut].astype(BF16)


def dispatch(at, routes, weight, x, g, experts, cap):
    tokens, width = x.shape
    half = width // 2
    slots = experts * cap
    whole = lambda i, c: (0, 0)
    mine = pl.BlockSpec((tokens, half), lambda i, c: (0, c[0]))
    wide = [half if n in shared_far(experts) else width for n in range(experts)]
    return pl.pallas_call(
        functools.partial(dispatch_kernel, experts=experts, cap=cap),
        grid_spec=pltpu.PrefetchScalarGridSpec(
            num_scalar_prefetch=1,
            grid=(1,),
            in_specs=[
                pl.BlockSpec(routes.shape, whole), pl.BlockSpec(weight.shape, whole), mine, mine,
            ],
            out_specs=[pl.BlockSpec((slots, tokens), whole)]
            + [pl.BlockSpec((cap, w), whole) for w in wide],
        ),
        out_shape=[jax.ShapeDtypeStruct((slots, tokens), BF16)]
        + [jax.ShapeDtypeStruct((cap, w), BF16) for w in wide],
        compiler_params=limit(12),
        name="dispatch",
    )(at, in_hbm(routes), in_hbm(weight), in_hbm(x), in_hbm(g))


def gather_kernel(at, *refs, homes):
    blocks, out = refs[:-1], refs[-1]
    half = out.shape[2] // 2
    quarter = half // 2

    def put(low):
        for block, (n, side) in zip(blocks, homes):
            if side is not None:
                for m in range(2):
                    begin = m * half + (0 if (side == 0) == low else quarter)
                    out[n, :, begin : begin + quarter] = block[:, m * quarter : (m + 1) * quarter]

    for block, (n, side) in zip(blocks, homes):
        if side is None:
            out[n] = block[...]

    @pl.when(at[2] == 0)
    def _():
        put(True)

    @pl.when(at[2] == 1)
    def _():
        put(False)


def stage_kernel(at, *refs, kinds):
    count = len(kinds)
    sources, outs, sems = refs[:count], refs[count:-1], refs[-1]
    copies = []

    def copy(source, target):
        copies.append(pltpu.make_async_copy(source, target, sems.at[len(copies)]))
        copies[-1].start()

    for source, target, kind in zip(sources, outs, kinds):
        if kind == PLAIN:
            copy(source, target)
            continue
        half = target.shape[1] if kind == TALL else target.shape[2]
        for side in range(2):
            begin = pl.multiple_of((at[0] if side == 0 else 1 - at[0]) * half, half)
            cut = pl.ds(begin, half)
            copy(source.at[cut, :] if kind == TALL else source.at[:, cut], target.at[side])
    for each in copies:
        each.wait()


def stage(at, kinds, arrays):
    shapes = []
    for a, kind in zip(arrays, kinds):
        if kind == TALL:
            shapes.append(pltpu.VMEM((2, a.shape[0] // 2, a.shape[1]), a.dtype))
        elif kind == WIDE:
            shapes.append(pltpu.VMEM((2, a.shape[0], a.shape[1] // 2), a.dtype))
        else:
            shapes.append(pltpu.VMEM(a.shape, a.dtype))
    count = len(arrays)
    return pl.pallas_call(
        functools.partial(stage_kernel, kinds=kinds),
        in_specs=[pl.BlockSpec(memory_space=pltpu.SMEM)]
        + [pl.BlockSpec(memory_space=pltpu.HBM)] * count,
        out_specs=[pl.BlockSpec(memory_space=pltpu.VMEM)] * count,
        out_shape=shapes,
        scratch_shapes=[pltpu.SemaphoreType.DMA((2 * count,))],
        compiler_params=limit(2),
        name="stage",
    )(at, *[in_hbm(a) for a in arrays])


def expert_kernel(at, own, other, wg, wu, wd, hidden, gback, uback, pb):
    half = own.shape[1] // 2
    units = hidden.shape[1]
    chunk = min(units, 256)
    for f in range(0, units, chunk):
        cut = slice(f, f + chunk)
        gate = dot(own[:, :half], wg[0, :, cut]) + dot(other[:, :half], wg[1, :, cut])
        up = dot(own[:, :half], wu[0, :, cut]) + dot(other[:, :half], wu[1, :, cut])
        back = dot(own[:, half:], wd[0, cut, :], 1, 1) + dot(other[:, half:], wd[1, cut, :], 1, 1)
        sig = 1.0 / (1.0 + jnp.exp(-gate))
        active = gate * sig
        hidden[:, cut] = (active * up).astype(BF16)
        gback[:, cut] = (back * up * (sig * (1.0 + gate * (1.0 - sig)))).astype(BF16)
        uback[:, cut] = (back * active).astype(BF16)
    pb[...] = (dot(gback[...], wg[1], 1, 1) + dot(uback[...], wu[1], 1, 1)).astype(BF16)


def partial_kernel(at, gback, uback, wg, wu, out):
    out[...] = (dot(gback[...], wg[0], 1, 1) + dot(uback[...], wu[0], 1, 1)).astype(BF16)


def add_blocks_kernel(at, a, b, *blocks):
    cap = blocks[0].shape[0]
    for n, block in enumerate(blocks):
        cut = slice(n * cap, (n + 1) * cap)
        block[...] = (a[cut, :].astype(F32) + b[cut, :].astype(F32)).astype(BF16)


def weights_kernel(core, ra, rb, gback, uback, gate_out, up_out):
    step = pl.program_id(0)
    turn = pl.num_programs(0) // 2

    def write(r):
        gate_out[...] = dot(r[...], gback[...], 0, 0).astype(BF16)
        up_out[...] = dot(r[...], uback[...], 0, 0).astype(BF16)

    @pl.when(step < turn)
    def _():
        write(ra)

    @pl.when(step >= turn)
    def _():
        write(rb)


def down_kernel(core, ga, gb, hidden, out):
    step = pl.program_id(0)
    turn = pl.num_programs(0) // 2

    @pl.when(step < turn)
    def _():
        out[...] = dot(hidden[...], ga[...], 0, 0).astype(BF16)

    @pl.when(step >= turn)
    def _():
        out[...] = dot(hidden[...], gb[...], 0, 0).astype(BF16)


def weight_grads(core, own, other, gback, uback):
    rows, width = own.shape
    half = width // 2
    units = gback.shape[1]
    chunk = min(half, 512)
    turn = half // chunk
    at = lambda i, c: jnp.where(i < turn, c[0] * turn + i, (1 - c[0]) * turn + i - turn)
    full = pl.BlockSpec((rows, units), lambda i, c: (0, 0))
    tall = pl.BlockSpec((None, chunk, units), lambda i, c: (0, at(i, c), 0))
    return pl.pallas_call(
        weights_kernel,
        grid_spec=pltpu.PrefetchScalarGridSpec(
            num_scalar_prefetch=1,
            grid=(2 * turn,),
            in_specs=[
                pl.BlockSpec((rows, chunk), lambda i, c: (0, jnp.minimum(i, turn - 1))),
                pl.BlockSpec((rows, chunk), lambda i, c: (0, jnp.maximum(i - turn, 0))),
                full, full,
            ],
            out_specs=[tall, tall],
        ),
        out_shape=[jax.ShapeDtypeStruct((1, width, units), BF16)] * 2,
        compiler_params=limit(16),
        name="weights",
    )(core, own, other, gback, uback)


def down_grads(core, own, other, hidden):
    rows, width = own.shape
    half = width // 2
    units = hidden.shape[1]
    chunk = min(half, 512)
    turn = half // chunk
    at = lambda i, c: jnp.where(i < turn, c[0] * turn + i, (1 - c[0]) * turn + i - turn)
    return pl.pallas_call(
        down_kernel,
        grid_spec=pltpu.PrefetchScalarGridSpec(
            num_scalar_prefetch=1,
            grid=(2 * turn,),
            in_specs=[
                pl.BlockSpec((rows, chunk), lambda i, c: (0, turn + jnp.minimum(i, turn - 1))),
                pl.BlockSpec((rows, chunk), lambda i, c: (0, turn + jnp.maximum(i - turn, 0))),
                pl.BlockSpec((rows, units), lambda i, c: (0, 0)),
            ],
            out_specs=pl.BlockSpec((None, units, chunk), lambda i, c: (0, 0, at(i, c))),
        ),
        out_shape=jax.ShapeDtypeStruct((1, units, width), BF16),
        compiler_params=limit(12),
        name="down",
    )(core, own, other, hidden)


def combine_kernel(at, place, *refs):
    blocks, out = refs[:-1], refs[-1]
    cap = blocks[0].shape[0]
    total = None
    for n, block in enumerate(blocks):
        part = dot(place[n * cap : (n + 1) * cap, :], block[...], 0, 0)
        total = part if total is None else total + part
    out[...] = total.astype(BF16)


def sum_kernel(at, g, own, came, out):
    total = own[...].astype(F32) + came[...].astype(F32)
    out[...] = (g[0].astype(F32) + total).astype(BF16)


def decays(log_decay, head):
    span = log_decay.shape[-1]
    row = iota((span, span), 0)
    col = iota((span, span), 1)
    keep = row >= col
    lower = jnp.where(keep, 1.0, 0.0)
    own = log_decay[head : head + 1, :]
    down = jnp.sum(lower * own, axis=1, keepdims=True)
    across = jnp.sum(jnp.where(row <= col, 1.0, 0.0) * jnp.sum(
        jnp.where(row == col, own, 0.0), axis=1, keepdims=True), axis=0, keepdims=True)
    total = jnp.sum(own, axis=1, keepdims=True)
    table = jnp.where(keep, jnp.exp(jnp.where(keep, down - across, 0.0)), 0.0)
    return table, jnp.exp(down), jnp.exp(total - down), total


def mixed_kernel(at, q, k, v, log_decay, state, mixed):
    heads, _, size = q.shape
    width = v.shape[2]
    scale = size**-0.5
    for h in range(heads):
        table, lead, _, _ = decays(log_decay[...], h)
        scores = (dot(q[h], k[h], 1, 1) * (scale * table)).astype(BF16)
        out = dot(scores, v[h]) + lead * dot(q[h], state[h, 0].astype(BF16))
        mixed[:, h * width : (h + 1) * width] = out.astype(BF16)


PIECES = 16


def pieces(decay, shape):
    row = iota(shape, 0)
    high = decay.astype(BF16).astype(F32)
    rest = decay - high
    middle = rest.astype(BF16).astype(F32)
    low = rest - middle
    return jnp.where(row == 0, high, jnp.where(row == 1, middle, jnp.where(row == 2, low, 0.0)))


def put_message(ref, h, body, decay):
    size = body.shape[0]
    ref[h, :size, :] = body.astype(BF16)
    ref[h, size:, :] = pieces(decay, (PIECES, body.shape[1])).astype(BF16)


def get_message(ref, h):
    size = ref.shape[1] - PIECES
    decay = jnp.sum(ref[h, size:, :].astype(F32), axis=0, keepdims=True)[:, 0:1]
    return ref[h, :size, :].astype(F32), decay


def carry_kernel(at, ma, mb, wo, q, log_decay, hg, keep, send, stay, leave):
    heads, span, _ = q.shape
    turn, rows, size = stay.shape
    width = hg.shape[2]
    half = width // 2
    upper = (at[1] & 1) == 1
    lower = jnp.where(iota((span, span), 0) >= iota((span, span), 1), 1.0, 0.0)
    for h in range(heads):
        cut = slice(h * width, (h + 1) * width)
        h_grad = (dot(ma[...], wo[0, :, cut]) + dot(mb[...], wo[1, :, cut])).astype(BF16)
        hg[h] = h_grad
        own = log_decay[h : h + 1, :]
        lead = jnp.exp(jnp.sum(lower * own, axis=1, keepdims=True))
        total = jnp.exp(jnp.sum(own, axis=1, keepdims=True))
        part = dot((q[h].astype(F32) * lead).astype(BF16), h_grad, 0, 0)
        put_message(keep, h, jnp.where(upper, part[:, half:], part[:, :half]), total)
        put_message(send, h, jnp.where(upper, part[:, :half], part[:, half:]), total)
    mine = pl.ds(pl.multiple_of(at[0] * rows, rows), rows)
    side = at[0] ^ (at[1] // turn)

    def sort(near, far):
        for i in range(turn):
            n = i ^ (at[1] % turn)
            stay[n] = near[mine, i * size : (i + 1) * size]
            leave[n] = far[mine, i * size : (i + 1) * size]

    @pl.when(side == 0)
    def _():
        sort(ma, mb)

    @pl.when(side == 1)
    def _():
        sort(mb, ma)


def split_kernel(at, kept, came, stay, leave):
    sources, count = kept.shape[:2]
    for n, part in enumerate((kept, came)):
        for m in range(sources):
            stay[n * sources + m] = part[m, : count // 2]
            leave[n * sources + m] = part[m, count // 2 :]


def pair_kernel(at, keep, came, out):
    upper = (at[1] & 1) == 1
    for h in range(keep.shape[0]):
        mine, mine_decay = get_message(keep, h)
        theirs, their_decay = get_message(came, h)
        first = jnp.where(upper, theirs, mine)
        second = jnp.where(upper, mine, theirs)
        decay = jnp.where(upper, their_decay, mine_decay)
        put_message(out, h, first + decay * second, mine_decay * their_decay)


def join_kernel(at, group, came, later, reach, out, later_out, reach_out, *, bit):
    upper = (at[1] & bit) != 0
    for h in range(group.shape[0]):
        mine, mine_decay = get_message(group, h)
        theirs, their_decay = get_message(came, h)
        first = jnp.where(upper, theirs, mine)
        second = jnp.where(upper, mine, theirs)
        decay = jnp.where(upper, their_decay, mine_decay)
        put_message(out, h, first + decay * second, mine_decay * their_decay)
        old = reach[h : h + 1, :]
        later_out[h] = later[h] + jnp.where(upper, 0.0, old[:, 0:1]) * theirs
        reach_out[h : h + 1, :] = old * jnp.where(upper, 1.0, their_decay)


def close_kernel(at, came, later, reach, keep, first_came, own, send, *, bit):
    upper = (at[1] & bit) != 0
    right = (at[1] & 1) == 1
    for h in range(keep.shape[0]):
        theirs, _ = get_message(came, h)
        after = later[h] + jnp.where(upper, 0.0, reach[h : h + 1, 0:1]) * theirs
        mine, mine_decay = get_message(keep, h)
        pair, pair_decay = get_message(first_came, h)
        second = jnp.where(right, mine, pair)
        decay = jnp.where(right, mine_decay, pair_decay)
        through = second + decay * after
        own[h] = jnp.where(right, after, through).astype(BF16)
        send[h] = jnp.where(right, through, after).astype(BF16)


def small(kernel, outs, at, *operands, mib=8):
    spec = pl.BlockSpec()
    many = isinstance(outs, (list, tuple))
    return pl.pallas_call(
        kernel,
        in_specs=[pl.BlockSpec(memory_space=pltpu.SMEM)] + [spec] * len(operands),
        out_specs=[spec] * len(outs) if many else spec,
        out_shape=outs,
        compiler_params=limit(mib),
    )(at, *operands)


def local_kernel(at, q, k, v, log_decay, state, hg, q_grad, k_part, v_part, trails):
    heads, _, size = q.shape
    scale = size**-0.5
    for h in range(heads):
        table, lead, trail, _ = decays(log_decay[...], h)
        trails[h] = scale * trail
        scores = (dot(q[h], k[h], 1, 1) * (scale * table)).astype(BF16)
        back = (dot(hg[h], v[h], 1, 1) * table).astype(BF16)
        from_state = dot(hg[h], state[h, 0].astype(BF16), 1, 1)
        q_grad[h] = (scale * dot(back, k[h]) + lead * from_state).astype(BF16)
        k_part[h] = scale * dot(back, q[h], 0, 0)
        v_part[h] = dot(scores, hg[h], 0, 0)


def final_kernel(at, k, v, trails, own, came, k_part, v_part, k_grad, v_grad):
    heads = k.shape[0]
    half = v.shape[2] // 2
    right = (at[1] & 1) == 1
    for h in range(heads):
        low = jnp.where(right, came[h].astype(F32), own[h].astype(F32)).astype(BF16)
        high = jnp.where(right, own[h].astype(F32), came[h].astype(F32)).astype(BF16)
        back = dot(v[h, :, :half], low, 1, 1) + dot(v[h, :, half:], high, 1, 1)
        trail = trails[h]
        k_grad[h] = (k_part[h] + trail * back).astype(BF16)
        v_grad[h, :, :half] = (v_part[h, :, :half] + trail * dot(k[h], low)).astype(BF16)
        v_grad[h, :, half:] = (v_part[h, :, half:] + trail * dot(k[h], high)).astype(BF16)


def project_kernel(core, a0, a1, b0, b1, *refs):
    out, x = refs[-2:]
    turn, rows, size = a0.shape

    @pl.when(pl.program_id(0) == 0)
    def _():
        mine = pl.ds(pl.multiple_of(core[0] * rows, rows), rows)
        other = pl.ds(pl.multiple_of((1 - core[0]) * rows, rows), rows)
        for place, pair in ((mine, (a0, a1)), (other, (b0, b1))):
            x[:turn, place, :] = pair[0][...]
            x[turn:, place, :] = pair[1][...]

    total, at = None, 0
    for y in refs[:-2]:
        blocks, span, width = y.shape
        left = x[at : at + blocks].reshape(blocks * span, size)
        part = dot(left, y[...].reshape(blocks * span, width), 0, 0)
        total = part if total is None else total + part
        at += blocks
    out[...] = total


def project(at, slices, parts):
    turn, rows, size = slices[0].shape
    width = parts[0].shape[2]
    chunk = min(width, 512)
    piece = pl.BlockSpec((turn, rows, size), lambda i, *_: (0, 0, 0))
    return pl.pallas_call(
        project_kernel,
        grid_spec=pltpu.PrefetchScalarGridSpec(
            num_scalar_prefetch=1,
            grid=(width // chunk,),
            in_specs=[piece] * 4
            + [pl.BlockSpec(y.shape[:2] + (chunk,), lambda i, *_: (0, 0, i)) for y in parts],
            out_specs=pl.BlockSpec((size, chunk), lambda i, *_: (0, i)),
            scratch_shapes=[pltpu.VMEM((2 * turn, 2 * rows, size), BF16)],
        ),
        out_shape=jax.ShapeDtypeStruct((size, width), F32),
        compiler_params=limit(16),
        name="project",
    )(at, *slices, *parts)


def swap(a, axis, bit):
    count = lax.axis_size(axis)
    return lax.ppermute(a, axis, [(i, i ^ bit) for i in range(count)])


def far_first(count):
    return list(range(count // 2, count)) + list(range(count // 2 - 1, 0, -1))


def way_back(count):
    return list(range(count - 1, 0, -1))


def shared_far(count):
    return far_first(count)[: count // 2]


def bits_of(count):
    return [1 << i for i in range(count.bit_length() - 1)]


def step(
    moe_input,
    out_grad,
    routes,
    route_weight,
    w_gate,
    w_up,
    w_down,
    w_out,
    query_heads,
    key_heads,
    value_heads,
    log_decay,
    state_in,
):
    tokens, width = moe_input.shape
    half = width // 2
    sp = lax.axis_size(SP)
    tp = lax.axis_size(TP)
    place = lax.axis_index(SP).astype(jnp.int32)
    column = lax.axis_index(TP).astype(jnp.int32)
    core = column & 1
    at = jnp.stack([core, place, (column >> 1) & 1])
    experts = w_gate.shape[0] * sp
    cap = 5 * tokens * routes.shape[1] // (4 * experts)
    slots = experts * cap
    units = w_gate.shape[2]
    heads, _, size = query_heads.shape
    value_size = value_heads.shape[-1]

    picked, *sent = dispatch(at, routes.T, route_weight.T, moe_input, out_grad, experts, cap)
    came = {0: sent[0]}
    for n in far_first(sp):
        came[n] = swap(sent[n], SP, n)
    wg, grad, q, k, v, state, decay = stage(
        at, (TALL, WIDE) + (PLAIN,) * 5,
        (w_gate[0], out_grad, query_heads, key_heads, value_heads, state_in, log_decay),
    )
    wu, wd = stage(at, (TALL, WIDE), (w_up[0], w_down[0]))
    (wo,) = stage(at, (TALL,), (w_out,))
    mixed = small(
        mixed_kernel, jax.ShapeDtypeStruct((tokens, heads * value_size), BF16),
        at, q, k, v, decay, state,
    )
    blocks, homes = [], []
    for n in range(sp):
        blocks.append(came[n])
        homes.append((n, 0 if n in shared_far(sp) else None))
        if n in shared_far(sp):
            blocks.append(swap(came[n], TP, 2))
            homes.append((n, 1))
    own = small(
        functools.partial(gather_kernel, homes=tuple(homes)),
        jax.ShapeDtypeStruct((experts, cap, width), BF16), at, *blocks,
    ).reshape(slots, width)
    other = swap(own, TP, 1)
    hidden, gate_back, up_back, part_b = small(
        expert_kernel,
        [jax.ShapeDtypeStruct((slots, units), BF16)] * 3
        + [jax.ShapeDtypeStruct((slots, half), BF16)],
        at, own, other, wg, wu, wd, mib=16,
    )
    part_came = swap(part_b, TP, 1)
    part_a = small(
        partial_kernel, jax.ShapeDtypeStruct((slots, half), BF16),
        at, gate_back, up_back, wg, wu,
    )
    parts_out = small(
        add_blocks_kernel, [jax.ShapeDtypeStruct((cap, half), BF16)] * sp,
        at, part_a, part_came,
    )
    back = {0: parts_out[0]}
    for n in way_back(sp):
        back[n] = swap(parts_out[n], SP, n)
    gate_grad, up_grad = weight_grads(at, own, other, gate_back, up_back)
    down_grad = down_grads(at, own, other, hidden)

    blocks = mixed[None]
    parts = []
    for bit in reversed(bits_of(sp)):
        if not parts:
            parts = [jnp.concatenate([blocks, swap(blocks, SP, bit)], axis=0)]
        else:
            came = []
            for piece in parts:
                came.append(swap(piece, SP, bit))
            parts = parts + came

    token_shape = jax.ShapeDtypeStruct((tokens, half), BF16)
    token_part = small(combine_kernel, token_shape, at, picked, *[back[n] for n in range(sp)])
    for bit in bits_of(tp)[1:]:
        came = swap(token_part, TP, bit)
        if bit * 2 < tp:
            token_part = (token_part.astype(F32) + came.astype(F32)).astype(BF16)
    mixed_a = small(sum_kernel, token_shape, at, grad, token_part, came)
    mixed_b = swap(mixed_a, TP, 1)

    message = jax.ShapeDtypeStruct((heads, size + PIECES, value_size // 2), BF16)
    turn = sp // 2
    block = (tokens // 2, width // sp)
    head_grad, keep, send, stay, leave = small(
        carry_kernel,
        [jax.ShapeDtypeStruct((heads, tokens, value_size), BF16), message, message]
        + [jax.ShapeDtypeStruct((turn,) + block, BF16)] * 2,
        at, mixed_a, mixed_b, wo, q, decay,
    )
    sources, slices = 1, []
    for bit in reversed(bits_of(sp)):
        came_slices = swap(leave, SP, bit)
        if bit > 1:
            grid = (sources, bit) + block
            out = jax.ShapeDtypeStruct((2 * sources, bit // 2) + block, BF16)
            stay, leave = small(
                split_kernel, [out, out], at,
                stay.reshape(grid), came_slices.reshape(grid),
            )
            sources *= 2
        stay, leave = stay.reshape((turn,) + block), leave.reshape((turn,) + block)
    slices = [stay, came_slices.reshape((turn,) + block)]
    for n in range(2):
        slices.append(swap(slices[n], TP, 1))
    first_came = swap(send, SP, 1)
    q_grad, k_part, v_part, trails = small(
        local_kernel,
        [
            jax.ShapeDtypeStruct(query_heads.shape, BF16),
            jax.ShapeDtypeStruct(key_heads.shape, F32),
            jax.ShapeDtypeStruct(value_heads.shape, F32),
            jax.ShapeDtypeStruct((heads, tokens, 1), F32),
        ],
        at,
        q, k, v, decay, state, head_grad, mib=12,
    )
    state_shape = (heads, size, value_size // 2)
    group = small(pair_kernel, message, at, keep, first_came)
    later = jnp.zeros(state_shape, F32)
    reach = jnp.ones((heads, 128), F32)
    for bit in bits_of(sp)[1:]:
        came_state = swap(group, SP, bit)
        if bit * 2 < sp:
            group, later, reach = small(
                functools.partial(join_kernel, bit=bit),
                [message, jax.ShapeDtypeStruct(state_shape, F32),
                 jax.ShapeDtypeStruct((heads, 128), F32)],
                at, group, came_state, later, reach,
            )
    state_out = jax.ShapeDtypeStruct(state_shape, BF16)
    own_state, send_state = small(
        functools.partial(close_kernel, bit=bit),
        [state_out, state_out], at, came_state, later, reach, keep, first_came,
    )
    other_state = swap(send_state, SP, 1)
    out_proj_grad = project(at, slices, parts)
    k_grad, v_grad = small(
        final_kernel,
        [jax.ShapeDtypeStruct(key_heads.shape, BF16),
         jax.ShapeDtypeStruct(value_heads.shape, BF16)],
        at, k, v, trails, own_state, other_state, k_part, v_part,
    )
    return gate_grad, up_grad, down_grad, out_proj_grad, q_grad, k_grad, v_grad


def solution(mesh):
    return jax.shard_map(
        step,
        mesh=mesh,
        in_specs=(
            P(SP, None),
            P(SP, None),
            P(SP, None),
            P(SP, None),
            P(SP, None, TP),
            P(SP, None, TP),
            P(SP, TP, None),
            P(None, TP),
            P(TP, SP, None),
            P(TP, SP, None),
            P(TP, SP, None),
            P(TP, SP),
            P(TP, SP, None, None),
        ),
        out_specs=(
            P(SP, None, TP),
            P(SP, None, TP),
            P(SP, TP, None),
            P(SP, TP),
            P(TP, SP, None),
            P(TP, SP, None),
            P(TP, SP, None),
        ),
        check_vma=False,
    )
```

```python
import functools

import jax
import jax.numpy as jnp
from jax import lax
from jax.experimental import pallas as pl
from jax.experimental.pallas import tpu as pltpu
from jax.sharding import PartitionSpec as P


F32 = jnp.float32
BF16 = jnp.bfloat16
EXACT = lax.Precision.HIGHEST
SP, TP = "sp", "tp"
TALL, WIDE, PLAIN = range(3)


def dot(a, b, ca=1, cb=0, precision=None):
    return lax.dot_general(
        a, b, (((ca,), (cb,)), ((), ())), preferred_element_type=F32, precision=precision
    )


def iota(shape, axis):
    return lax.broadcasted_iota(jnp.int32, shape, axis)


def in_hbm(a):
    return pltpu.with_memory_space_constraint(a, pltpu.HBM)


def limit(mib):
    return pltpu.CompilerParams(vmem_limit_bytes=mib << 20)


def dispatch_kernel(at, routes, weight, x, g, place, *blocks, experts, cap):
    tokens, half = x.shape
    slots = experts * cap
    expert = iota((experts, tokens), 0)
    first = routes[0:1, :] == expert
    second = routes[1:2, :] == expert
    named = jnp.where(first | second, 1.0, 0.0)
    share = jnp.where(first, weight[0:1, :], 0.0) + jnp.where(second, weight[1:2, :], 0.0)
    before = jnp.where(iota((tokens, tokens), 0) < iota((tokens, tokens), 1), 1.0, 0.0)
    rank_t = dot(named.astype(BF16), before.astype(BF16))
    rank_t = jnp.where(named > 0.5, rank_t, 2.0 * cap)
    slot = iota((slots, experts), 0)
    base = (iota((slots, experts), 1) ^ at[1]) * cap
    owner = (slot >= base) & (slot < base + cap)
    owner_f = jnp.where(owner, 1.0, 0.0)
    number = jnp.sum(jnp.where(owner, slot - base, 0).astype(F32), axis=1, keepdims=True)
    hit = dot(owner_f.astype(BF16), rank_t.astype(BF16)) == number
    picked = jnp.where(hit, 1.0, 0.0).astype(BF16)
    share_slot = jnp.sum(
        jnp.where(hit, dot(owner_f, share, precision=EXACT), 0.0), axis=1, keepdims=True
    )
    place[...] = picked
    rows = dot(picked, x[...])
    grads = share_slot * dot(picked, g[...])
    quarter = half // 2
    upper = at[2] == 1
    for n, block in enumerate(blocks):
        cut = slice(n * cap, (n + 1) * cap)
        if block.shape[1] == half:
            for m, a in enumerate((rows, grads)):
                mine = jnp.where(upper, a[cut, quarter:], a[cut, :quarter])
                block[:, m * quarter : (m + 1) * quarter] = mine.astype(BF16)
        else:
            block[:, :half] = rows[cut].astype(BF16)
            block[:, half:] = grads[cut].astype(BF16)


def dispatch(at, routes, weight, x, g, experts, cap):
    tokens, width = x.shape
    half = width // 2
    slots = experts * cap
    whole = lambda i, c: (0, 0)
    mine = pl.BlockSpec((tokens, half), lambda i, c: (0, c[0]))
    wide = [half if n in shared_far(experts) else width for n in range(experts)]
    return pl.pallas_call(
        functools.partial(dispatch_kernel, experts=experts, cap=cap),
        grid_spec=pltpu.PrefetchScalarGridSpec(
            num_scalar_prefetch=1,
            grid=(1,),
            in_specs=[
                pl.BlockSpec(routes.shape, whole), pl.BlockSpec(weight.shape, whole), mine, mine,
            ],
            out_specs=[pl.BlockSpec((slots, tokens), whole)]
            + [pl.BlockSpec((cap, w), whole) for w in wide],
        ),
        out_shape=[jax.ShapeDtypeStruct((slots, tokens), BF16)]
        + [jax.ShapeDtypeStruct((cap, w), BF16) for w in wide],
        compiler_params=limit(12),
        name="dispatch",
    )(at, in_hbm(routes), in_hbm(weight), in_hbm(x), in_hbm(g))


def gather_kernel(at, *refs, homes):
    blocks, out = refs[:-1], refs[-1]
    half = out.shape[2] // 2
    quarter = half // 2

    def put(low):
        for block, (n, side) in zip(blocks, homes):
            if side is not None:
                for m in range(2):
                    begin = m * half + (0 if (side == 0) == low else quarter)
                    out[n, :, begin : begin + quarter] = block[:, m * quarter : (m + 1) * quarter]

    for block, (n, side) in zip(blocks, homes):
        if side is None:
            out[n] = block[...]

    @pl.when(at[2] == 0)
    def _():
        put(True)

    @pl.when(at[2] == 1)
    def _():
        put(False)


def stage_kernel(at, *refs, kinds):
    count = len(kinds)
    sources, outs, sems = refs[:count], refs[count:-1], refs[-1]
    copies = []

    def copy(source, target):
        copies.append(pltpu.make_async_copy(source, target, sems.at[len(copies)]))
        copies[-1].start()

    for source, target, kind in zip(sources, outs, kinds):
        if kind == PLAIN:
            copy(source, target)
            continue
        half = target.shape[1] if kind == TALL else target.shape[2]
        for side in range(2):
            begin = pl.multiple_of((at[0] if side == 0 else 1 - at[0]) * half, half)
            cut = pl.ds(begin, half)
            copy(source.at[cut, :] if kind == TALL else source.at[:, cut], target.at[side])
    for each in copies:
        each.wait()


def stage(at, kinds, arrays):
    shapes = []
    for a, kind in zip(arrays, kinds):
        if kind == TALL:
            shapes.append(pltpu.VMEM((2, a.shape[0] // 2, a.shape[1]), a.dtype))
        elif kind == WIDE:
            shapes.append(pltpu.VMEM((2, a.shape[0], a.shape[1] // 2), a.dtype))
        else:
            shapes.append(pltpu.VMEM(a.shape, a.dtype))
    count = len(arrays)
    return pl.pallas_call(
        functools.partial(stage_kernel, kinds=kinds),
        in_specs=[pl.BlockSpec(memory_space=pltpu.SMEM)]
        + [pl.BlockSpec(memory_space=pltpu.HBM)] * count,
        out_specs=[pl.BlockSpec(memory_space=pltpu.VMEM)] * count,
        out_shape=shapes,
        scratch_shapes=[pltpu.SemaphoreType.DMA((2 * count,))],
        compiler_params=limit(2),
        name="stage",
    )(at, *[in_hbm(a) for a in arrays])


def expert_kernel(at, own, other, wg, wu, wd, hidden, gback, uback, pb):
    half = own.shape[1] // 2
    units = hidden.shape[1]
    chunk = min(units, 256)
    for f in range(0, units, chunk):
        cut = slice(f, f + chunk)
        gate = dot(own[:, :half], wg[0, :, cut]) + dot(other[:, :half], wg[1, :, cut])
        up = dot(own[:, :half], wu[0, :, cut]) + dot(other[:, :half], wu[1, :, cut])
        back = dot(own[:, half:], wd[0, cut, :], 1, 1) + dot(other[:, half:], wd[1, cut, :], 1, 1)
        sig = 1.0 / (1.0 + jnp.exp(-gate))
        active = gate * sig
        hidden[:, cut] = (active * up).astype(BF16)
        gback[:, cut] = (back * up * (sig * (1.0 + gate * (1.0 - sig)))).astype(BF16)
        uback[:, cut] = (back * active).astype(BF16)
    pb[...] = (dot(gback[...], wg[1], 1, 1) + dot(uback[...], wu[1], 1, 1)).astype(BF16)


def partial_kernel(at, gback, uback, wg, wu, out):
    out[...] = (dot(gback[...], wg[0], 1, 1) + dot(uback[...], wu[0], 1, 1)).astype(BF16)


def add_blocks_kernel(at, a, b, *blocks):
    cap = blocks[0].shape[0]
    for n, block in enumerate(blocks):
        cut = slice(n * cap, (n + 1) * cap)
        block[...] = (a[cut, :].astype(F32) + b[cut, :].astype(F32)).astype(BF16)


def weights_kernel(core, ra, rb, gback, uback, gate_out, up_out):
    step = pl.program_id(0)
    turn = pl.num_programs(0) // 2

    def write(r):
        gate_out[...] = dot(r[...], gback[...], 0, 0).astype(BF16)
        up_out[...] = dot(r[...], uback[...], 0, 0).astype(BF16)

    @pl.when(step < turn)
    def _():
        write(ra)

    @pl.when(step >= turn)
    def _():
        write(rb)


def down_kernel(core, ga, gb, hidden, out):
    step = pl.program_id(0)
    turn = pl.num_programs(0) // 2

    @pl.when(step < turn)
    def _():
        out[...] = dot(hidden[...], ga[...], 0, 0).astype(BF16)

    @pl.when(step >= turn)
    def _():
        out[...] = dot(hidden[...], gb[...], 0, 0).astype(BF16)


def weight_grads(core, own, other, gback, uback):
    rows, width = own.shape
    half = width // 2
    units = gback.shape[1]
    chunk = min(half, 512)
    turn = half // chunk
    at = lambda i, c: jnp.where(i < turn, c[0] * turn + i, (1 - c[0]) * turn + i - turn)
    full = pl.BlockSpec((rows, units), lambda i, c: (0, 0))
    tall = pl.BlockSpec((None, chunk, units), lambda i, c: (0, at(i, c), 0))
    return pl.pallas_call(
        weights_kernel,
        grid_spec=pltpu.PrefetchScalarGridSpec(
            num_scalar_prefetch=1,
            grid=(2 * turn,),
            in_specs=[
                pl.BlockSpec((rows, chunk), lambda i, c: (0, jnp.minimum(i, turn - 1))),
                pl.BlockSpec((rows, chunk), lambda i, c: (0, jnp.maximum(i - turn, 0))),
                full, full,
            ],
            out_specs=[tall, tall],
        ),
        out_shape=[jax.ShapeDtypeStruct((1, width, units), BF16)] * 2,
        compiler_params=limit(16),
        name="weights",
    )(core, own, other, gback, uback)


def down_grads(core, own, other, hidden):
    rows, width = own.shape
    half = width // 2
    units = hidden.shape[1]
    chunk = min(half, 512)
    turn = half // chunk
    at = lambda i, c: jnp.where(i < turn, c[0] * turn + i, (1 - c[0]) * turn + i - turn)
    return pl.pallas_call(
        down_kernel,
        grid_spec=pltpu.PrefetchScalarGridSpec(
            num_scalar_prefetch=1,
            grid=(2 * turn,),
            in_specs=[
                pl.BlockSpec((rows, chunk), lambda i, c: (0, turn + jnp.minimum(i, turn - 1))),
                pl.BlockSpec((rows, chunk), lambda i, c: (0, turn + jnp.maximum(i - turn, 0))),
                pl.BlockSpec((rows, units), lambda i, c: (0, 0)),
            ],
            out_specs=pl.BlockSpec((None, units, chunk), lambda i, c: (0, 0, at(i, c))),
        ),
        out_shape=jax.ShapeDtypeStruct((1, units, width), BF16),
        compiler_params=limit(12),
        name="down",
    )(core, own, other, hidden)


def combine_kernel(at, place, *refs):
    blocks, out = refs[:-1], refs[-1]
    cap = blocks[0].shape[0]
    total = None
    for n, block in enumerate(blocks):
        part = dot(place[n * cap : (n + 1) * cap, :], block[...], 0, 0)
        total = part if total is None else total + part
    out[...] = total.astype(BF16)


def sum_kernel(at, g, own, came, out):
    total = own[...].astype(F32) + came[...].astype(F32)
    out[...] = (g[0].astype(F32) + total).astype(BF16)


def decays(log_decay, head):
    span = log_decay.shape[-1]
    row = iota((span, span), 0)
    col = iota((span, span), 1)
    keep = row >= col
    lower = jnp.where(keep, 1.0, 0.0)
    own = log_decay[head : head + 1, :]
    down = jnp.sum(lower * own, axis=1, keepdims=True)
    across = jnp.sum(jnp.where(row <= col, 1.0, 0.0) * jnp.sum(
        jnp.where(row == col, own, 0.0), axis=1, keepdims=True), axis=0, keepdims=True)
    total = jnp.sum(own, axis=1, keepdims=True)
    table = jnp.where(keep, jnp.exp(jnp.where(keep, down - across, 0.0)), 0.0)
    return table, jnp.exp(down), jnp.exp(total - down), total


def mixed_kernel(at, q, k, v, log_decay, state, mixed):
    heads, _, size = q.shape
    width = v.shape[2]
    scale = size**-0.5
    for h in range(heads):
        table, lead, _, _ = decays(log_decay[...], h)
        scores = (dot(q[h], k[h], 1, 1) * (scale * table)).astype(BF16)
        out = dot(scores, v[h]) + lead * dot(q[h], state[h, 0].astype(BF16))
        mixed[:, h * width : (h + 1) * width] = out.astype(BF16)


PIECES = 16


def pieces(decay, shape):
    row = iota(shape, 0)
    high = decay.astype(BF16).astype(F32)
    rest = decay - high
    middle = rest.astype(BF16).astype(F32)
    low = rest - middle
    return jnp.where(row == 0, high, jnp.where(row == 1, middle, jnp.where(row == 2, low, 0.0)))


def put_message(ref, h, body, decay):
    size = body.shape[0]
    ref[h, :size, :] = body.astype(BF16)
    if ref.shape[1] > size:
        ref[h, size:, :] = pieces(decay, (PIECES, body.shape[1])).astype(BF16)


def get_message(ref, h):
    size = ref.shape[1] - PIECES
    decay = jnp.sum(ref[h, size:, :].astype(F32), axis=0, keepdims=True)[:, 0:1]
    return ref[h, :size, :].astype(F32), decay


def carry_kernel(at, ma, mb, wo, q, log_decay, hg, keep, send, stay, leave):
    heads, span, _ = q.shape
    turn, rows, size = stay.shape
    width = hg.shape[2]
    half = width // 2
    upper = (at[1] & 1) == 1
    lower = jnp.where(iota((span, span), 0) >= iota((span, span), 1), 1.0, 0.0)
    for h in range(heads):
        cut = slice(h * width, (h + 1) * width)
        h_grad = (dot(ma[...], wo[0, :, cut]) + dot(mb[...], wo[1, :, cut])).astype(BF16)
        hg[h] = h_grad
        own = log_decay[h : h + 1, :]
        lead = jnp.exp(jnp.sum(lower * own, axis=1, keepdims=True))
        total = jnp.exp(jnp.sum(own, axis=1, keepdims=True))
        part = dot((q[h].astype(F32) * lead).astype(BF16), h_grad, 0, 0)
        put_message(keep, h, jnp.where(upper, part[:, half:], part[:, :half]), total)
        put_message(send, h, jnp.where(upper, part[:, :half], part[:, half:]), total)
    mine = pl.ds(pl.multiple_of(at[0] * rows, rows), rows)
    side = at[0] ^ (at[1] // turn)

    def sort(near, far):
        for i in range(turn):
            n = i ^ (at[1] % turn)
            stay[n] = near[mine, i * size : (i + 1) * size]
            leave[n] = far[mine, i * size : (i + 1) * size]

    @pl.when(side == 0)
    def _():
        sort(ma, mb)

    @pl.when(side == 1)
    def _():
        sort(mb, ma)


def split_kernel(at, kept, came, stay, leave):
    sources, count = kept.shape[:2]
    for n, part in enumerate((kept, came)):
        for m in range(sources):
            stay[n * sources + m] = part[m, : count // 2]
            leave[n * sources + m] = part[m, count // 2 :]


def pair_kernel(at, keep, came, out):
    upper = (at[1] & 1) == 1
    for h in range(keep.shape[0]):
        mine, mine_decay = get_message(keep, h)
        theirs, their_decay = get_message(came, h)
        first = jnp.where(upper, theirs, mine)
        second = jnp.where(upper, mine, theirs)
        decay = jnp.where(upper, their_decay, mine_decay)
        put_message(out, h, first + decay * second, mine_decay * their_decay)


def join_kernel(at, group, came, later, reach, out, later_out, reach_out, *, bit):
    upper = (at[1] & bit) != 0
    for h in range(group.shape[0]):
        mine, mine_decay = get_message(group, h)
        theirs, their_decay = get_message(came, h)
        first = jnp.where(upper, theirs, mine)
        second = jnp.where(upper, mine, theirs)
        decay = jnp.where(upper, their_decay, mine_decay)
        put_message(out, h, first + decay * second, mine_decay * their_decay)
        old = reach[h : h + 1, :]
        later_out[h] = later[h] + jnp.where(upper, 0.0, old[:, 0:1]) * theirs
        reach_out[h : h + 1, :] = old * jnp.where(upper, 1.0, their_decay)


def close_kernel(at, came, later, reach, keep, first_came, own, send, *, bit):
    upper = (at[1] & bit) != 0
    right = (at[1] & 1) == 1
    for h in range(keep.shape[0]):
        theirs = came[h, : later.shape[1], :].astype(F32)
        after = later[h] + jnp.where(upper, 0.0, reach[h : h + 1, 0:1]) * theirs
        mine, mine_decay = get_message(keep, h)
        pair, pair_decay = get_message(first_came, h)
        second = jnp.where(right, mine, pair)
        decay = jnp.where(right, mine_decay, pair_decay)
        through = second + decay * after
        own[h] = jnp.where(right, after, through).astype(BF16)
        send[h] = jnp.where(right, through, after).astype(BF16)


def small(kernel, outs, at, *operands, mib=8):
    spec = pl.BlockSpec()
    many = isinstance(outs, (list, tuple))
    return pl.pallas_call(
        kernel,
        in_specs=[pl.BlockSpec(memory_space=pltpu.SMEM)] + [spec] * len(operands),
        out_specs=[spec] * len(outs) if many else spec,
        out_shape=outs,
        compiler_params=limit(mib),
    )(at, *operands)


def local_kernel(at, q, k, v, log_decay, state, hg, q_grad, k_part, v_part, trails):
    heads, _, size = q.shape
    scale = size**-0.5
    for h in range(heads):
        table, lead, trail, _ = decays(log_decay[...], h)
        trails[h] = scale * trail
        scores = (dot(q[h], k[h], 1, 1) * (scale * table)).astype(BF16)
        back = (dot(hg[h], v[h], 1, 1) * table).astype(BF16)
        from_state = dot(hg[h], state[h, 0].astype(BF16), 1, 1)
        q_grad[h] = (scale * dot(back, k[h]) + lead * from_state).astype(BF16)
        k_part[h] = scale * dot(back, q[h], 0, 0)
        v_part[h] = dot(scores, hg[h], 0, 0)


def final_kernel(at, k, v, trails, own, came, k_part, v_part, k_grad, v_grad):
    heads = k.shape[0]
    half = v.shape[2] // 2
    right = (at[1] & 1) == 1
    for h in range(heads):
        low = jnp.where(right, came[h].astype(F32), own[h].astype(F32)).astype(BF16)
        high = jnp.where(right, own[h].astype(F32), came[h].astype(F32)).astype(BF16)
        back = dot(v[h, :, :half], low, 1, 1) + dot(v[h, :, half:], high, 1, 1)
        trail = trails[h]
        k_grad[h] = (k_part[h] + trail * back).astype(BF16)
        v_grad[h, :, :half] = (v_part[h, :, :half] + trail * dot(k[h], low)).astype(BF16)
        v_grad[h, :, half:] = (v_part[h, :, half:] + trail * dot(k[h], high)).astype(BF16)


def project_kernel(core, a, b, *refs, held):
    out, x = refs[-2:]
    _, rows, size = a.shape

    @pl.when(pl.program_id(0) == 0)
    def _():
        x[:, pl.ds(pl.multiple_of(core[0] * rows, rows), rows), :] = a[...]
        x[:, pl.ds(pl.multiple_of((1 - core[0]) * rows, rows), rows), :] = b[...]

    total, at = (refs[0][...] if held else None), 0
    for y in refs[1 if held else 0 : -2]:
        count, span, width = y.shape
        left = x[at : at + count].reshape(count * span, size)
        part = dot(left, y[...].reshape(count * span, width), 0, 0)
        total = part if total is None else total + part
        at += count
    out[...] = total


def project(at, slices, parts, held=()):
    blocks, rows, size = slices[0].shape
    width = parts[0].shape[2]
    chunk = min(width, 512)
    piece = pl.BlockSpec((blocks, rows, size), lambda i, *_: (0, 0, 0))
    result = pl.BlockSpec((size, chunk), lambda i, *_: (0, i))
    return pl.pallas_call(
        functools.partial(project_kernel, held=len(held) > 0),
        grid_spec=pltpu.PrefetchScalarGridSpec(
            num_scalar_prefetch=1,
            grid=(width // chunk,),
            in_specs=[piece] * 2
            + [result] * len(held)
            + [pl.BlockSpec(y.shape[:2] + (chunk,), lambda i, *_: (0, 0, i)) for y in parts],
            out_specs=result,
            scratch_shapes=[pltpu.VMEM((blocks, 2 * rows, size), BF16)],
        ),
        out_shape=jax.ShapeDtypeStruct((size, width), F32),
        compiler_params=limit(16),
        name="project",
    )(at, *slices, *held, *parts)


def swap(a, axis, bit):
    count = lax.axis_size(axis)
    return lax.ppermute(a, axis, [(i, i ^ bit) for i in range(count)])


def far_first(count):
    return list(range(count // 2, count)) + list(range(count // 2 - 1, 0, -1))


def way_back(count):
    return list(range(count - 1, 0, -1))


def shared_far(count):
    return far_first(count)[: count // 2]


def bits_of(count):
    return [1 << i for i in range(count.bit_length() - 1)]


def step(
    moe_input,
    out_grad,
    routes,
    route_weight,
    w_gate,
    w_up,
    w_down,
    w_out,
    query_heads,
    key_heads,
    value_heads,
    log_decay,
    state_in,
):
    tokens, width = moe_input.shape
    half = width // 2
    sp = lax.axis_size(SP)
    tp = lax.axis_size(TP)
    place = lax.axis_index(SP).astype(jnp.int32)
    column = lax.axis_index(TP).astype(jnp.int32)
    core = column & 1
    at = jnp.stack([core, place, (column >> 1) & 1])
    experts = w_gate.shape[0] * sp
    cap = 5 * tokens * routes.shape[1] // (4 * experts)
    slots = experts * cap
    units = w_gate.shape[2]
    heads, _, size = query_heads.shape
    value_size = value_heads.shape[-1]

    picked, *sent = dispatch(at, routes.T, route_weight.T, moe_input, out_grad, experts, cap)
    came = {0: sent[0]}
    for n in far_first(sp):
        came[n] = swap(sent[n], SP, n)
    wg, grad, q, k, v, state, decay = stage(
        at, (TALL, WIDE) + (PLAIN,) * 5,
        (w_gate[0], out_grad, query_heads, key_heads, value_heads, state_in, log_decay),
    )
    wu, wd = stage(at, (TALL, WIDE), (w_up[0], w_down[0]))
    (wo,) = stage(at, (TALL,), (w_out,))
    mixed = small(
        mixed_kernel, jax.ShapeDtypeStruct((tokens, heads * value_size), BF16),
        at, q, k, v, decay, state,
    )
    blocks, homes = [], []
    for n in range(sp):
        blocks.append(came[n])
        homes.append((n, 0 if n in shared_far(sp) else None))
        if n in shared_far(sp):
            blocks.append(swap(came[n], TP, 2))
            homes.append((n, 1))
    own = small(
        functools.partial(gather_kernel, homes=tuple(homes)),
        jax.ShapeDtypeStruct((experts, cap, width), BF16), at, *blocks,
    ).reshape(slots, width)
    other = swap(own, TP, 1)
    hidden, gate_back, up_back, part_b = small(
        expert_kernel,
        [jax.ShapeDtypeStruct((slots, units), BF16)] * 3
        + [jax.ShapeDtypeStruct((slots, half), BF16)],
        at, own, other, wg, wu, wd, mib=16,
    )
    part_came = swap(part_b, TP, 1)
    part_a = small(
        partial_kernel, jax.ShapeDtypeStruct((slots, half), BF16),
        at, gate_back, up_back, wg, wu,
    )
    parts_out = small(
        add_blocks_kernel, [jax.ShapeDtypeStruct((cap, half), BF16)] * sp,
        at, part_a, part_came,
    )
    back = {0: parts_out[0]}
    for n in way_back(sp):
        back[n] = swap(parts_out[n], SP, n)
    gate_grad, up_grad = weight_grads(at, own, other, gate_back, up_back)
    down_grad = down_grads(at, own, other, hidden)

    blocks = mixed[None]
    parts = []
    for bit in reversed(bits_of(sp)):
        if not parts:
            parts = [jnp.concatenate([blocks, swap(blocks, SP, bit)], axis=0)]
        else:
            came = []
            for piece in parts:
                came.append(swap(piece, SP, bit))
            parts = parts + came

    token_shape = jax.ShapeDtypeStruct((tokens, half), BF16)
    token_part = small(combine_kernel, token_shape, at, picked, *[back[n] for n in range(sp)])
    for bit in bits_of(tp)[1:]:
        came = swap(token_part, TP, bit)
        if bit * 2 < tp:
            token_part = (token_part.astype(F32) + came.astype(F32)).astype(BF16)
    mixed_a = small(sum_kernel, token_shape, at, grad, token_part, came)
    mixed_b = swap(mixed_a, TP, 1)

    message = jax.ShapeDtypeStruct((heads, size + PIECES, value_size // 2), BF16)
    turn = sp // 2
    block = (tokens // 2, width // sp)
    head_grad, keep, send, stay, leave = small(
        carry_kernel,
        [jax.ShapeDtypeStruct((heads, tokens, value_size), BF16), message, message]
        + [jax.ShapeDtypeStruct((turn,) + block, BF16)] * 2,
        at, mixed_a, mixed_b, wo, q, decay,
    )
    sources, slices = 1, []
    for bit in reversed(bits_of(sp)):
        came_slices = swap(leave, SP, bit)
        if bit > 1:
            grid = (sources, bit) + block
            out = jax.ShapeDtypeStruct((2 * sources, bit // 2) + block, BF16)
            stay, leave = small(
                split_kernel, [out, out], at,
                stay.reshape(grid), came_slices.reshape(grid),
            )
            sources *= 2
        stay, leave = stay.reshape((turn,) + block), leave.reshape((turn,) + block)
    slices = [stay, came_slices.reshape((turn,) + block)]
    for n in range(2):
        slices.append(swap(slices[n], TP, 1))
    first_came = swap(send, SP, 1)
    q_grad, k_part, v_part, trails = small(
        local_kernel,
        [
            jax.ShapeDtypeStruct(query_heads.shape, BF16),
            jax.ShapeDtypeStruct(key_heads.shape, F32),
            jax.ShapeDtypeStruct(value_heads.shape, F32),
            jax.ShapeDtypeStruct((heads, tokens, 1), F32),
        ],
        at,
        q, k, v, decay, state, head_grad, mib=12,
    )
    state_shape = (heads, size, value_size // 2)
    group = small(pair_kernel, message, at, keep, first_came)
    later = jnp.zeros(state_shape, F32)
    reach = jnp.ones((heads, 128), F32)
    for bit in bits_of(sp)[1:]:
        came_state = swap(group, SP, bit)
        if bit * 2 < sp:
            group, later, reach = small(
                functools.partial(join_kernel, bit=bit),
                [message if bit * 4 < sp else jax.ShapeDtypeStruct(state_shape, BF16),
                 jax.ShapeDtypeStruct(state_shape, F32),
                 jax.ShapeDtypeStruct((heads, 128), F32)],
                at, group, came_state, later, reach,
            )
    state_out = jax.ShapeDtypeStruct(state_shape, BF16)
    own_state, send_state = small(
        functools.partial(close_kernel, bit=bit),
        [state_out, state_out], at, came_state, later, reach, keep, first_came,
    )
    other_state = swap(send_state, SP, 1)
    middle = len(parts) // 2
    held = project(at, slices[0::2], parts[:middle])
    out_proj_grad = project(at, slices[1::2], parts[middle:], (held,))
    k_grad, v_grad = small(
        final_kernel,
        [jax.ShapeDtypeStruct(key_heads.shape, BF16),
         jax.ShapeDtypeStruct(value_heads.shape, BF16)],
        at, k, v, trails, own_state, other_state, k_part, v_part,
    )
    return gate_grad, up_grad, down_grad, out_proj_grad, q_grad, k_grad, v_grad


def solution(mesh):
    return jax.shard_map(
        step,
        mesh=mesh,
        in_specs=(
            P(SP, None),
            P(SP, None),
            P(SP, None),
            P(SP, None),
            P(SP, None, TP),
            P(SP, None, TP),
            P(SP, TP, None),
            P(None, TP),
            P(TP, SP, None),
            P(TP, SP, None),
            P(TP, SP, None),
            P(TP, SP),
            P(TP, SP, None, None),
        ),
        out_specs=(
            P(SP, None, TP),
            P(SP, None, TP),
            P(SP, TP, None),
            P(SP, TP),
            P(TP, SP, None),
            P(TP, SP, None),
            P(TP, SP, None),
        ),
        check_vma=False,
    )
```
